512 devices in a mesh: sp: 16 (over z), fs: 4 (over y), tp: 8 (over x, core).
Axes of the slice: x: 4, y: 4, z: 16, core: 2. Of those that a mesh axis runs over, the one named last changes fastest.
Arguments:
- activations: bfloat16 [4, 4096, 4096], P('fs', 'sp'), may hold values from -60 to 60
- input_norm_gain: float32 [4096], replicated, may hold values from 0.1 to 1.9
- pooling_channel_weight: bfloat16 [4096, 1024], P(('sp', 'fs'), 'tp'), may hold values from -0.09375 to 0.09375
- query_projection_weight: bfloat16 [4096, 1024], P(('sp', 'fs'), 'tp'), may hold values from -0.09375 to 0.09375
- key_projection_weight: bfloat16 [4096, 1024], P(('sp', 'fs'), 'tp'), may hold values from -0.09375 to 0.09375
- value_projection_weight: bfloat16 [4096, 1024], P(('sp', 'fs'), 'tp'), may hold values from -0.09375 to 0.09375
- output_gate_weight: bfloat16 [4096, 1024], P(('sp', 'fs'), 'tp'), may hold values from -0.09375 to 0.09375
- decay_first_factor: bfloat16 [4096, 64], P(('sp', 'fs')), may hold values from -0.09375 to 0.09375
- decay_second_factor: bfloat16 [64, 1024], P(None, 'tp'), may hold values from -0.75 to 0.75
- decay_gate_bias: float32 [1024], P('tp')
- decay_extra_log: float32 [16, 4096], P('tp', 'sp'), may hold values from -1.5 to 0
- head_norm_gain: float32 [1024], P('tp'), may hold values from 0.1 to 1.9
- starting_state: float32 [4, 16, 64, 64], P('fs', 'tp'), may hold values from -384 to 384
- pooling_group_weight: bfloat16 [8, 128, 128], P('tp'), may hold values from -0.5 to 0.5
- pooling_channel_scale: float32 [1024], P('tp'), may hold values from 0.1 to 1.9
- pooling_output_rows: bfloat16 [1024, 4096], P('sp', 'tp'), may hold values from -0.125 to 0.125
- attention_output_rows: bfloat16 [1024, 4096], P('sp', 'tp'), may hold values from -0.125 to 0.125
Outputs:
- mixed: bfloat16 [4, 4096, 4096], P('fs', 'sp', 'tp')
The draws below stay inside these ranges and needn't reach their ends.
All inputs are finite; a program needn't handle non-finite values.
Results may differ from the reference program's by a relative error of at most 0.012.
Values may be sent and summed in bfloat16 or wider, within the bound.
No kernel may reach another device: no remote copies, remote signals or barrier semaphores. Data moves between devices by JAX's collectives and lax.ppermute only.
A program may use at most 64 MiB of HBM per device.

```python
import math
import jax
import jax.numpy as jnp
from jax import lax

D = 4096
POOL_WIDTH = 1024
POOL_GROUP_WIDTH = 128
GLA_HEADS = 16
HEAD_WIDTH = 64
RANK = 64
BLOCK = 64
REACH = 15
TOK_DEV = 256
LENGTH = 4096
SEQS = 4
POOL_GROUPS = 8
GLA_WIDTH = 1024


def draw_activations(key, part):
    normal_part = jax.random.normal(jax.random.fold_in(key, 1), (SEQS, LENGTH, D), jnp.float32)
    drawn = jnp.clip(normal_part, -6.0, 6.0)
    return drawn.astype(jnp.bfloat16)


def draw_decay_gate_bias(key, part):
    slow_share = 0.5
    slow_heads = jax.random.bernoulli(jax.random.fold_in(key, 11), slow_share, (GLA_HEADS,))
    jitter = jax.random.uniform(jax.random.fold_in(key, 12), (GLA_HEADS, HEAD_WIDTH), jnp.float32, -0.3, 0.3)
    slow_level = math.log(LENGTH / (0.3 * 16.0))
    levels = jnp.where(slow_heads[:, None], slow_level, 0.7) + jitter
    return levels.reshape(GLA_HEADS * HEAD_WIDTH).astype(jnp.float32)


def draw_decay_extra_log(key, part):
    shard_count = LENGTH // TOK_DEV
    rates = jnp.exp(jax.random.uniform(jax.random.fold_in(key, 21), (shard_count,), jnp.float32, math.log(0.15), math.log(1.2)))
    baseline = -jnp.repeat(rates, TOK_DEV) / LENGTH
    spots = jax.random.randint(jax.random.fold_in(key, 22), (GLA_HEADS, 2), 0, LENGTH)
    depths = jnp.log(jax.random.uniform(jax.random.fold_in(key, 23), (GLA_HEADS, 2), jnp.float32, 0.5, 0.8))
    hits = (jnp.arange(LENGTH)[None, None, :] == spots[:, :, None]).astype(jnp.float32) * depths[:, :, None]
    return (baseline[None, :] + jnp.sum(hits, axis=1)).astype(jnp.float32)


def level_of(key, shape, pieces, low, largest):
    loudness, own = 1.0, jax.random.fold_in(key, 6)
    for dim, blocks in pieces:
        steps = jnp.exp(jax.random.uniform(jax.random.fold_in(own, dim), (blocks,), jnp.float32, low / len(pieces), largest / len(pieces)))
        loudness = loudness * jnp.repeat(steps, shape[dim] // blocks).reshape([-1 if axis == dim else 1 for axis in range(len(shape))])
    return loudness


def gaussian(key, extent, width, reach, shards=(), kind=jnp.bfloat16):
    entries = width * jax.random.normal(key, extent, jnp.float32)
    if shards:
        entries = entries * level_of(key, extent, shards, -0.22, 0.18)
    return jnp.clip(entries, -reach, reach).astype(kind)


def setup_inputs(seed: int = 0) -> dict:
    streams_of = jax.random.split(jax.random.key(seed), 18)
    return {
        "activations": draw_activations(jax.random.fold_in(streams_of[17], 71), 0),
        "input_norm_gain": jnp.clip(1.0 + 0.18 * jax.random.normal(streams_of[1], (D,), jnp.float32), 0.1, 1.9),
        "pooling_channel_weight": gaussian(streams_of[2], (D, POOL_WIDTH), D ** -0.5, 0.09375, ((0, 64), (1, 8))),
        "query_projection_weight": gaussian(streams_of[3], (D, GLA_WIDTH), D ** -0.5, 0.09375, ((0, 64), (1, 8))),
        "key_projection_weight": gaussian(streams_of[4], (D, GLA_WIDTH), D ** -0.5, 0.09375, ((0, 64), (1, 8))),
        "value_projection_weight": gaussian(streams_of[5], (D, GLA_WIDTH), D ** -0.5, 0.09375, ((0, 64), (1, 8))),
        "output_gate_weight": gaussian(streams_of[6], (D, GLA_WIDTH), D ** -0.5, 0.09375, ((0, 64), (1, 8))),
        "decay_first_factor": gaussian(streams_of[7], (D, RANK), D ** -0.5, 0.09375, ((0, 64),)),
        "decay_second_factor": gaussian(streams_of[8], (RANK, GLA_WIDTH), RANK ** -0.5, 0.75, ((1, 8),)),
        "decay_gate_bias": draw_decay_gate_bias(jax.random.fold_in(streams_of[17], 71), 0),
        "decay_extra_log": draw_decay_extra_log(jax.random.fold_in(streams_of[17], 71), 0),
        "head_norm_gain": jnp.clip(1.0 + 0.18 * jax.random.normal(streams_of[11], (GLA_WIDTH,), jnp.float32), 0.1, 1.9),
        "starting_state": gaussian(streams_of[12], (SEQS, GLA_HEADS, HEAD_WIDTH, HEAD_WIDTH), (LENGTH ** 0.5), 384.0, ((0, 4), (1, 8)), jnp.float32),
        "pooling_group_weight": gaussian(streams_of[13], (POOL_GROUPS, POOL_GROUP_WIDTH, POOL_GROUP_WIDTH), POOL_GROUP_WIDTH ** -0.5, 0.5, ((0, 8),)),
        "pooling_channel_scale": jnp.clip(1.0 + 0.18 * jax.random.normal(streams_of[14], (POOL_WIDTH,), jnp.float32), 0.1, 1.9),
        "pooling_output_rows": gaussian(streams_of[15], (POOL_WIDTH, D), (POOL_WIDTH + GLA_WIDTH) ** -0.5, 0.125, ((0, 16), (1, 8))),
        "attention_output_rows": gaussian(streams_of[16], (GLA_WIDTH, D), (POOL_WIDTH + GLA_WIDTH) ** -0.5, 0.125, ((0, 16), (1, 8))),
    }


norm_eps = 1e-06
decay_temper = 16.0
highest = lax.Precision.HIGHEST

def window_levels(extended, total_row_count):
    width_two = extended[:, 1:] + extended[:, :-1]
    width_four = width_two[:, 2:] + width_two[:, :-2]
    width_eight = width_four[:, 4:] + width_four[:, :-4]
    width_sixteen = width_eight[:, 8:] + width_eight[:, :-8]
    return (width_two[:, -total_row_count:], width_four[:, -total_row_count:], width_eight[:, -total_row_count:], width_sixteen)

def pool_reference(pool_input, pooling_group_weight, pooling_channel_scale):
    sequence_count, length_all, channels = pool_input.shape
    current = pool_input.astype(jnp.float32)
    extended = jnp.concatenate([jnp.zeros((sequence_count, REACH, channels), jnp.float32), current], axis=1)
    window_sums = window_levels(extended, length_all)
    level_ids = jnp.arange(channels) // POOL_GROUP_WIDTH % 4
    window = jnp.where(level_ids == 0, 2.0, jnp.where(level_ids == 1, 4.0, jnp.where(level_ids == 2, 8.0, 16.0))).astype(jnp.float32)
    chosen = jnp.where(level_ids == 0, window_sums[0], jnp.where(level_ids == 1, window_sums[1], jnp.where(level_ids == 2, window_sums[2], window_sums[3])))
    positions = jnp.arange(length_all).astype(jnp.float32)
    counts = jnp.minimum(positions[:, None] + 1.0, window[None, :])
    deviation = (chosen / counts - current).astype(jnp.bfloat16)
    grouped = deviation.reshape(sequence_count, length_all, POOL_GROUPS, POOL_GROUP_WIDTH).astype(jnp.float32)
    mixture = jnp.einsum('btgc,gcd->btgd', grouped, pooling_group_weight.astype(jnp.float32))
    return (mixture.reshape(sequence_count, length_all, channels) * pooling_channel_scale).astype(jnp.bfloat16)

def decay_log_values(decay_lower_bound, decay_second_factor, decay_gate_bias, decay_extra_log):
    sequence_count, total_row_count, rank_width = decay_lower_bound.shape
    gate_input = jnp.dot(decay_lower_bound.reshape(sequence_count * total_row_count, rank_width), decay_second_factor, preferred_element_type=jnp.float32) + decay_gate_bias
    logarithm_rates = jax.nn.log_sigmoid(gate_input) / decay_temper
    local_head_count = decay_extra_log.shape[0]
    logarithm_rates = logarithm_rates.reshape(sequence_count, total_row_count, local_head_count, HEAD_WIDTH) + decay_extra_log.T[None, :, :, None]
    return logarithm_rates.reshape(sequence_count, total_row_count, local_head_count * HEAD_WIDTH)

def to_blocks(source, local_head_count):
    sequence_count, total_row_count, _ = source.shape
    shaped = source.astype(jnp.float32).reshape(sequence_count, total_row_count // BLOCK, BLOCK, local_head_count, HEAD_WIDTH)
    return shaped.transpose(0, 3, 1, 2, 4)

def block_terms(queries, keys, values, decay_logarithm, local_head_count):
    scaled_query = to_blocks(queries, local_head_count) * HEAD_WIDTH ** (-0.5)
    key_blocks = to_blocks(keys, local_head_count)
    value_blocks = to_blocks(values, local_head_count)
    decay_sum = jnp.cumsum(to_blocks(decay_logarithm, local_head_count), axis=3)
    final_log = decay_sum[:, :, :, -1:, :]
    middle = decay_sum[:, :, :, BLOCK // 2 - 1:BLOCK // 2, :]
    scores = jnp.einsum('bhncd,bhnsd->bhncs', scaled_query * jnp.exp(decay_sum - middle), key_blocks * jnp.exp(middle - decay_sum), precision=highest)
    causal = jnp.tril(jnp.ones((BLOCK, BLOCK), dtype=bool))
    scores = jnp.where(causal, scores, 0.0)
    within = jnp.einsum('bhncs,bhnse->bhnce', scores, value_blocks, precision=highest)
    block_states = jnp.einsum('bhncd,bhnce->bhnde', key_blocks * jnp.exp(final_log - decay_sum), value_blocks, precision=highest)
    return (scaled_query, decay_sum, within, block_states)

def finish(scaled_query, decay_sum, within, prior_states, outgate, head_norm_gain):
    carried = jnp.einsum('bhncd,bhnde->bhnce', scaled_query * jnp.exp(decay_sum), prior_states, precision=highest)
    merged = within + carried
    merged = merged * lax.rsqrt(lax.optimization_barrier(jnp.mean(merged * merged, axis=-1, keepdims=True)) + norm_eps)
    sequence_count, local_head_count, blocks, _, _ = merged.shape
    merged = merged.transpose(0, 2, 3, 1, 4).reshape(sequence_count, blocks * BLOCK, local_head_count * HEAD_WIDTH) * head_norm_gain
    return (merged * jax.nn.silu(outgate.astype(jnp.float32))).astype(jnp.bfloat16)

def reference(activations, input_norm_gain, pooling_channel_weight, query_projection_weight, key_projection_weight, value_projection_weight, output_gate_weight, decay_first_factor, decay_second_factor, decay_gate_bias, decay_extra_log, head_norm_gain, starting_state, pooling_group_weight, pooling_channel_scale, pooling_output_rows, attention_output_rows):
    sequence_count, length_all, model_width = activations.shape
    flat_rows = activations.reshape(sequence_count * length_all, model_width).astype(jnp.float32)
    inverse = lax.rsqrt(lax.optimization_barrier(jnp.mean(flat_rows * flat_rows, axis=1, keepdims=True)) + norm_eps)
    scaled = (flat_rows * input_norm_gain).astype(jnp.bfloat16)

    def apply_projection(weight):
        product = jnp.dot(scaled, weight, preferred_element_type=jnp.float32)
        return (product * inverse).astype(jnp.bfloat16).reshape(sequence_count, length_all, weight.shape[1])
    pool_out = pool_reference(apply_projection(pooling_channel_weight), pooling_group_weight, pooling_channel_scale)
    queries = apply_projection(query_projection_weight)
    keys = apply_projection(key_projection_weight)
    values = apply_projection(value_projection_weight)
    outgate = apply_projection(output_gate_weight)
    decay_logarithm = decay_log_values(apply_projection(decay_first_factor), decay_second_factor, decay_gate_bias, decay_extra_log)
    local_head_count = starting_state.shape[1]
    scaled_query, decay_sum, within, block_states = block_terms(queries, keys, values, decay_logarithm, local_head_count)
    block_decay = jnp.exp(decay_sum[:, :, :, -1, :])

    def advance(state_now, block_pair):
        return (block_pair[1][..., None] * state_now + block_pair[0], state_now)
    _, prior_states = lax.scan(advance, starting_state, (block_states.transpose(2, 0, 1, 3, 4), block_decay.transpose(2, 0, 1, 3)))
    prior_states = prior_states.transpose(1, 2, 0, 3, 4)
    state_out = finish(scaled_query, decay_sum, within, prior_states, outgate, head_norm_gain)
    rows_all = sequence_count * length_all
    projected = jnp.dot(pool_out.reshape(rows_all, -1), pooling_output_rows, preferred_element_type=jnp.float32)
    projected = projected + jnp.dot(state_out.reshape(rows_all, -1), attention_output_rows, preferred_element_type=jnp.float32)
    return projected.astype(jnp.bfloat16).reshape(sequence_count, length_all, model_width)
```

```python
import jax
import jax.numpy as jnp
from jax import lax
from jax.experimental import pallas as pl
from jax.experimental.pallas import tpu as pltpu
from jax.sharding import PartitionSpec as P

POOL_GROUP_WIDTH = 128
HEAD_WIDTH = 64
BLOCK = 64
REACH = 15

norm_eps = 1e-06
decay_temper = 16.0
highest = lax.Precision.HIGHEST


def shifted(x, axis, by, wrap):
    n = lax.axis_size(axis)
    if wrap:
        pairs = [(i, (i + by) % n) for i in range(n)]
    else:
        pairs = [(i, i + by) for i in range(n) if 0 <= i + by < n]
    return lax.ppermute(x, axis, pairs)


def prep_kernel(own, act, gain, x0, x1, x2, x3, inverse):
    f32 = jnp.float32
    rows, width = act.shape
    outs = (x0, x1, x2, x3)
    lane = lax.broadcasted_iota(jnp.int32, (rows, 128), 1)
    low = lane < 64
    squares = jnp.zeros((rows, 128), f32)
    me = own[0]
    for p in range(width // 512):
        tiles = []
        for q in range(4):
            at = p * 512 + q * 128
            t = act[:, at : at + 128].astype(f32)
            squares = squares + t * t
            tiles.append(t * gain[:, at : at + 128])
        blocks = []
        for a, b in ((tiles[0], tiles[2]), (tiles[1], tiles[3])):
            blocks.append(jnp.where(low, a, pltpu.roll(b, 64, 1)).astype(jnp.bfloat16))
            blocks.append(jnp.where(low, pltpu.roll(a, 64, 1), b).astype(jnp.bfloat16))
        for f in range(4):

            @pl.when(me == f)
            def _(f=f, blocks=blocks, p=p):
                for k in range(4):
                    outs[k][:, p * 128 : (p + 1) * 128] = blocks[(f + k) % 4]

    total = jnp.sum(squares, axis=1, keepdims=True)
    inverse[...] = jnp.broadcast_to(lax.rsqrt(total / width + norm_eps), (rows, 128))


def prepare(act, gain, own):
    tokens, width = act.shape
    rows = 64
    part = pl.BlockSpec((rows, width // 4), lambda i, own: (i, 0))
    return pl.pallas_call(
        prep_kernel,
        grid_spec=pltpu.PrefetchScalarGridSpec(
            num_scalar_prefetch=1,
            grid=(tokens // rows,),
            in_specs=[
                pl.BlockSpec((rows, width), lambda i, own: (i, 0)),
                pl.BlockSpec((1, width), lambda i, own: (0, 0)),
            ],
            out_specs=[part, part, part, part, pl.BlockSpec((rows, 128), lambda i, own: (i, 0))],
        ),
        out_shape=[jax.ShapeDtypeStruct((tokens, width // 4), jnp.bfloat16)] * 4
        + [jax.ShapeDtypeStruct((tokens, 128), jnp.float32)],
        name="prep",
    )(own, act, gain)


def pool_branch(pool_input, previous, group_weight, channel_scale, group, position_first):
    rows, channels = pool_input.shape
    current = pool_input.astype(jnp.float32)
    extended = jnp.concatenate([previous.astype(jnp.float32), current], axis=0)
    two = extended[1:] + extended[:-1]
    four = two[2:] + two[:-2]
    eight = four[4:] + four[:-4]
    sixteen = eight[8:] + eight[:-8]
    level = group % 4
    chosen = jnp.where(
        level == 0,
        two[-rows:],
        jnp.where(level == 1, four[-rows:], jnp.where(level == 2, eight[-rows:], sixteen)),
    )
    window = jnp.where(
        level == 0, 2.0, jnp.where(level == 1, 4.0, jnp.where(level == 2, 8.0, 16.0))
    ).astype(jnp.float32)
    positions = (position_first + jnp.arange(rows)).astype(jnp.float32)
    counts = jnp.minimum(positions[:, None] + 1.0, window)
    deviation = (chosen / counts - current).astype(jnp.bfloat16)
    mixture = jnp.dot(deviation, group_weight[0], preferred_element_type=jnp.float32)
    return (mixture * channel_scale).astype(jnp.bfloat16)


def to_blocks(source, heads):
    rows, _ = source.shape
    shaped = source.astype(jnp.float32).reshape(rows // BLOCK, BLOCK, heads, HEAD_WIDTH)
    return shaped.transpose(2, 0, 1, 3)


def project_back(parts):
    total = parts[0]
    for k in (1, 2, 3):
        total = total + shifted(parts[k].astype(jnp.bfloat16), "fs", -k, True).astype(jnp.float32)
    return total


def body(
    activations,
    input_norm_gain,
    pooling_channel_weight,
    query_projection_weight,
    key_projection_weight,
    value_projection_weight,
    output_gate_weight,
    decay_first_factor,
    decay_second_factor,
    decay_gate_bias,
    decay_extra_log,
    head_norm_gain,
    starting_state,
    pooling_group_weight,
    pooling_channel_scale,
    pooling_output_rows,
    attention_output_rows,
):
    f32 = jnp.float32
    bf16 = jnp.bfloat16
    _, tokens, width = activations.shape
    heads = starting_state.shape[1]
    own = lax.axis_index("fs").astype(jnp.int32).reshape(1)
    late = jnp.concatenate(
        [
            query_projection_weight,
            output_gate_weight,
            pooling_channel_weight,
            pooling_output_rows,
            attention_output_rows,
        ],
        axis=1,
    )
    late = lax.all_gather(late, "sp", axis=0, tiled=True)
    x0, x1, x2, x3, inverse = prepare(
        activations.reshape(tokens, width), input_norm_gain.reshape(1, width), own
    )
    early = jnp.concatenate(
        [key_projection_weight, value_projection_weight, decay_first_factor], axis=1
    )
    with jax.named_scope("early"):
        early = lax.all_gather(early, "sp", axis=0, tiled=True)
    with jax.named_scope("exchange"):
        x1 = shifted(x1, "fs", 1, True)
        x2 = shifted(x2, "fs", 2, True)
        x3 = shifted(x3, "fs", 3, True)
    xs = (x0, x1, x2, x3)
    inverse = inverse[:, :1]
    got = project_back([jnp.dot(x, early, preferred_element_type=f32) for x in xs])
    got = (got * inverse).astype(bf16)
    keys, values, low = got[:, :128], got[:, 128:256], got[:, 256:]

    gate_input = jnp.dot(low, decay_second_factor, preferred_element_type=f32) + decay_gate_bias
    rates = jax.nn.log_sigmoid(gate_input) / decay_temper
    rates = rates + jnp.repeat(decay_extra_log.T, HEAD_WIDTH, axis=1)
    key_blocks = to_blocks(keys, heads)
    value_blocks = to_blocks(values, heads)
    decay_sum = jnp.cumsum(to_blocks(rates, heads), axis=2)
    final_log = decay_sum[:, :, -1:, :]
    middle = decay_sum[:, :, BLOCK // 2 - 1 : BLOCK // 2, :]
    block_states = jnp.einsum(
        "hncd,hnce->hnde",
        key_blocks * jnp.exp(final_log - decay_sum),
        value_blocks,
        precision=highest,
    )
    block_log = decay_sum[:, :, -1, :]
    blocks = tokens // BLOCK
    state = jnp.zeros((heads, HEAD_WIDTH, HEAD_WIDTH), f32)
    local_prior = []
    opening = []
    log_before = jnp.zeros((heads, HEAD_WIDTH), f32)
    for n in range(blocks):
        local_prior.append(state)
        opening.append(jnp.exp(log_before))
        state = jnp.exp(block_log[:, n])[..., None] * state + block_states[:, n]
        log_before = log_before + block_log[:, n]

    run = jnp.concatenate(
        [
            state.transpose(2, 0, 1).reshape(HEAD_WIDTH, heads * HEAD_WIDTH),
            log_before.reshape(1, -1),
            jnp.zeros((7, heads * HEAD_WIDTH), f32),
        ],
        axis=0,
    )

    def join(earlier, later):
        log_later = later[HEAD_WIDTH : HEAD_WIDTH + 1]
        top = jnp.exp(log_later) * earlier[:HEAD_WIDTH] + later[:HEAD_WIDTH]
        return jnp.concatenate([top, earlier[HEAD_WIDTH:] + later[HEAD_WIDTH:]], axis=0)

    before = None
    for step in (1, 2, 4, 8):
        with jax.named_scope("scan"):
            came = shifted(run, "sp", step, False)
        before = came if before is None else join(came, before)
        run = join(came, run)
    start = starting_state[0].transpose(2, 0, 1).reshape(HEAD_WIDTH, heads * HEAD_WIDTH)
    incoming = jnp.exp(before[HEAD_WIDTH : HEAD_WIDTH + 1]) * start + before[:HEAD_WIDTH]
    incoming = incoming.reshape(HEAD_WIDTH, heads, HEAD_WIDTH).transpose(1, 2, 0)

    rest = late[:, :384]
    got = project_back([jnp.dot(x, rest, preferred_element_type=f32) for x in xs])
    got = (got * inverse).astype(bf16)
    queries, outgate, pool_input = got[:, :128], got[:, 128:256], got[:, 256:]
    previous = shifted(pool_input[tokens - REACH :], "sp", 1, False)

    scaled_query = to_blocks(queries, heads) * HEAD_WIDTH ** (-0.5)
    scores = jnp.einsum(
        "hncd,hnsd->hncs",
        scaled_query * jnp.exp(decay_sum - middle),
        key_blocks * jnp.exp(middle - decay_sum),
        precision=highest,
    )
    causal = jnp.tril(jnp.ones((BLOCK, BLOCK), dtype=bool))
    scores = jnp.where(causal, scores, 0.0)
    within = jnp.einsum("hncs,hnse->hnce", scores, value_blocks, precision=highest)
    prior = jnp.stack(
        [local_prior[n] + opening[n][..., None] * incoming for n in range(blocks)], axis=1
    )
    carried = jnp.einsum(
        "hncd,hnde->hnce", scaled_query * jnp.exp(decay_sum), prior, precision=highest
    )
    merged = within + carried
    merged = merged * lax.rsqrt(jnp.mean(merged * merged, axis=-1, keepdims=True) + norm_eps)
    merged = merged.transpose(1, 2, 0, 3).reshape(tokens, heads * HEAD_WIDTH) * head_norm_gain
    state_out = (merged * jax.nn.silu(outgate.astype(f32))).astype(bf16)

    pool_out = pool_branch(
        pool_input,
        previous,
        pooling_group_weight,
        pooling_channel_scale,
        lax.axis_index("tp"),
        lax.axis_index("sp") * tokens,
    )
    mine = jnp.concatenate([pool_out, state_out], axis=1)
    peers = lax.axis_size("tp")
    spread = lax.all_to_all(jnp.broadcast_to(mine[None], (peers,) + mine.shape), "tp", 0, 0)
    pool_rows = late[:, 384:896].reshape(peers, 128, -1)
    state_rows = late[:, 896:].reshape(peers, 128, -1)
    result = jnp.zeros((tokens, 512), f32)
    for t in range(peers):
        result = result + jnp.dot(spread[t, :, :128], pool_rows[t], preferred_element_type=f32)
        result = result + jnp.dot(spread[t, :, 128:], state_rows[t], preferred_element_type=f32)
    return result.astype(bf16)[None]


def solution(mesh):
    in_specs = (
        P("fs", "sp", None),
        P(),
        P(("sp", "fs"), "tp"),
        P(("sp", "fs"), "tp"),
        P(("sp", "fs"), "tp"),
        P(("sp", "fs"), "tp"),
        P(("sp", "fs"), "tp"),
        P(("sp", "fs"), None),
        P(None, "tp"),
        P("tp"),
        P("tp", "sp"),
        P("tp"),
        P("fs", "tp", None, None),
        P("tp", None, None),
        P("tp"),
        P("sp", "tp"),
        P("sp", "tp"),
    )
    out_specs = P("fs", "sp", "tp")
    return jax.shard_map(body, mesh=mesh, in_specs=in_specs, out_specs=out_specs, check_vma=False)
```

```python
import jax
import jax.numpy as jnp
from jax import lax
from jax.experimental import pallas as pl
from jax.experimental.pallas import tpu as pltpu
from jax.sharding import PartitionSpec as P

BLOCK = 64
HEAD = 64
LANES = 128
HALO = 16
RUN_ROWS = 72
norm_eps = 1e-06
decay_temper = 16.0
highest = lax.Precision.HIGHEST
f32 = jnp.float32
bf16 = jnp.bfloat16


def shifted(x, axis, by, wrap):
    n = lax.axis_size(axis)
    if wrap:
        pairs = [(i, (i + by) % n) for i in range(n)]
    else:
        pairs = [(i, i + by) for i in range(n) if 0 <= i + by < n]
    return lax.ppermute(x, axis, pairs)


def call(kernel, outs, name, *args, scalars=1):
    smem = pl.BlockSpec(memory_space=pltpu.SMEM)
    vmem = pl.BlockSpec(memory_space=pltpu.VMEM)
    return pl.pallas_call(
        kernel,
        in_specs=[smem] * scalars + [vmem] * (len(args) - scalars),
        out_specs=[vmem] * len(outs),
        out_shape=outs,
        name=name,
    )(*args)


def struct(shape, dtype):
    return jax.ShapeDtypeStruct(shape, dtype)


def pack_kernel(key, value, pool, low, query, gate, pool_rows, state_rows, early, late):
    for out, refs in ((early, (key, value, pool, low)), (late, (query, gate, pool_rows, state_rows))):
        at = 0
        for r in refs:
            out[:, at : at + r.shape[1]] = r[...]
            at += r.shape[1]


def prep_kernel(own, act, gain, x0, x1, x2, x3, inverse):
    rows, width = act.shape
    outs = (x0, x1, x2, x3)
    half = lax.broadcasted_iota(jnp.int32, (rows, LANES), 1) < HEAD

    for f in range(4):

        @pl.when(own[0] == f)
        def _(f=f):
            squares = jnp.zeros((rows, LANES), f32)
            for p in range(width // 512):
                tiles = []
                for q in range(4):
                    at = p * 512 + q * LANES
                    t = act[:, at : at + LANES].astype(f32)
                    squares = squares + t * t
                    tiles.append(t * gain[:, at : at + LANES])
                blocks = []
                for a, b in ((tiles[0], tiles[2]), (tiles[1], tiles[3])):
                    blocks.append(jnp.where(half, a, pltpu.roll(b, HEAD, 1)).astype(bf16))
                    blocks.append(jnp.where(half, pltpu.roll(a, HEAD, 1), b).astype(bf16))
                for k in range(4):
                    outs[k][:, p * LANES : (p + 1) * LANES] = blocks[(f + k) % 4]
            total = jnp.sum(squares, axis=1, keepdims=True)
            inverse[...] = jnp.broadcast_to(lax.rsqrt(total / width + norm_eps), (rows, LANES))


def prepare(act, gain, own):
    tokens, width = act.shape
    rows = 64
    part = pl.BlockSpec((rows, width // 4), lambda i, own: (i, 0))
    return pl.pallas_call(
        prep_kernel,
        grid_spec=pltpu.PrefetchScalarGridSpec(
            num_scalar_prefetch=1,
            grid=(tokens // rows,),
            in_specs=[
                pl.BlockSpec((rows, width), lambda i, own: (i, 0)),
                pl.BlockSpec((1, width), lambda i, own: (0, 0)),
            ],
            out_specs=[part, part, part, part, pl.BlockSpec((rows, LANES), lambda i, own: (i, 0))],
        ),
        out_shape=[struct((tokens, width // 4), bf16)] * 4 + [struct((tokens, LANES), f32)],
        name="prep",
    )(own, act, gain)


def partial_kernel(own, x0, x1, x2, x3, w, out):
    tokens = x0.shape[0]
    wide = out.shape[1] // tokens * LANES
    columns = out.shape[1] * LANES // tokens
    half = lax.broadcasted_iota(jnp.int32, (tokens // 2, LANES), 1) < HEAD
    weight = w[:, :columns]
    for k, x in enumerate((x0, x1, x2, x3)):
        target = (own[0] - k + 4) % 4
        p = jnp.dot(x[...], weight, preferred_element_type=f32)
        for j in range(wide // LANES):
            out[target, j * tokens : (j + 1) * tokens] = p[:, j * LANES : (j + 1) * LANES].astype(bf16)
        if columns > wide:
            d = jnp.concatenate([p[:, wide:], p[:, wide:]], axis=1)
            d = jnp.where(half, d[: tokens // 2], d[tokens // 2 :])
            out[target, wide // LANES * tokens :] = d.astype(bf16)


def partials(own, xs, w, columns, name):
    tokens, _ = xs[0].shape
    (out,) = call(
        partial_kernel,
        [struct((4, tokens * columns // LANES, LANES), bf16)],
        name,
        own,
        *xs,
        w,
    )
    return out


def total_of(parts, at, rows):
    s = parts[0, at : at + rows].astype(f32)
    for k in (1, 2, 3):
        s = s + parts[k, at : at + rows].astype(f32)
    return s


def projected(parts, inverse, j):
    tokens = inverse.shape[0]
    return (total_of(parts, j * tokens, tokens) * inverse).astype(bf16)


def heads_of(x, half):
    return jnp.where(half, x[:HEAD], x[HEAD:])


def local_kernel(
    parts, inverse, second, bias, extra, keys, values, pool, tail, sums, prior, opening, run
):
    inv = inverse[...]
    tokens = inv.shape[0]
    keys[...] = projected(parts, inv, 0).astype(f32)
    values[...] = projected(parts, inv, 1).astype(f32)
    pooled = projected(parts, inv, 2)
    pool[...] = pooled
    tail[...] = pooled[tokens - HALO :]
    both = total_of(parts, 3 * tokens, tokens // 2)
    low = jnp.concatenate([both[:, :HEAD], both[:, HEAD:]], axis=0)
    low = (low * inv[:, :HEAD]).astype(bf16)
    x = jnp.dot(low, second[...], preferred_element_type=f32) + bias[...]
    rates = (jnp.minimum(x, 0.0) - jnp.log1p(jnp.exp(-jnp.abs(x)))) / decay_temper
    wide = lax.broadcasted_iota(jnp.int32, (2, LANES), 1) // HEAD
    pick = (wide == lax.broadcasted_iota(jnp.int32, (2, LANES), 0)).astype(f32)
    rates = rates + lax.dot_general(
        extra[...], pick, (((0,), (0,)), ((), ())), precision=highest, preferred_element_type=f32
    )
    r = lax.broadcasted_iota(jnp.int32, (BLOCK, BLOCK), 0)
    c = lax.broadcasted_iota(jnp.int32, (BLOCK, BLOCK), 1)
    lower = (r >= c).astype(f32)
    half = lax.broadcasted_iota(jnp.int32, (HEAD, LANES), 1) < HEAD
    state = jnp.zeros((HEAD, LANES), f32)
    before = jnp.zeros((1, LANES), f32)
    for n in range(tokens // BLOCK):
        at = slice(n * BLOCK, (n + 1) * BLOCK)
        total = jnp.dot(lower, rates[at], precision=highest, preferred_element_type=f32)
        sums[at] = total
        final = total[BLOCK - 1 :]
        pairs = lax.dot_general(
            values[at],
            keys[at] * jnp.exp(final - total),
            (((0,), (0,)), ((), ())),
            precision=highest,
            preferred_element_type=f32,
        )
        prior[at] = state
        opening[n : n + 1] = before
        state = jnp.exp(final) * state + heads_of(pairs, half)
        before = before + final
    run[:HEAD] = state
    run[HEAD:] = jnp.broadcast_to(before, (RUN_ROWS - HEAD, LANES))


def finish_kernel(
    where,
    runs,
    start,
    parts,
    inverse,
    keys,
    values,
    sums,
    prior,
    opening,
    gain,
    pool,
    previous,
    pool_weight,
    pool_scale,
    mine,
):
    inv = inverse[...]
    tokens = inv.shape[0]
    place = where[0]
    state = start[...]
    for j in range(runs.shape[0] // RUN_ROWS):
        at = j * RUN_ROWS
        log = runs[at + HEAD : at + HEAD + 1]
        folded = jnp.exp(log) * state + runs[at : at + HEAD]
        state = jnp.where(j < place, folded, state)
    queries = projected(parts, inv, 0).astype(f32) * HEAD ** (-0.5)
    outgate = projected(parts, inv, 1).astype(f32)
    half = lax.broadcasted_iota(jnp.int32, (HEAD, LANES), 1) < HEAD
    r = lax.broadcasted_iota(jnp.int32, (2 * BLOCK, BLOCK), 0) % BLOCK
    c = lax.broadcasted_iota(jnp.int32, (2 * BLOCK, BLOCK), 1)
    causal = r >= c

    def split(x):
        return jnp.concatenate([jnp.where(half, x, 0.0), jnp.where(half, 0.0, x)], axis=0)

    last = (((1,), (1,)), ((), ()))
    for n in range(tokens // BLOCK):
        at = slice(n * BLOCK, (n + 1) * BLOCK)
        total = sums[at]
        middle = total[BLOCK // 2 - 1 : BLOCK // 2]
        q = queries[at]
        scores = lax.dot_general(
            split(q * jnp.exp(total - middle)),
            keys[at] * jnp.exp(middle - total),
            last,
            precision=highest,
            preferred_element_type=f32,
        )
        scores = jnp.where(causal, scores, 0.0)
        within = jnp.dot(scores, values[at], precision=highest, preferred_element_type=f32)
        begin = prior[at] + jnp.exp(opening[n : n + 1]) * state
        carried = lax.dot_general(
            split(q * jnp.exp(total)),
            jnp.concatenate([begin, begin], axis=0),
            last,
            precision=highest,
            preferred_element_type=f32,
        )
        raw = heads_of(within + carried, half)
        square = raw * raw
        first = jnp.sum(jnp.where(half, square, 0.0), axis=1, keepdims=True)
        second = jnp.sum(jnp.where(half, 0.0, square), axis=1, keepdims=True)
        mean = jnp.where(half, first, second) / HEAD
        g = outgate[at]
        scaled = raw * lax.rsqrt(mean + norm_eps) * gain[...]
        mine[at, LANES:] = (scaled * (g / (1.0 + jnp.exp(-g)))).astype(bf16)

    current = pool[...].astype(f32)
    extended = jnp.concatenate([previous[...].astype(f32), current], axis=0)

    def back(x, by):
        return x + pltpu.roll(x, by, 0)

    two = back(extended, 1)
    four = back(two, 2)
    eight = back(four, 4)
    sixteen = back(eight, 8)
    level = where[1] % 4
    chosen = jnp.where(
        level == 0, two, jnp.where(level == 1, four, jnp.where(level == 2, eight, sixteen))
    )[HALO:]
    window = jnp.where(
        level == 0, 2.0, jnp.where(level == 1, 4.0, jnp.where(level == 2, 8.0, 16.0))
    )
    position = place * tokens + lax.broadcasted_iota(jnp.int32, (tokens, LANES), 0)
    counts = jnp.minimum(position.astype(f32) + 1.0, window)
    deviation = (chosen / counts - current).astype(bf16)
    mixture = jnp.dot(deviation, pool_weight[...], preferred_element_type=f32)
    mine[:, :LANES] = (mixture * pool_scale[...]).astype(bf16)


def output_kernel(core, same, other, late, out):
    first = 2 * LANES
    width = out.shape[1]
    total = jnp.zeros(out.shape, f32)
    for x in range(same.shape[0]):
        for z, c in ((same, core[0]), (other, 1 - core[0])):
            rows = pl.ds((2 * x + c) * LANES, LANES)
            total = total + jnp.dot(
                z[x, :, :LANES], late[rows, first : first + width], preferred_element_type=f32
            )
            total = total + jnp.dot(
                z[x, :, LANES:], late[rows, first + width :], preferred_element_type=f32
            )
    out[...] = total.astype(bf16)


def body(
    activations,
    input_norm_gain,
    pooling_channel_weight,
    query_projection_weight,
    key_projection_weight,
    value_projection_weight,
    output_gate_weight,
    decay_first_factor,
    decay_second_factor,
    decay_gate_bias,
    decay_extra_log,
    head_norm_gain,
    starting_state,
    pooling_group_weight,
    pooling_channel_scale,
    pooling_output_rows,
    attention_output_rows,
):
    _, tokens, width = activations.shape
    rows = key_projection_weight.shape[0]
    columns = pooling_output_rows.shape[1]
    own = lax.axis_index("fs").astype(jnp.int32).reshape(1)
    tp = lax.axis_index("tp").astype(jnp.int32)
    early, late = call(
        pack_kernel,
        [struct((rows, 3 * LANES + HEAD), bf16), struct((rows, 2 * LANES + 2 * columns), bf16)],
        "pack",
        key_projection_weight,
        value_projection_weight,
        pooling_channel_weight,
        decay_first_factor,
        query_projection_weight,
        output_gate_weight,
        pooling_output_rows,
        attention_output_rows,
        scalars=0,
    )
    late = lax.all_gather(late, "sp", axis=0, tiled=True)
    x0, x1, x2, x3, inverse = prepare(
        activations.reshape(tokens, width), input_norm_gain.reshape(1, width), own
    )
    with jax.named_scope("early"):
        early = lax.all_gather(early, "sp", axis=0, tiled=True)
    with jax.named_scope("exchange"):
        x1 = shifted(x1, "fs", 1, True)
        x2 = shifted(x2, "fs", 2, True)
        x3 = shifted(x3, "fs", 3, True)
    xs = (x0, x1, x2, x3)
    parts = partials(own, xs, early, early.shape[1], "early_parts")
    parts = lax.all_to_all(parts, "fs", 0, 0)
    wide = struct((tokens, LANES), f32)
    keys, values, pool, tail, sums, prior, opening, run = call(
        local_kernel,
        [
            wide,
            wide,
            struct((tokens, LANES), bf16),
            struct((HALO, LANES), bf16),
            wide,
            wide,
            struct((tokens // BLOCK, LANES), f32),
            struct((RUN_ROWS, LANES), f32),
        ],
        "local",
        parts,
        inverse,
        decay_second_factor,
        decay_gate_bias.reshape(1, LANES),
        decay_extra_log,
        scalars=0,
    )
    with jax.named_scope("halo"):
        previous = shifted(tail, "sp", 1, False)
    with jax.named_scope("states"):
        runs = lax.all_gather(run, "sp", axis=0, tiled=True)
    start = starting_state[0].transpose(2, 0, 1).reshape(HEAD, LANES)
    late, runs = lax.optimization_barrier((late, runs))
    parts = partials(own, xs, late, 2 * LANES, "late_parts")
    parts = lax.all_to_all(parts, "fs", 0, 0)
    (mine,) = call(
        finish_kernel,
        [struct((tokens, 2 * LANES), bf16)],
        "finish",
        jnp.stack([lax.axis_index("sp").astype(jnp.int32), tp]),
        runs,
        start,
        parts,
        inverse,
        keys,
        values,
        sums,
        prior,
        opening,
        head_norm_gain.reshape(1, LANES),
        pool,
        previous,
        pooling_group_weight[0],
        pooling_channel_scale.reshape(1, LANES),
    )
    peers = lax.axis_size("tp")
    groups = [[c + 2 * x for x in range(peers // 2)] for c in range(2)]
    same = lax.all_to_all(
        jnp.broadcast_to(mine[None], (peers // 2,) + mine.shape), "tp", 0, 0, axis_index_groups=groups
    )
    other = lax.ppermute(same, "tp", [(i, i ^ 1) for i in range(peers)])
    (result,) = call(
        output_kernel,
        [struct((tokens, columns), bf16)],
        "output",
        (tp % 2).reshape(1),
        same,
        other,
        late,
    )
    return result[None]


def solution(mesh):
    in_specs = (
        P("fs", "sp", None),
        P(),
        P(("sp", "fs"), "tp"),
        P(("sp", "fs"), "tp"),
        P(("sp", "fs"), "tp"),
        P(("sp", "fs"), "tp"),
        P(("sp", "fs"), "tp"),
        P(("sp", "fs"), None),
        P(None, "tp"),
        P("tp"),
        P("tp", "sp"),
        P("tp"),
        P("fs", "tp", None, None),
        P("tp", None, None),
        P("tp"),
        P("sp", "tp"),
        P("sp", "tp"),
    )
    out_specs = P("fs", "sp", "tp")
    return jax.shard_map(body, mesh=mesh, in_specs=in_specs, out_specs=out_specs, check_vma=False)
```

```python
import jax
import jax.numpy as jnp
from jax import lax
from jax.experimental import pallas as pl
from jax.experimental.pallas import tpu as pltpu
from jax.sharding import PartitionSpec as P

BLOCK = 64
HEAD = 64
LANES = 128
HALO = 16
RUN_ROWS = 72
norm_eps = 1e-06
decay_temper = 16.0
highest = lax.Precision.HIGHEST
f32 = jnp.float32
bf16 = jnp.bfloat16


def shifted(x, axis, by, wrap):
    n = lax.axis_size(axis)
    if wrap:
        pairs = [(i, (i + by) % n) for i in range(n)]
    else:
        pairs = [(i, i + by) for i in range(n) if 0 <= i + by < n]
    return lax.ppermute(x, axis, pairs)


def call(kernel, outs, name, *args, scalars=1):
    smem = pl.BlockSpec(memory_space=pltpu.SMEM)
    vmem = pl.BlockSpec(memory_space=pltpu.VMEM)
    return pl.pallas_call(
        kernel,
        in_specs=[smem] * scalars + [vmem] * (len(args) - scalars),
        out_specs=[vmem] * len(outs),
        out_shape=outs,
        name=name,
    )(*args)


def near(x):
    return pltpu.with_memory_space_constraint(x, pltpu.VMEM)


def struct(shape, dtype):
    return jax.ShapeDtypeStruct(shape, dtype)


def pack_kernel(
    own, key, value, pool, low, query, gate, pool_rows, state_rows, early, late
):
    at = 0
    for r in (key, value, pool, low):
        early[:, at : at + r.shape[1]] = r[...]
        at += r.shape[1]
    mine = pl.ds(pl.multiple_of(own[0] * LANES, LANES), LANES)
    for j, block in enumerate(
        (query[...], gate[...], pool_rows[:, mine], state_rows[:, mine])
    ):
        late[:, j * LANES : (j + 1) * LANES] = block


def prep_kernel(own, act, gain, x0, x1, x2, x3, inverse):
    rows, width = act.shape
    outs = (x0, x1, x2, x3)
    half = lax.broadcasted_iota(jnp.int32, (rows, LANES), 1) < HEAD

    for f in range(4):

        @pl.when(own[0] == f)
        def _(f=f):
            squares = jnp.zeros((rows, LANES), f32)
            for p in range(width // 512):
                tiles = []
                for q in range(4):
                    at = p * 512 + q * LANES
                    t = act[:, at : at + LANES].astype(f32)
                    squares = squares + t * t
                    tiles.append(t * gain[:, at : at + LANES])
                blocks = []
                for a, b in ((tiles[0], tiles[2]), (tiles[1], tiles[3])):
                    blocks.append(jnp.where(half, a, pltpu.roll(b, HEAD, 1)).astype(bf16))
                    blocks.append(jnp.where(half, pltpu.roll(a, HEAD, 1), b).astype(bf16))
                for k in range(4):
                    outs[k][:, p * LANES : (p + 1) * LANES] = blocks[(f + k) % 4]
            total = jnp.sum(squares, axis=1, keepdims=True)
            inverse[...] = jnp.broadcast_to(lax.rsqrt(total / width + norm_eps), (rows, LANES))


def prepare(act, gain, own):
    tokens, width = act.shape
    rows = 64
    part = pl.BlockSpec((rows, width // 4), lambda i, own: (i, 0))
    return pl.pallas_call(
        prep_kernel,
        grid_spec=pltpu.PrefetchScalarGridSpec(
            num_scalar_prefetch=1,
            grid=(tokens // rows,),
            in_specs=[
                pl.BlockSpec((rows, width), lambda i, own: (i, 0)),
                pl.BlockSpec((1, width), lambda i, own: (0, 0)),
            ],
            out_specs=[part, part, part, part, pl.BlockSpec((rows, LANES), lambda i, own: (i, 0))],
        ),
        out_shape=[struct((tokens, width // 4), bf16)] * 4 + [struct((tokens, LANES), f32)],
        name="prep",
    )(own, act, gain)


def partial_kernel(own, x0, x1, x2, x3, w, out, *rest):
    *rest, held, arrived = rest
    copies = []
    for k, x in enumerate((x0, x1, x2, x3)):
        copies.append(pltpu.make_async_copy(x, held.at[k], arrived.at[k]))
        copies[k].start()
    tokens = x0.shape[0]
    wide = out.shape[1] // tokens * LANES
    columns = out.shape[1] * LANES // tokens
    half = lax.broadcasted_iota(jnp.int32, (tokens // 2, LANES), 1) < HEAD
    weight = w[:, :columns]
    for k in range(4):
        target = (own[0] - k + 4) % 4
        copies[k].wait()
        p = jnp.dot(held[k], weight, preferred_element_type=f32)
        for j in range(wide // LANES):
            out[target, j * tokens : (j + 1) * tokens] = p[:, j * LANES : (j + 1) * LANES].astype(bf16)
        if columns > wide:
            d = jnp.concatenate([p[:, wide:], p[:, wide:]], axis=1)
            d = jnp.where(half, d[: tokens // 2], d[tokens // 2 :])
            out[target, wide // LANES * tokens :] = d.astype(bf16)
    for r in rest:
        r[...] = w[:, columns:]


def partials(own, xs, w, columns, name):
    tokens, _ = xs[0].shape
    outs = [struct((4, tokens * columns // LANES, LANES), bf16)]
    if w.shape[1] > columns:
        outs.append(struct((w.shape[0], w.shape[1] - columns), bf16))
    anywhere = pl.BlockSpec(memory_space=pl.ANY)
    vmem = pl.BlockSpec(memory_space=pltpu.VMEM)
    return pl.pallas_call(
        partial_kernel,
        in_specs=[pl.BlockSpec(memory_space=pltpu.SMEM)] + [anywhere] * 4 + [vmem],
        out_specs=[vmem] * len(outs),
        out_shape=outs,
        scratch_shapes=[pltpu.VMEM((4,) + xs[0].shape, bf16), pltpu.SemaphoreType.DMA((4,))],
        name=name,
    )(own, *xs, w)


def total_of(parts, at, rows):
    s = parts[0, at : at + rows].astype(f32)
    for k in (1, 2, 3):
        s = s + parts[k, at : at + rows].astype(f32)
    return s


def projected(parts, inverse, j):
    tokens = inverse.shape[0]
    return (total_of(parts, j * tokens, tokens) * inverse).astype(bf16)


def heads_of(x, half):
    return jnp.where(half, x[:HEAD], x[HEAD:])


def local_kernel(
    parts, inverse, second, bias, extra, keys, values, pool, tail, sums, prior, opening, run
):
    inv = inverse[...]
    tokens = inv.shape[0]
    keys[...] = projected(parts, inv, 0).astype(f32)
    values[...] = projected(parts, inv, 1).astype(f32)
    pooled = projected(parts, inv, 2)
    pool[...] = pooled
    tail[...] = pooled[tokens - HALO :]
    both = total_of(parts, 3 * tokens, tokens // 2)
    low = jnp.concatenate([both[:, :HEAD], both[:, HEAD:]], axis=0)
    low = (low * inv[:, :HEAD]).astype(bf16)
    x = jnp.dot(low, second[...], preferred_element_type=f32) + bias[...]
    rates = (jnp.minimum(x, 0.0) - jnp.log1p(jnp.exp(-jnp.abs(x)))) / decay_temper
    wide = lax.broadcasted_iota(jnp.int32, (2, LANES), 1) // HEAD
    pick = (wide == lax.broadcasted_iota(jnp.int32, (2, LANES), 0)).astype(f32)
    rates = rates + lax.dot_general(
        extra[...], pick, (((0,), (0,)), ((), ())), precision=highest, preferred_element_type=f32
    )
    r = lax.broadcasted_iota(jnp.int32, (BLOCK, BLOCK), 0)
    c = lax.broadcasted_iota(jnp.int32, (BLOCK, BLOCK), 1)
    lower = (r >= c).astype(f32)
    half = lax.broadcasted_iota(jnp.int32, (HEAD, LANES), 1) < HEAD
    state = jnp.zeros((HEAD, LANES), f32)
    before = jnp.zeros((1, LANES), f32)
    for n in range(tokens // BLOCK):
        at = slice(n * BLOCK, (n + 1) * BLOCK)
        total = jnp.dot(lower, rates[at], precision=highest, preferred_element_type=f32)
        sums[at] = total
        final = total[BLOCK - 1 :]
        pairs = lax.dot_general(
            values[at],
            keys[at] * jnp.exp(final - total),
            (((0,), (0,)), ((), ())),
            precision=highest,
            preferred_element_type=f32,
        )
        prior[at] = state
        opening[n : n + 1] = before
        state = jnp.exp(final) * state + heads_of(pairs, half)
        before = before + final
    run[:HEAD] = state
    run[HEAD:] = jnp.broadcast_to(before, (RUN_ROWS - HEAD, LANES))


def finish_kernel(
    where,
    runs,
    start,
    parts,
    inverse,
    keys,
    values,
    sums,
    prior,
    opening,
    gain,
    pool,
    previous,
    pool_weight,
    pool_scale,
    mine,
):
    inv = inverse[...]
    tokens = inv.shape[0]
    place = where[0]
    state = start[...]
    for j in range(runs.shape[0] // RUN_ROWS):
        at = j * RUN_ROWS
        log = runs[at + HEAD : at + HEAD + 1]
        folded = jnp.exp(log) * state + runs[at : at + HEAD]
        state = jnp.where(j < place, folded, state)
    queries = projected(parts, inv, 0).astype(f32) * HEAD ** (-0.5)
    outgate = projected(parts, inv, 1).astype(f32)
    half = lax.broadcasted_iota(jnp.int32, (HEAD, LANES), 1) < HEAD
    r = lax.broadcasted_iota(jnp.int32, (2 * BLOCK, BLOCK), 0) % BLOCK
    c = lax.broadcasted_iota(jnp.int32, (2 * BLOCK, BLOCK), 1)
    causal = r >= c

    def split(x):
        return jnp.concatenate([jnp.where(half, x, 0.0), jnp.where(half, 0.0, x)], axis=0)

    last = (((1,), (1,)), ((), ()))
    for n in range(tokens // BLOCK):
        at = slice(n * BLOCK, (n + 1) * BLOCK)
        total = sums[at]
        middle = total[BLOCK // 2 - 1 : BLOCK // 2]
        q = queries[at]
        scores = lax.dot_general(
            split(q * jnp.exp(total - middle)),
            keys[at] * jnp.exp(middle - total),
            last,
            precision=highest,
            preferred_element_type=f32,
        )
        scores = jnp.where(causal, scores, 0.0)
        within = jnp.dot(scores, values[at], precision=highest, preferred_element_type=f32)
        begin = prior[at] + jnp.exp(opening[n : n + 1]) * state
        carried = lax.dot_general(
            split(q * jnp.exp(total)),
            jnp.concatenate([begin, begin], axis=0),
            last,
            precision=highest,
            preferred_element_type=f32,
        )
        raw = heads_of(within + carried, half)
        square = raw * raw
        first = jnp.sum(jnp.where(half, square, 0.0), axis=1, keepdims=True)
        second = jnp.sum(jnp.where(half, 0.0, square), axis=1, keepdims=True)
        mean = jnp.where(half, first, second) / HEAD
        g = outgate[at]
        scaled = raw * lax.rsqrt(mean + norm_eps) * gain[...]
        mine[at, LANES:] = (scaled * (g / (1.0 + jnp.exp(-g)))).astype(bf16)

    current = pool[...].astype(f32)
    extended = jnp.concatenate([previous[...].astype(f32), current], axis=0)

    def back(x, by):
        return x + pltpu.roll(x, by, 0)

    two = back(extended, 1)
    four = back(two, 2)
    eight = back(four, 4)
    sixteen = back(eight, 8)
    level = where[1] % 4
    chosen = jnp.where(
        level == 0, two, jnp.where(level == 1, four, jnp.where(level == 2, eight, sixteen))
    )[HALO:]
    window = jnp.where(
        level == 0, 2.0, jnp.where(level == 1, 4.0, jnp.where(level == 2, 8.0, 16.0))
    )
    position = place * tokens + lax.broadcasted_iota(jnp.int32, (tokens, LANES), 0)
    counts = jnp.minimum(position.astype(f32) + 1.0, window)
    deviation = (chosen / counts - current).astype(bf16)
    mixture = jnp.dot(deviation, pool_weight[...], preferred_element_type=f32)
    mine[:, :LANES] = (mixture * pool_scale[...]).astype(bf16)


def output_kernel(core, same, other, rows, out):
    total = jnp.zeros(out.shape, f32)
    for x in range(same.shape[0]):
        for z, c in ((same, core[0]), (other, 1 - core[0])):
            at = pl.ds(pl.multiple_of((2 * x + c) * LANES, LANES), LANES)
            w = jnp.concatenate(
                [
                    jnp.concatenate([rows[f, at, :LANES], rows[f, at, LANES:]], axis=0)
                    for f in range(rows.shape[0])
                ],
                axis=1,
            )
            total = total + jnp.dot(z[x], w, preferred_element_type=f32)
    out[...] = total.astype(bf16)


def body(
    activations,
    input_norm_gain,
    pooling_channel_weight,
    query_projection_weight,
    key_projection_weight,
    value_projection_weight,
    output_gate_weight,
    decay_first_factor,
    decay_second_factor,
    decay_gate_bias,
    decay_extra_log,
    head_norm_gain,
    starting_state,
    pooling_group_weight,
    pooling_channel_scale,
    pooling_output_rows,
    attention_output_rows,
):
    _, tokens, width = activations.shape
    rows = key_projection_weight.shape[0]
    columns = pooling_output_rows.shape[1]
    own = lax.axis_index("fs").astype(jnp.int32).reshape(1)
    tp = lax.axis_index("tp").astype(jnp.int32)
    early, late = call(
        pack_kernel,
        [struct((rows, 3 * LANES + HEAD), bf16), struct((rows, 4 * LANES), bf16)],
        "pack",
        own,
        key_projection_weight,
        value_projection_weight,
        pooling_channel_weight,
        decay_first_factor,
        query_projection_weight,
        output_gate_weight,
        pooling_output_rows,
        attention_output_rows,
    )
    late = lax.all_gather(late, "sp", axis=0, tiled=True)
    x0, x1, x2, x3, inverse = prepare(
        activations.reshape(tokens, width), input_norm_gain.reshape(1, width), own
    )
    with jax.named_scope("early"):
        early = lax.all_gather(early, "sp", axis=0, tiled=True)
    with jax.named_scope("exchange"):
        x1 = shifted(x1, "fs", 1, True)
        x2 = shifted(x2, "fs", 2, True)
        x3 = shifted(x3, "fs", 3, True)
    xs = (x0, x1, x2, x3)
    inverse = near(inverse)
    (parts,) = partials(own, xs, near(early), early.shape[1], "early_parts")
    parts = near(lax.all_to_all(parts, "fs", 0, 0))
    wide = pltpu.VMEM((tokens, LANES), f32)
    keys, values, pool, tail, sums, prior, opening, run = call(
        local_kernel,
        [
            wide,
            wide,
            pltpu.VMEM((tokens, LANES), bf16),
            struct((HALO, LANES), bf16),
            wide,
            wide,
            pltpu.VMEM((tokens // BLOCK, LANES), f32),
            struct((RUN_ROWS, LANES), f32),
        ],
        "local",
        parts,
        inverse,
        decay_second_factor,
        decay_gate_bias.reshape(1, LANES),
        decay_extra_log,
        scalars=0,
    )
    with jax.named_scope("halo"):
        previous = shifted(tail, "sp", 1, False)
    start = starting_state[0].transpose(2, 0, 1).reshape(HEAD, LANES)
    late, run = lax.optimization_barrier((late, run))
    late_parts, quarter = partials(own, xs, late, 2 * LANES, "late_parts")
    late_parts, quarter, run = lax.optimization_barrier((late_parts, quarter, run))
    with jax.named_scope("rows"):
        out_rows = lax.all_gather(quarter, "fs")
    with jax.named_scope("late_back"):
        late_parts = lax.all_to_all(late_parts, "fs", 0, 0)
    with jax.named_scope("states"):
        runs = lax.all_gather(run, "sp", axis=0, tiled=True)
    (mine,) = call(
        finish_kernel,
        [struct((tokens, 2 * LANES), bf16)],
        "finish",
        jnp.stack([lax.axis_index("sp").astype(jnp.int32), tp]),
        near(runs),
        near(start),
        near(late_parts),
        inverse,
        near(keys),
        near(values),
        near(sums),
        near(prior),
        near(opening),
        head_norm_gain.reshape(1, LANES),
        near(pool),
        near(previous),
        pooling_group_weight[0],
        pooling_channel_scale.reshape(1, LANES),
    )
    peers = lax.axis_size("tp")
    groups = [[c + 2 * x for x in range(peers // 2)] for c in range(2)]
    same = lax.all_to_all(
        jnp.broadcast_to(mine[None], (peers // 2,) + mine.shape), "tp", 0, 0, axis_index_groups=groups
    )
    other = lax.ppermute(same, "tp", [(i, i ^ 1) for i in range(peers)])
    (result,) = call(
        output_kernel,
        [struct((tokens, columns), bf16)],
        "output",
        (tp % 2).reshape(1),
        near(same),
        near(other),
        near(out_rows),
    )
    return result[None]


def solution(mesh):
    in_specs = (
        P("fs", "sp", None),
        P(),
        P(("sp", "fs"), "tp"),
        P(("sp", "fs"), "tp"),
        P(("sp", "fs"), "tp"),
        P(("sp", "fs"), "tp"),
        P(("sp", "fs"), "tp"),
        P(("sp", "fs"), None),
        P(None, "tp"),
        P("tp"),
        P("tp", "sp"),
        P("tp"),
        P("fs", "tp", None, None),
        P("tp", None, None),
        P("tp"),
        P("sp", "tp"),
        P("sp", "tp"),
    )
    out_specs = P("fs", "sp", "tp")
    return jax.shard_map(body, mesh=mesh, in_specs=in_specs, out_specs=out_specs, check_vma=False)
```

```python
import jax
import jax.numpy as jnp
from jax import lax
from jax.experimental import pallas as pl
from jax.experimental.pallas import tpu as pltpu
from jax.sharding import PartitionSpec as P


BLOCK = 64
HEAD = 64
LANES = 128
HALO = 16
RUN_ROWS = 80
norm_eps = 1e-06
decay_temper = 16.0
highest = lax.Precision.HIGHEST
f32 = jnp.float32
bf16 = jnp.bfloat16
limit = pltpu.CompilerParams(vmem_limit_bytes=24 << 20)


def shifted(x, axis, by, wrap):
    n = lax.axis_size(axis)
    if wrap:
        pairs = [(i, (i + by) % n) for i in range(n)]
    else:
        pairs = [(i, i + by) for i in range(n) if 0 <= i + by < n]
    return lax.ppermute(x, axis, pairs)


def call(kernel, outs, name, *args, scalars=1, aliases={}):
    smem = pl.BlockSpec(memory_space=pltpu.SMEM)
    vmem = pl.BlockSpec(memory_space=pltpu.VMEM)
    return pl.pallas_call(
        kernel,
        in_specs=[smem] * scalars + [vmem] * (len(args) - scalars),
        out_specs=[vmem] * len(outs),
        out_shape=outs,
        input_output_aliases=aliases,
        compiler_params=limit if name == "local" else None,
    )(*args)


def near(x):
    return pltpu.with_memory_space_constraint(x, pltpu.VMEM)


def struct(shape, dtype):
    return jax.ShapeDtypeStruct(shape, dtype)


def pack_kernel(
    own, key, value, pool, low, query, gate, pool_rows, state_rows, early, late
):
    at = 0
    for r in (key, value, pool, low):
        early[:, at : at + r.shape[1]] = r[...]
        at += r.shape[1]
    mine = pl.ds(pl.multiple_of(own[0] * LANES, LANES), LANES)
    for j, block in enumerate(
        (query[...], gate[...], pool_rows[:, mine], state_rows[:, mine])
    ):
        late[:, j * LANES : (j + 1) * LANES] = block


def prep_kernel(act, gain, x, inverse, held, arrived):
    tokens, width = act.shape
    rows = tokens // 4
    copies = []
    for c in range(4):
        at = pl.ds(c * rows, rows)
        copies.append(pltpu.make_async_copy(act.at[at], held.at[at], arrived.at[c]))
        copies[c].start()
    half = lax.broadcasted_iota(jnp.int32, (rows, LANES), 1) < HEAD
    for c in range(4):
        copies[c].wait()
        block = pl.ds(c * rows, rows)
        squares = jnp.zeros((rows, LANES), f32)
        for p in range(width // 512):
            tiles = []
            for q in range(4):
                at = p * 512 + q * LANES
                t = held[block, at : at + LANES].astype(f32)
                squares = squares + t * t
                tiles.append(t * gain[:, at : at + LANES])
            to = slice(p * LANES, (p + 1) * LANES)
            for j, (a, b) in enumerate(((tiles[0], tiles[2]), (tiles[1], tiles[3]))):
                x[2 * j, block, to] = jnp.where(half, a, pltpu.roll(b, HEAD, 1)).astype(bf16)
                x[2 * j + 1, block, to] = jnp.where(half, pltpu.roll(a, HEAD, 1), b).astype(bf16)
        total = jnp.sum(squares, axis=1, keepdims=True)
        inverse[block] = jnp.broadcast_to(lax.rsqrt(total / width + norm_eps), (rows, LANES))


def prepare(act, gain):
    tokens, width = act.shape
    vmem = pl.BlockSpec(memory_space=pltpu.VMEM)
    return pl.pallas_call(
        prep_kernel,
        in_specs=[pl.BlockSpec(memory_space=pl.ANY), vmem],
        out_specs=[vmem, vmem],
        out_shape=[struct((4, tokens, width // 4), bf16), struct((tokens, LANES), f32)],
        scratch_shapes=[pltpu.VMEM((tokens, width), bf16), pltpu.SemaphoreType.DMA((4,))],
        name="prep",
    )(act, gain)


def thirds(x):
    first = x.astype(bf16)
    left = x - first.astype(f32)
    second = left.astype(bf16)
    return first, second, (left - second.astype(f32)).astype(bf16)


def early_kernel(x, w, out, same_x, made, left):
    tokens = x.shape[1]
    half = lax.broadcasted_iota(jnp.int32, (tokens // 2, LANES), 1) < HEAD
    weight = w[...]
    copies = []
    for f in range(4):
        p = jnp.dot(x[f], weight, preferred_element_type=f32)
        for j in range(3):
            at = slice(j * tokens, (j + 1) * tokens)
            made[f, at] = p[:, j * LANES : (j + 1) * LANES].astype(bf16)
        d = jnp.concatenate([p[:, 3 * LANES :], p[:, 3 * LANES :]], axis=1)
        d = jnp.where(half, d[: tokens // 2], d[tokens // 2 :])
        made[f, 3 * tokens :] = d.astype(bf16)
        copies.append(pltpu.make_async_copy(made.at[f], out.at[f], left.at[f]))
        copies[f].start()
    for c in copies:
        c.wait()


def late_kernel(x, w, out, quarter, held, made, arrived, left):
    tokens = x.shape[1]
    columns = 2 * LANES
    into = pltpu.make_async_copy(w.at[:, :columns], held, arrived)
    into.start()
    across = pltpu.make_async_copy(w.at[:, columns:], quarter, left.at[4])
    across.start()
    into.wait()
    weight = held[...]
    copies = [across]
    for f in range(4):
        p = jnp.dot(x[f], weight, preferred_element_type=f32)
        made[f, :tokens] = p[:, :LANES].astype(bf16)
        made[f, tokens:] = p[:, LANES:].astype(bf16)
        copies.append(pltpu.make_async_copy(made.at[f], out.at[f], left.at[f]))
        copies[f + 1].start()
    for c in copies:
        c.wait()


def early_partials(x, w):
    _, tokens, _ = x.shape
    vmem = pl.BlockSpec(memory_space=pltpu.VMEM)
    anywhere = pl.BlockSpec(memory_space=pl.ANY)
    shape = (4, tokens * w.shape[1] // LANES, LANES)
    return pl.pallas_call(
        early_kernel,
        in_specs=[vmem, vmem],
        out_specs=[anywhere, vmem],
        out_shape=[struct(shape, bf16), pltpu.VMEM(x.shape, bf16)],
        scratch_shapes=[pltpu.VMEM(shape, bf16), pltpu.SemaphoreType.DMA((4,))],
        input_output_aliases={0: 1},
        compiler_params=limit,
        name="early_parts",
    )(x, w)


def late_partials(x, w):
    _, tokens, depth = x.shape
    vmem = pl.BlockSpec(memory_space=pltpu.VMEM)
    anywhere = pl.BlockSpec(memory_space=pl.ANY)
    shape = (4, 2 * tokens, LANES)
    return pl.pallas_call(
        late_kernel,
        in_specs=[vmem, anywhere],
        out_specs=[anywhere, anywhere],
        out_shape=[struct(shape, bf16), struct((depth, w.shape[1] - 2 * LANES), bf16)],
        scratch_shapes=[
            pltpu.VMEM((depth, 2 * LANES), bf16),
            pltpu.VMEM(shape, bf16),
            pltpu.SemaphoreType.DMA,
            pltpu.SemaphoreType.DMA((5,)),
        ],
        compiler_params=limit,
        name="late_parts",
    )(x, w)


def total_of(parts, at, rows):
    s = parts[0, at : at + rows].astype(f32)
    for k in (1, 2, 3):
        s = s + parts[k, at : at + rows].astype(f32)
    return s


def projected(parts, inverse, j):
    tokens = inverse.shape[0]
    return (total_of(parts, j * tokens, tokens) * inverse).astype(bf16)


def heads_of(x, half):
    return jnp.where(half, x[:HEAD], x[HEAD:])


def thirds(x):
    first = x.astype(bf16)
    left = x - first.astype(f32)
    second = left.astype(bf16)
    return first, second, (left - second.astype(f32)).astype(bf16)


def local_kernel(
    parts, inverse, second, bias, extra, keys, values, pool, tail, sums, prior, opening, run
):
    inv = inverse[...]
    tokens = inv.shape[0]
    keys[...] = projected(parts, inv, 0).astype(f32)
    values[...] = projected(parts, inv, 1).astype(f32)
    pooled = projected(parts, inv, 2)
    pool[...] = pooled
    tail[...] = pooled[tokens - HALO :]
    both = total_of(parts, 3 * tokens, tokens // 2)
    low = jnp.concatenate([both[:, :HEAD], both[:, HEAD:]], axis=0)
    low = (low * inv[:, :HEAD]).astype(bf16)
    x = jnp.dot(low, second[...], preferred_element_type=f32) + bias[...]
    rates = (jnp.minimum(x, 0.0) - jnp.log1p(jnp.exp(-jnp.abs(x)))) / decay_temper
    wide = lax.broadcasted_iota(jnp.int32, (2, LANES), 1) // HEAD
    pick = (wide == lax.broadcasted_iota(jnp.int32, (2, LANES), 0)).astype(f32)
    rates = rates + lax.dot_general(
        extra[...], pick, (((0,), (0,)), ((), ())), precision=highest, preferred_element_type=f32
    )
    r = lax.broadcasted_iota(jnp.int32, (BLOCK, BLOCK), 0)
    c = lax.broadcasted_iota(jnp.int32, (BLOCK, BLOCK), 1)
    lower = (r >= c).astype(f32)
    half = lax.broadcasted_iota(jnp.int32, (HEAD, LANES), 1) < HEAD
    state = jnp.zeros((HEAD, LANES), f32)
    before = jnp.zeros((1, LANES), f32)
    for n in range(tokens // BLOCK):
        at = slice(n * BLOCK, (n + 1) * BLOCK)
        total = jnp.dot(lower, rates[at], precision=highest, preferred_element_type=f32)
        sums[at] = total
        final = total[BLOCK - 1 :]
        pairs = lax.dot_general(
            values[at],
            keys[at] * jnp.exp(final - total),
            (((0,), (0,)), ((), ())),
            precision=highest,
            preferred_element_type=f32,
        )
        prior[at] = state
        opening[n : n + 1] = before
        state = jnp.exp(final) * state + heads_of(pairs, half)
        before = before + final
    run[:HEAD] = state.astype(bf16)
    row = lax.broadcasted_iota(jnp.int32, (RUN_ROWS - HEAD, LANES), 0)
    logs = jnp.zeros((RUN_ROWS - HEAD, LANES), f32)
    for j, part in enumerate(thirds(before)):
        logs = jnp.where(row == j, part.astype(f32), logs)
    run[HEAD:] = logs.astype(bf16)


def finish_kernel(
    sp,
    tp,
    runs,
    start,
    parts,
    inverse,
    pool,
    previous,
    keys,
    values,
    sums,
    prior,
    opening,
    gain,
    pool_weight,
    pool_scale,
    mine,
):
    inv = inverse[...]
    tokens = inv.shape[0]
    place = sp[0]
    state = start[...]
    for j in range(runs.shape[0] // RUN_ROWS):
        at = j * RUN_ROWS
        came = runs[at : at + RUN_ROWS].astype(f32)
        log = came[HEAD : HEAD + 1] + came[HEAD + 1 : HEAD + 2] + came[HEAD + 2 : HEAD + 3]
        state = jnp.where(j < place, jnp.exp(log) * state + came[:HEAD], state)
    queries = projected(parts, inv, 0).astype(f32) * HEAD ** (-0.5)
    outgate = projected(parts, inv, 1).astype(f32)
    half = lax.broadcasted_iota(jnp.int32, (HEAD, LANES), 1) < HEAD
    r = lax.broadcasted_iota(jnp.int32, (2 * BLOCK, BLOCK), 0) % BLOCK
    c = lax.broadcasted_iota(jnp.int32, (2 * BLOCK, BLOCK), 1)
    causal = r >= c

    def split(x):
        return jnp.concatenate([jnp.where(half, x, 0.0), jnp.where(half, 0.0, x)], axis=0)

    last = (((1,), (1,)), ((), ()))
    for n in range(tokens // BLOCK):
        at = slice(n * BLOCK, (n + 1) * BLOCK)
        total = sums[at]
        middle = total[BLOCK // 2 - 1 : BLOCK // 2]
        q = queries[at]
        scores = lax.dot_general(
            split(q * jnp.exp(total - middle)),
            keys[at] * jnp.exp(middle - total),
            last,
            precision=highest,
            preferred_element_type=f32,
        )
        scores = jnp.where(causal, scores, 0.0)
        within = jnp.dot(scores, values[at], precision=highest, preferred_element_type=f32)
        begin = prior[at] + jnp.exp(opening[n : n + 1]) * state
        carried = lax.dot_general(
            split(q * jnp.exp(total)),
            jnp.concatenate([begin, begin], axis=0),
            last,
            precision=highest,
            preferred_element_type=f32,
        )
        raw = heads_of(within + carried, half)
        square = raw * raw
        first = jnp.sum(jnp.where(half, square, 0.0), axis=1, keepdims=True)
        second = jnp.sum(jnp.where(half, 0.0, square), axis=1, keepdims=True)
        mean = jnp.where(half, first, second) / HEAD
        g = outgate[at]
        scaled = raw * lax.rsqrt(mean + norm_eps) * gain[...]
        done = (scaled * (g / (1.0 + jnp.exp(-g)))).astype(bf16)
        for to in range(mine.shape[0]):
            mine[to, at, LANES:] = done

    current = pool[...].astype(f32)
    extended = jnp.concatenate([previous[...].astype(f32), current], axis=0)

    def back(x, by):
        return x + pltpu.roll(x, by, 0)

    two = back(extended, 1)
    four = back(two, 2)
    eight = back(four, 4)
    sixteen = back(eight, 8)
    level = tp[0] % 4
    chosen = jnp.where(
        level == 0, two, jnp.where(level == 1, four, jnp.where(level == 2, eight, sixteen))
    )[HALO:]
    window = jnp.where(
        level == 0, 2.0, jnp.where(level == 1, 4.0, jnp.where(level == 2, 8.0, 16.0))
    )
    position = place * tokens + lax.broadcasted_iota(jnp.int32, (tokens, LANES), 0)
    counts = jnp.minimum(position.astype(f32) + 1.0, window)
    deviation = (chosen / counts - current).astype(bf16)
    mixture = jnp.dot(deviation, pool_weight[...], preferred_element_type=f32)
    done = (mixture * pool_scale[...]).astype(bf16)
    for to in range(mine.shape[0]):
        mine[to, :, :LANES] = done


def output_kernel(core, same, other, rows, out, held, arrived):
    steps = [(x, z, c) for z, c in ((same, core[0]), (other, 1 - core[0])) for x in range(same.shape[0])]
    copies = []
    for j, (x, _, c) in enumerate(steps):
        at = pl.ds(pl.multiple_of((2 * x + c) * LANES, LANES), LANES)
        copies.append(pltpu.make_async_copy(rows.at[:, at], held.at[j], arrived.at[j]))
        copies[j].start()
    total = jnp.zeros(out.shape, f32)
    for j, (x, z, _) in enumerate(steps):
        copies[j].wait()
        w = jnp.concatenate(
            [
                jnp.concatenate([held[j, f, :, :LANES], held[j, f, :, LANES:]], axis=0)
                for f in range(rows.shape[0])
            ],
            axis=1,
        )
        total = total + jnp.dot(z[x], w, preferred_element_type=f32)
    out[...] = total.astype(bf16)


def output(core, same, other, rows):
    tokens = same.shape[1]
    parts, _, width = rows.shape
    steps = 2 * same.shape[0]
    vmem = pl.BlockSpec(memory_space=pltpu.VMEM)
    return pl.pallas_call(
        output_kernel,
        in_specs=[
            pl.BlockSpec(memory_space=pltpu.SMEM),
            vmem,
            vmem,
            pl.BlockSpec(memory_space=pl.ANY),
        ],
        out_specs=vmem,
        out_shape=struct((tokens, parts * LANES), bf16),
        scratch_shapes=[
            pltpu.VMEM((steps, parts, LANES, width), bf16),
            pltpu.SemaphoreType.DMA((steps,)),
        ],
        name="output",
    )(core, same, other, rows)


def body(
    activations,
    input_norm_gain,
    pooling_channel_weight,
    query_projection_weight,
    key_projection_weight,
    value_projection_weight,
    output_gate_weight,
    decay_first_factor,
    decay_second_factor,
    decay_gate_bias,
    decay_extra_log,
    head_norm_gain,
    starting_state,
    pooling_group_weight,
    pooling_channel_scale,
    pooling_output_rows,
    attention_output_rows,
):
    _, tokens, width = activations.shape
    rows = key_projection_weight.shape[0]
    own = lax.axis_index("fs").astype(jnp.int32).reshape(1)
    tp = lax.axis_index("tp").astype(jnp.int32)
    early, late = call(
        pack_kernel,
        [struct((rows, 3 * LANES + HEAD), bf16), struct((rows, 4 * LANES), bf16)],
        "pack",
        own,
        key_projection_weight,
        value_projection_weight,
        pooling_channel_weight,
        decay_first_factor,
        query_projection_weight,
        output_gate_weight,
        pooling_output_rows,
        attention_output_rows,
    )
    late, early, activations = lax.optimization_barrier((late, early, activations))
    late = lax.all_gather(late, "sp", axis=0, tiled=True)
    x, inverse = prepare(activations.reshape(tokens, width), input_norm_gain.reshape(1, width))
    x = lax.all_to_all(x, "fs", 0, 0)
    early = lax.all_gather(early, "sp", axis=0, tiled=True)
    inverse = near(inverse)
    parts, x = early_partials(near(x), near(early))
    parts = lax.all_to_all(parts, "fs", 0, 0)
    wide = pltpu.VMEM((tokens, LANES), f32)
    keys, values, pool, tail, sums, prior, opening, run = call(
        local_kernel,
        [
            wide,
            wide,
            pltpu.VMEM((tokens, LANES), bf16),
            struct((HALO, LANES), bf16),
            wide,
            wide,
            pltpu.VMEM((tokens // BLOCK, LANES), f32),
            struct((RUN_ROWS, LANES), bf16),
        ],
        "local",
        near(parts),
        inverse,
        decay_second_factor,
        decay_gate_bias.reshape(1, LANES),
        decay_extra_log,
        scalars=0,
    )
    previous = shifted(tail, "sp", 1, False)
    start = starting_state[0].transpose(2, 0, 1).reshape(HEAD, LANES)
    late, run = lax.optimization_barrier((late, run))
    late, quarter = late_partials(near(x), late)
    late, quarter, run = lax.optimization_barrier((late, quarter, run))
    out_rows = lax.all_gather(quarter, "fs")
    late = lax.all_to_all(late, "fs", 0, 0)
    runs = lax.all_gather(run, "sp", axis=0, tiled=True)
    peers = lax.axis_size("tp")
    (mine,) = call(
        finish_kernel,
        [struct((peers // 2, tokens, 2 * LANES), bf16)],
        "finish",
        lax.axis_index("sp").astype(jnp.int32).reshape(1),
        tp.reshape(1),
        near(runs),
        near(start),
        near(late),
        inverse,
        near(pool),
        near(previous),
        near(keys),
        near(values),
        near(sums),
        near(prior),
        near(opening),
        head_norm_gain.reshape(1, LANES),
        pooling_group_weight[0],
        pooling_channel_scale.reshape(1, LANES),
        scalars=2,
    )
    groups = [[c + 2 * x for x in range(peers // 2)] for c in range(2)]
    same = lax.all_to_all(mine, "tp", 0, 0, axis_index_groups=groups)
    other = lax.ppermute(same, "tp", [(i, i ^ 1) for i in range(peers)])
    return output((tp & 1).reshape(1), near(same), near(other), out_rows)[None]


def solution(mesh):
    in_specs = (
        P("fs", "sp", None),
        P(),
        P(("sp", "fs"), "tp"),
        P(("sp", "fs"), "tp"),
        P(("sp", "fs"), "tp"),
        P(("sp", "fs"), "tp"),
        P(("sp", "fs"), "tp"),
        P(("sp", "fs"), None),
        P(None, "tp"),
        P("tp"),
        P("tp", "sp"),
        P("tp"),
        P("fs", "tp", None, None),
        P("tp", None, None),
        P("tp"),
        P("sp", "tp"),
        P("sp", "tp"),
    )
    out_specs = P("fs", "sp", "tp")

    return jax.shard_map(body, mesh=mesh, in_specs=in_specs, out_specs=out_specs, check_vma=False)
```

```python
import jax
import jax.numpy as jnp
from jax import lax
from jax.experimental import pallas as pl
from jax.experimental.pallas import tpu as pltpu
from jax.sharding import PartitionSpec as P


BLOCK = 64
HEAD = 64
LANES = 128
HALO = 16
RUN_ROWS = 96
norm_eps = 1e-06
decay_temper = 16.0
highest = lax.Precision.HIGHEST
f32 = jnp.float32
bf16 = jnp.bfloat16
limit = pltpu.CompilerParams(vmem_limit_bytes=24 << 20)


def call(kernel, outs, name, *args, scalars=1, aliases={}):
    smem = pl.BlockSpec(memory_space=pltpu.SMEM)
    vmem = pl.BlockSpec(memory_space=pltpu.VMEM)
    return pl.pallas_call(
        kernel,
        in_specs=[smem] * scalars + [vmem] * (len(args) - scalars),
        out_specs=[vmem] * len(outs),
        out_shape=outs,
        input_output_aliases=aliases,
        compiler_params=limit if name == "local" else None,
    )(*args)


def near(x):
    return pltpu.with_memory_space_constraint(x, pltpu.VMEM)


def struct(shape, dtype):
    return jax.ShapeDtypeStruct(shape, dtype)


def pack_kernel(
    own, key, value, pool, low, query, gate, pool_rows, state_rows, early, late, moved
):
    mine = pl.ds(pl.multiple_of(own[0] * LANES, LANES), LANES)
    moves = []
    for out, blocks in (
        (late, (query, gate, pool_rows.at[:, mine], state_rows.at[:, mine])),
        (early, (key, value, pool, low)),
    ):
        at = 0
        for block in blocks:
            width = block.shape[1]
            to = out.at[:, at : at + width]
            moves.append(pltpu.make_async_copy(block, to, moved.at[len(moves)]))
            moves[-1].start()
            at += width
    for move in moves:
        move.wait()


def pack(own, blocks, outs):
    anywhere = pl.BlockSpec(memory_space=pl.ANY)
    return pl.pallas_call(
        pack_kernel,
        in_specs=[pl.BlockSpec(memory_space=pltpu.SMEM)] + [anywhere] * len(blocks),
        out_specs=[anywhere] * len(outs),
        out_shape=outs,
        scratch_shapes=[pltpu.SemaphoreType.DMA((len(blocks),))],
        name="pack",
    )(own, *blocks)


def prep_kernel(act, gain, x, inverse, held, arrived):
    tokens, width = act.shape
    rows = tokens // 4
    copies = []
    for c in range(4):
        at = pl.ds(c * rows, rows)
        copies.append(pltpu.make_async_copy(act.at[at], held.at[at], arrived.at[c]))
        copies[c].start()
    half = lax.broadcasted_iota(jnp.int32, (rows, LANES), 1) < HEAD
    for c in range(4):
        copies[c].wait()
        block = pl.ds(c * rows, rows)
        squares = jnp.zeros((rows, LANES), f32)
        for p in range(width // 512):
            tiles = []
            for q in range(4):
                at = p * 512 + q * LANES
                t = held[block, at : at + LANES].astype(f32)
                squares = squares + t * t
                tiles.append(t * gain[:, at : at + LANES])
            to = slice(p * LANES, (p + 1) * LANES)
            for j, (a, b) in enumerate(((tiles[0], tiles[2]), (tiles[1], tiles[3]))):
                x[2 * j, block, to] = jnp.where(half, a, pltpu.roll(b, HEAD, 1)).astype(bf16)
                x[2 * j + 1, block, to] = jnp.where(half, pltpu.roll(a, HEAD, 1), b).astype(bf16)
        total = jnp.sum(squares, axis=1, keepdims=True)
        inverse[block] = jnp.broadcast_to(lax.rsqrt(total / width + norm_eps), (rows, LANES))


def prepare(act, gain):
    tokens, width = act.shape
    vmem = pl.BlockSpec(memory_space=pltpu.VMEM)
    return pl.pallas_call(
        prep_kernel,
        in_specs=[pl.BlockSpec(memory_space=pl.ANY), vmem],
        out_specs=[vmem, vmem],
        out_shape=[struct((4, tokens, width // 4), bf16), struct((tokens, LANES), f32)],
        scratch_shapes=[pltpu.VMEM((tokens, width), bf16), pltpu.SemaphoreType.DMA((4,))],
        name="prep",
    )(act, gain)


def thirds(x):
    first = x.astype(bf16)
    left = x - first.astype(f32)
    second = left.astype(bf16)
    return first, second, (left - second.astype(f32)).astype(bf16)


def early_kernel(x, w, out, same_x, made, left):
    tokens = x.shape[1]
    half = lax.broadcasted_iota(jnp.int32, (tokens // 2, LANES), 1) < HEAD
    weight = w[...]
    copies = []
    for f in range(4):
        p = jnp.dot(x[f], weight, preferred_element_type=f32)
        for j in range(3):
            at = slice(j * tokens, (j + 1) * tokens)
            made[f, at] = p[:, j * LANES : (j + 1) * LANES].astype(bf16)
        d = jnp.concatenate([p[:, 3 * LANES :], p[:, 3 * LANES :]], axis=1)
        d = jnp.where(half, d[: tokens // 2], d[tokens // 2 :])
        made[f, 3 * tokens :] = d.astype(bf16)
        copies.append(pltpu.make_async_copy(made.at[f], out.at[f], left.at[f]))
        copies[f].start()
    for c in copies:
        c.wait()


def late_kernel(x, w, out, quarter, held, made, arrived, left):
    tokens = x.shape[1]
    columns = 2 * LANES
    into = pltpu.make_async_copy(w.at[:, :columns], held, arrived)
    into.start()
    across = pltpu.make_async_copy(w.at[:, columns:], quarter, left.at[4])
    across.start()
    into.wait()
    weight = held[...]
    copies = [across]
    for f in range(4):
        p = jnp.dot(x[f], weight, preferred_element_type=f32)
        made[f, :tokens] = p[:, :LANES].astype(bf16)
        made[f, tokens:] = p[:, LANES:].astype(bf16)
        copies.append(pltpu.make_async_copy(made.at[f], out.at[f], left.at[f]))
        copies[f + 1].start()
    for c in copies:
        c.wait()


def early_partials(x, w):
    _, tokens, _ = x.shape
    vmem = pl.BlockSpec(memory_space=pltpu.VMEM)
    anywhere = pl.BlockSpec(memory_space=pl.ANY)
    shape = (4, tokens * w.shape[1] // LANES, LANES)
    return pl.pallas_call(
        early_kernel,
        in_specs=[vmem, vmem],
        out_specs=[anywhere, vmem],
        out_shape=[struct(shape, bf16), pltpu.VMEM(x.shape, bf16)],
        scratch_shapes=[pltpu.VMEM(shape, bf16), pltpu.SemaphoreType.DMA((4,))],
        input_output_aliases={0: 1},
        compiler_params=limit,
        name="early_parts",
    )(x, w)


def late_partials(x, w):
    _, tokens, depth = x.shape
    vmem = pl.BlockSpec(memory_space=pltpu.VMEM)
    anywhere = pl.BlockSpec(memory_space=pl.ANY)
    shape = (4, 2 * tokens, LANES)
    return pl.pallas_call(
        late_kernel,
        in_specs=[vmem, pl.BlockSpec(memory_space=pltpu.HBM)],
        out_specs=[anywhere, anywhere],
        out_shape=[struct(shape, bf16), struct((depth, w.shape[1] - 2 * LANES), bf16)],
        scratch_shapes=[
            pltpu.VMEM((depth, 2 * LANES), bf16),
            pltpu.VMEM(shape, bf16),
            pltpu.SemaphoreType.DMA,
            pltpu.SemaphoreType.DMA((5,)),
        ],
        compiler_params=limit,
        name="late_parts",
    )(x, pltpu.with_memory_space_constraint(w, pltpu.HBM))


def total_of(parts, at, rows):
    s = parts[0, at : at + rows].astype(f32)
    for k in (1, 2, 3):
        s = s + parts[k, at : at + rows].astype(f32)
    return s


def projected(parts, inverse, j):
    tokens = inverse.shape[0]
    return (total_of(parts, j * tokens, tokens) * inverse).astype(bf16)


def heads_of(x, half):
    return jnp.where(half, x[:HEAD], x[HEAD:])


def thirds(x):
    first = x.astype(bf16)
    left = x - first.astype(f32)
    second = left.astype(bf16)
    return first, second, (left - second.astype(f32)).astype(bf16)


def local_kernel(
    parts, inverse, second, bias, extra, keys, values, pool, sums, prior, opening, run
):
    inv = inverse[...]
    tokens = inv.shape[0]
    keys[...] = projected(parts, inv, 0).astype(f32)
    values[...] = projected(parts, inv, 1).astype(f32)
    pooled = projected(parts, inv, 2)
    pool[...] = pooled
    run[RUN_ROWS - HALO :] = pooled[tokens - HALO :]
    both = total_of(parts, 3 * tokens, tokens // 2)
    low = jnp.concatenate([both[:, :HEAD], both[:, HEAD:]], axis=0)
    low = (low * inv[:, :HEAD]).astype(bf16)
    x = jnp.dot(low, second[...], preferred_element_type=f32) + bias[...]
    rates = (jnp.minimum(x, 0.0) - jnp.log1p(jnp.exp(-jnp.abs(x)))) / decay_temper
    wide = lax.broadcasted_iota(jnp.int32, (2, LANES), 1) // HEAD
    pick = (wide == lax.broadcasted_iota(jnp.int32, (2, LANES), 0)).astype(f32)
    rates = rates + lax.dot_general(
        extra[...], pick, (((0,), (0,)), ((), ())), precision=highest, preferred_element_type=f32
    )
    r = lax.broadcasted_iota(jnp.int32, (BLOCK, BLOCK), 0)
    c = lax.broadcasted_iota(jnp.int32, (BLOCK, BLOCK), 1)
    lower = (r >= c).astype(f32)
    half = lax.broadcasted_iota(jnp.int32, (HEAD, LANES), 1) < HEAD
    state = jnp.zeros((HEAD, LANES), f32)
    before = jnp.zeros((1, LANES), f32)
    for n in range(tokens // BLOCK):
        at = slice(n * BLOCK, (n + 1) * BLOCK)
        total = jnp.dot(lower, rates[at], precision=highest, preferred_element_type=f32)
        sums[at] = total
        final = total[BLOCK - 1 :]
        pairs = lax.dot_general(
            values[at],
            keys[at] * jnp.exp(final - total),
            (((0,), (0,)), ((), ())),
            precision=highest,
            preferred_element_type=f32,
        )
        prior[at] = state
        opening[n : n + 1] = before
        state = jnp.exp(final) * state + heads_of(pairs, half)
        before = before + final
    run[:HEAD] = state.astype(bf16)
    row = lax.broadcasted_iota(jnp.int32, (HALO, LANES), 0)
    logs = jnp.zeros((HALO, LANES), f32)
    for j, part in enumerate(thirds(before)):
        logs = jnp.where(row == j, part.astype(f32), logs)
    run[HEAD : HEAD + HALO] = logs.astype(bf16)


def finish_kernel(
    sp,
    tp,
    runs,
    start,
    parts,
    inverse,
    pool,
    keys,
    values,
    sums,
    prior,
    opening,
    gain,
    pool_weight,
    pool_scale,
    mine,
):
    inv = inverse[...]
    tokens = inv.shape[0]
    place = sp[0]
    state = start[...]
    for j in range(runs.shape[0]):
        came = runs[j].astype(f32)
        log = came[HEAD : HEAD + 1] + came[HEAD + 1 : HEAD + 2] + came[HEAD + 2 : HEAD + 3]
        state = jnp.where(j < place, jnp.exp(log) * state + came[:HEAD], state)
    queries = projected(parts, inv, 0).astype(f32) * HEAD ** (-0.5)
    outgate = projected(parts, inv, 1).astype(f32)
    half = lax.broadcasted_iota(jnp.int32, (HEAD, LANES), 1) < HEAD
    r = lax.broadcasted_iota(jnp.int32, (2 * BLOCK, BLOCK), 0) % BLOCK
    c = lax.broadcasted_iota(jnp.int32, (2 * BLOCK, BLOCK), 1)
    causal = r >= c

    def split(x):
        return jnp.concatenate([jnp.where(half, x, 0.0), jnp.where(half, 0.0, x)], axis=0)

    last = (((1,), (1,)), ((), ()))
    for n in range(tokens // BLOCK):
        at = slice(n * BLOCK, (n + 1) * BLOCK)
        total = sums[at]
        middle = total[BLOCK // 2 - 1 : BLOCK // 2]
        q = queries[at]
        scores = lax.dot_general(
            split(q * jnp.exp(total - middle)),
            keys[at] * jnp.exp(middle - total),
            last,
            precision=highest,
            preferred_element_type=f32,
        )
        scores = jnp.where(causal, scores, 0.0)
        within = jnp.dot(scores, values[at], precision=highest, preferred_element_type=f32)
        begin = prior[at] + jnp.exp(opening[n : n + 1]) * state
        carried = lax.dot_general(
            split(q * jnp.exp(total)),
            jnp.concatenate([begin, begin], axis=0),
            last,
            precision=highest,
            preferred_element_type=f32,
        )
        raw = heads_of(within + carried, half)
        square = raw * raw
        first = jnp.sum(jnp.where(half, square, 0.0), axis=1, keepdims=True)
        second = jnp.sum(jnp.where(half, 0.0, square), axis=1, keepdims=True)
        mean = jnp.where(half, first, second) / HEAD
        g = outgate[at]
        scaled = raw * lax.rsqrt(mean + norm_eps) * gain[...]
        done = (scaled * (g / (1.0 + jnp.exp(-g)))).astype(bf16)
        for to in range(mine.shape[0]):
            mine[to, at, LANES:] = done

    current = pool[...].astype(f32)
    previous = runs[jnp.maximum(place - 1, 0), RUN_ROWS - HALO :].astype(f32)
    previous = jnp.where(place > 0, previous, 0.0)
    extended = jnp.concatenate([previous, current], axis=0)

    def back(x, by):
        return x + pltpu.roll(x, by, 0)

    two = back(extended, 1)
    four = back(two, 2)
    eight = back(four, 4)
    sixteen = back(eight, 8)
    level = tp[0] % 4
    chosen = jnp.where(
        level == 0, two, jnp.where(level == 1, four, jnp.where(level == 2, eight, sixteen))
    )[HALO:]
    window = jnp.where(
        level == 0, 2.0, jnp.where(level == 1, 4.0, jnp.where(level == 2, 8.0, 16.0))
    )
    position = place * tokens + lax.broadcasted_iota(jnp.int32, (tokens, LANES), 0)
    counts = jnp.minimum(position.astype(f32) + 1.0, window)
    deviation = (chosen / counts - current).astype(bf16)
    mixture = jnp.dot(deviation, pool_weight[...], preferred_element_type=f32)
    done = (mixture * pool_scale[...]).astype(bf16)
    for to in range(mine.shape[0]):
        mine[to, :, :LANES] = done


def output_kernel(core, z, rows, *rest):
    *before, out, held, arrived = rest
    copies = []
    for x in range(z.shape[0]):
        at = pl.ds(pl.multiple_of((2 * x + core[0]) * LANES, LANES), LANES)
        copies.append(pltpu.make_async_copy(rows.at[:, at], held.at[x], arrived.at[x]))
        copies[x].start()
    total = jnp.zeros(out.shape, f32)
    for b in before:
        total = b[...]
    for x in range(z.shape[0]):
        copies[x].wait()
        w = jnp.concatenate(
            [
                jnp.concatenate([held[x, f, :, :LANES], held[x, f, :, LANES:]], axis=0)
                for f in range(rows.shape[0])
            ],
            axis=1,
        )
        total = total + jnp.dot(z[x], w, preferred_element_type=f32)
    out[...] = total.astype(out.dtype)


def output(core, z, rows, before, out):
    vmem = pl.BlockSpec(memory_space=pltpu.VMEM)
    steps = z.shape[0]
    parts, _, width = rows.shape
    return pl.pallas_call(
        output_kernel,
        in_specs=[
            pl.BlockSpec(memory_space=pltpu.SMEM),
            vmem,
            pl.BlockSpec(memory_space=pl.ANY),
        ]
        + [vmem] * len(before),
        out_specs=vmem,
        out_shape=out,
        scratch_shapes=[
            pltpu.VMEM((steps, parts, LANES, width), bf16),
            pltpu.SemaphoreType.DMA((steps,)),
        ],
    )(core, near(z), rows, *before)


def body(
    activations,
    input_norm_gain,
    pooling_channel_weight,
    query_projection_weight,
    key_projection_weight,
    value_projection_weight,
    output_gate_weight,
    decay_first_factor,
    decay_second_factor,
    decay_gate_bias,
    decay_extra_log,
    head_norm_gain,
    starting_state,
    pooling_group_weight,
    pooling_channel_scale,
    pooling_output_rows,
    attention_output_rows,
):
    _, tokens, width = activations.shape
    rows = key_projection_weight.shape[0]
    columns = pooling_output_rows.shape[1]
    own = lax.axis_index("fs").astype(jnp.int32).reshape(1)
    tp = lax.axis_index("tp").astype(jnp.int32)
    early, late = pack(
        own,
        (
            key_projection_weight,
            value_projection_weight,
            pooling_channel_weight,
            decay_first_factor,
            query_projection_weight,
            output_gate_weight,
            pooling_output_rows,
            attention_output_rows,
        ),
        [struct((rows, 3 * LANES + HEAD), bf16), struct((rows, 4 * LANES), bf16)],
    )
    late, early, activations = lax.optimization_barrier((late, early, activations))
    late = lax.all_gather(late, "sp", axis=0, tiled=True)
    x, inverse = prepare(activations.reshape(tokens, width), input_norm_gain.reshape(1, width))
    x = lax.all_to_all(x, "fs", 0, 0)
    early = lax.all_gather(early, "sp").reshape(-1, early.shape[1])
    inverse = near(inverse)
    parts, x = early_partials(near(x), near(early))
    parts = lax.all_to_all(parts, "fs", 0, 0)
    wide = pltpu.VMEM((tokens, LANES), f32)
    keys, values, pool, sums, prior, opening, run = call(
        local_kernel,
        [
            wide,
            wide,
            pltpu.VMEM((tokens, LANES), bf16),
            wide,
            wide,
            pltpu.VMEM((tokens // BLOCK, LANES), f32),
            struct((RUN_ROWS, LANES), bf16),
        ],
        "local",
        near(parts),
        inverse,
        decay_second_factor,
        decay_gate_bias.reshape(1, LANES),
        decay_extra_log,
        scalars=0,
    )
    start = starting_state[0].transpose(2, 0, 1).reshape(HEAD, LANES)
    late, run = lax.optimization_barrier((late, run))
    late, quarter = late_partials(near(x), late)
    late, quarter, run = lax.optimization_barrier((late, quarter, run))
    out_rows = lax.all_gather(quarter, "fs")
    late = lax.all_to_all(late, "fs", 0, 0)
    runs = lax.all_gather(run, "sp")
    peers = lax.axis_size("tp")
    (mine,) = call(
        finish_kernel,
        [struct((peers // 2, tokens, 2 * LANES), bf16)],
        "finish",
        lax.axis_index("sp").astype(jnp.int32).reshape(1),
        tp.reshape(1),
        near(runs),
        near(start),
        near(late),
        inverse,
        near(pool),
        near(keys),
        near(values),
        near(sums),
        near(prior),
        near(opening),
        head_norm_gain.reshape(1, LANES),
        pooling_group_weight[0],
        pooling_channel_scale.reshape(1, LANES),
        scalars=2,
    )
    groups = [[c + 2 * x for x in range(peers // 2)] for c in range(2)]
    same = lax.all_to_all(mine, "tp", 0, 0, axis_index_groups=groups)
    same, out_rows = lax.optimization_barrier((same, out_rows))
    other = lax.ppermute(same, "tp", [(i, i ^ 1) for i in range(peers)])
    core = (tp & 1).reshape(1)
    half = output(core, same, out_rows, (), pltpu.VMEM((tokens, columns), f32))
    result = output(1 - core, other, out_rows, (near(half),), struct((tokens, columns), bf16))
    return result[None]


def solution(mesh):
    in_specs = (
        P("fs", "sp", None),
        P(),
        P(("sp", "fs"), "tp"),
        P(("sp", "fs"), "tp"),
        P(("sp", "fs"), "tp"),
        P(("sp", "fs"), "tp"),
        P(("sp", "fs"), "tp"),
        P(("sp", "fs"), None),
        P(None, "tp"),
        P("tp"),
        P("tp", "sp"),
        P("tp"),
        P("fs", "tp", None, None),
        P("tp", None, None),
        P("tp"),
        P("sp", "tp"),
        P("sp", "tp"),
    )
    out_specs = P("fs", "sp", "tp")

    return jax.shard_map(body, mesh=mesh, in_specs=in_specs, out_specs=out_specs, check_vma=False)
```

```python
import jax
import jax.numpy as jnp
from jax import lax
from jax.experimental import pallas as pl
from jax.experimental.pallas import tpu as pltpu
from jax.sharding import PartitionSpec as P


BLOCK = 64
HEAD = 64
LANES = 128
HALO = 16
RUN_ROWS = 96
norm_eps = 1e-06
decay_temper = 16.0
highest = lax.Precision.HIGHEST
f32 = jnp.float32
bf16 = jnp.bfloat16
limit = pltpu.CompilerParams(vmem_limit_bytes=24 << 20)


def call(kernel, outs, name, *args, scalars=1, aliases={}):
    smem = pl.BlockSpec(memory_space=pltpu.SMEM)
    vmem = pl.BlockSpec(memory_space=pltpu.VMEM)
    return pl.pallas_call(
        kernel,
        in_specs=[smem] * scalars + [vmem] * (len(args) - scalars),
        out_specs=[vmem] * len(outs),
        out_shape=outs,
        input_output_aliases=aliases,
        compiler_params=limit if name == "local" else None,
    )(*args)


def near(x):
    return pltpu.with_memory_space_constraint(x, pltpu.VMEM)


def struct(shape, dtype):
    return jax.ShapeDtypeStruct(shape, dtype)


def pack_kernel(own, key, value, pool, low, query, gate, pool_rows, state_rows, early, late):
    at = 0
    for r in (key, value, pool, low):
        early[:, at : at + r.shape[1]] = r[...]
        at += r.shape[1]
    mine = pl.ds(pl.multiple_of(own[0] * LANES, LANES), LANES)
    blocks = (query[...], gate[...], pool_rows[:, mine], state_rows[:, mine])
    for j, block in enumerate(blocks):
        late[:, j * LANES : (j + 1) * LANES] = block


def prep_kernel(act, gain, x, inverse, held, arrived):
    tokens, width = act.shape
    rows = tokens // 4
    copies = []
    for c in range(4):
        at = pl.ds(c * rows, rows)
        copies.append(pltpu.make_async_copy(act.at[at], held.at[at], arrived.at[c]))
        copies[c].start()
    half = lax.broadcasted_iota(jnp.int32, (rows, LANES), 1) < HEAD
    for c in range(4):
        copies[c].wait()
        block = pl.ds(c * rows, rows)
        squares = jnp.zeros((rows, LANES), f32)
        for p in range(width // 512):
            tiles = []
            for q in range(4):
                at = p * 512 + q * LANES
                t = held[block, at : at + LANES].astype(f32)
                squares = squares + t * t
                tiles.append(t * gain[:, at : at + LANES])
            to = slice(p * LANES, (p + 1) * LANES)
            for j, (a, b) in enumerate(((tiles[0], tiles[2]), (tiles[1], tiles[3]))):
                x[2 * j, block, to] = jnp.where(half, a, pltpu.roll(b, HEAD, 1)).astype(bf16)
                x[2 * j + 1, block, to] = jnp.where(half, pltpu.roll(a, HEAD, 1), b).astype(bf16)
        total = jnp.sum(squares, axis=1, keepdims=True)
        inverse[block] = jnp.broadcast_to(lax.rsqrt(total / width + norm_eps), (rows, LANES))


def prepare(act, gain):
    tokens, width = act.shape
    vmem = pl.BlockSpec(memory_space=pltpu.VMEM)
    return pl.pallas_call(
        prep_kernel,
        in_specs=[pl.BlockSpec(memory_space=pl.ANY), vmem],
        out_specs=[vmem, vmem],
        out_shape=[struct((4, tokens, width // 4), bf16), struct((tokens, LANES), f32)],
        scratch_shapes=[pltpu.VMEM((tokens, width), bf16), pltpu.SemaphoreType.DMA((4,))],
        name="prep",
    )(act, gain)


def thirds(x):
    first = x.astype(bf16)
    left = x - first.astype(f32)
    second = left.astype(bf16)
    return first, second, (left - second.astype(f32)).astype(bf16)


def early_kernel(x, w, out, same_x, made, left):
    tokens = x.shape[1]
    half = lax.broadcasted_iota(jnp.int32, (tokens // 2, LANES), 1) < HEAD
    weight = w[...]
    copies = []
    for f in range(4):
        p = jnp.dot(x[f], weight, preferred_element_type=f32)
        for j in range(3):
            at = slice(j * tokens, (j + 1) * tokens)
            made[f, at] = p[:, j * LANES : (j + 1) * LANES].astype(bf16)
        d = jnp.concatenate([p[:, 3 * LANES :], p[:, 3 * LANES :]], axis=1)
        d = jnp.where(half, d[: tokens // 2], d[tokens // 2 :])
        made[f, 3 * tokens :] = d.astype(bf16)
        copies.append(pltpu.make_async_copy(made.at[f], out.at[f], left.at[f]))
        copies[f].start()
    for c in copies:
        c.wait()


def late_kernel(x, w, out, quarter, held, made, arrived, left):
    tokens = x.shape[1]
    columns = 2 * LANES
    into = pltpu.make_async_copy(w, held, arrived)
    into.start()
    into.wait()
    across = pltpu.make_async_copy(held.at[:, columns:], quarter, left.at[4])
    across.start()
    weight = held[:, :columns]
    copies = [across]
    for f in range(4):
        p = jnp.dot(x[f], weight, preferred_element_type=f32)
        made[f, :tokens] = p[:, :LANES].astype(bf16)
        made[f, tokens:] = p[:, LANES:].astype(bf16)
        copies.append(pltpu.make_async_copy(made.at[f], out.at[f], left.at[f]))
        copies[f + 1].start()
    for c in copies:
        c.wait()


def early_partials(x, w):
    _, tokens, _ = x.shape
    vmem = pl.BlockSpec(memory_space=pltpu.VMEM)
    anywhere = pl.BlockSpec(memory_space=pl.ANY)
    shape = (4, tokens * w.shape[1] // LANES, LANES)
    return pl.pallas_call(
        early_kernel,
        in_specs=[vmem, vmem],
        out_specs=[anywhere, vmem],
        out_shape=[struct(shape, bf16), pltpu.VMEM(x.shape, bf16)],
        scratch_shapes=[pltpu.VMEM(shape, bf16), pltpu.SemaphoreType.DMA((4,))],
        input_output_aliases={0: 1},
        compiler_params=limit,
        name="early_parts",
    )(x, w)


def late_partials(x, w):
    _, tokens, depth = x.shape
    vmem = pl.BlockSpec(memory_space=pltpu.VMEM)
    anywhere = pl.BlockSpec(memory_space=pl.ANY)
    shape = (4, 2 * tokens, LANES)
    return pl.pallas_call(
        late_kernel,
        in_specs=[vmem, pl.BlockSpec(memory_space=pltpu.HBM)],
        out_specs=[anywhere, anywhere],
        out_shape=[struct(shape, bf16), struct((depth, w.shape[1] - 2 * LANES), bf16)],
        scratch_shapes=[
            pltpu.VMEM(w.shape, bf16),
            pltpu.VMEM(shape, bf16),
            pltpu.SemaphoreType.DMA,
            pltpu.SemaphoreType.DMA((5,)),
        ],
        compiler_params=limit,
        name="late_parts",
    )(x, pltpu.with_memory_space_constraint(w, pltpu.HBM))


def total_of(parts, at, rows):
    s = parts[0, at : at + rows].astype(f32)
    for k in (1, 2, 3):
        s = s + parts[k, at : at + rows].astype(f32)
    return s


def projected(parts, inverse, j):
    tokens = inverse.shape[0]
    return (total_of(parts, j * tokens, tokens) * inverse).astype(bf16)


def heads_of(x, half):
    return jnp.where(half, x[:HEAD], x[HEAD:])


def thirds(x):
    first = x.astype(bf16)
    left = x - first.astype(f32)
    second = left.astype(bf16)
    return first, second, (left - second.astype(f32)).astype(bf16)


def local_kernel(
    parts, inverse, second, bias, extra, keys, values, pool, sums, prior, opening, run
):
    inv = inverse[...]
    tokens = inv.shape[0]
    keys[...] = projected(parts, inv, 0).astype(f32)
    values[...] = projected(parts, inv, 1).astype(f32)
    pooled = projected(parts, inv, 2)
    pool[...] = pooled
    run[RUN_ROWS - HALO :] = pooled[tokens - HALO :]
    both = total_of(parts, 3 * tokens, tokens // 2)
    low = jnp.concatenate([both[:, :HEAD], both[:, HEAD:]], axis=0)
    low = (low * inv[:, :HEAD]).astype(bf16)
    x = jnp.dot(low, second[...], preferred_element_type=f32) + bias[...]
    rates = (jnp.minimum(x, 0.0) - jnp.log1p(jnp.exp(-jnp.abs(x)))) / decay_temper
    wide = lax.broadcasted_iota(jnp.int32, (2, LANES), 1) // HEAD
    pick = (wide == lax.broadcasted_iota(jnp.int32, (2, LANES), 0)).astype(f32)
    rates = rates + lax.dot_general(
        extra[...], pick, (((0,), (0,)), ((), ())), precision=highest, preferred_element_type=f32
    )
    r = lax.broadcasted_iota(jnp.int32, (BLOCK, BLOCK), 0)
    c = lax.broadcasted_iota(jnp.int32, (BLOCK, BLOCK), 1)
    lower = (r >= c).astype(f32)
    half = lax.broadcasted_iota(jnp.int32, (HEAD, LANES), 1) < HEAD
    state = jnp.zeros((HEAD, LANES), f32)
    before = jnp.zeros((1, LANES), f32)
    for n in range(tokens // BLOCK):
        at = slice(n * BLOCK, (n + 1) * BLOCK)
        total = jnp.dot(lower, rates[at], precision=highest, preferred_element_type=f32)
        sums[at] = total
        final = total[BLOCK - 1 :]
        pairs = lax.dot_general(
            values[at],
            keys[at] * jnp.exp(final - total),
            (((0,), (0,)), ((), ())),
            precision=highest,
            preferred_element_type=f32,
        )
        prior[at] = state
        opening[n : n + 1] = before
        state = jnp.exp(final) * state + heads_of(pairs, half)
        before = before + final
    run[:HEAD] = state.astype(bf16)
    row = lax.broadcasted_iota(jnp.int32, (HALO, LANES), 0)
    logs = jnp.zeros((HALO, LANES), f32)
    for j, part in enumerate(thirds(before)):
        logs = jnp.where(row == j, part.astype(f32), logs)
    run[HEAD : HEAD + HALO] = logs.astype(bf16)


def finish_kernel(
    sp,
    tp,
    runs,
    start,
    parts,
    inverse,
    pool,
    keys,
    values,
    sums,
    prior,
    opening,
    gain,
    pool_weight,
    pool_scale,
    mine,
):
    inv = inverse[...]
    tokens = inv.shape[0]
    place = sp[0]
    state = start[...]
    for j in range(runs.shape[0]):
        came = runs[j].astype(f32)
        log = came[HEAD : HEAD + 1] + came[HEAD + 1 : HEAD + 2] + came[HEAD + 2 : HEAD + 3]
        state = jnp.where(j < place, jnp.exp(log) * state + came[:HEAD], state)
    queries = projected(parts, inv, 0).astype(f32) * HEAD ** (-0.5)
    outgate = projected(parts, inv, 1).astype(f32)
    half = lax.broadcasted_iota(jnp.int32, (HEAD, LANES), 1) < HEAD
    r = lax.broadcasted_iota(jnp.int32, (2 * BLOCK, BLOCK), 0) % BLOCK
    c = lax.broadcasted_iota(jnp.int32, (2 * BLOCK, BLOCK), 1)
    causal = r >= c

    def split(x):
        return jnp.concatenate([jnp.where(half, x, 0.0), jnp.where(half, 0.0, x)], axis=0)

    last = (((1,), (1,)), ((), ()))
    for n in range(tokens // BLOCK):
        at = slice(n * BLOCK, (n + 1) * BLOCK)
        total = sums[at]
        middle = total[BLOCK // 2 - 1 : BLOCK // 2]
        q = queries[at]
        scores = lax.dot_general(
            split(q * jnp.exp(total - middle)),
            keys[at] * jnp.exp(middle - total),
            last,
            precision=highest,
            preferred_element_type=f32,
        )
        scores = jnp.where(causal, scores, 0.0)
        within = jnp.dot(scores, values[at], precision=highest, preferred_element_type=f32)
        begin = prior[at] + jnp.exp(opening[n : n + 1]) * state
        carried = lax.dot_general(
            split(q * jnp.exp(total)),
            jnp.concatenate([begin, begin], axis=0),
            last,
            precision=highest,
            preferred_element_type=f32,
        )
        raw = heads_of(within + carried, half)
        square = raw * raw
        first = jnp.sum(jnp.where(half, square, 0.0), axis=1, keepdims=True)
        second = jnp.sum(jnp.where(half, 0.0, square), axis=1, keepdims=True)
        mean = jnp.where(half, first, second) / HEAD
        g = outgate[at]
        scaled = raw * lax.rsqrt(mean + norm_eps) * gain[...]
        done = (scaled * (g / (1.0 + jnp.exp(-g)))).astype(bf16)
        for to in range(mine.shape[0]):
            mine[to, at, LANES:] = done

    current = pool[...].astype(f32)
    previous = runs[jnp.maximum(place - 1, 0), RUN_ROWS - HALO :].astype(f32)
    previous = jnp.where(place > 0, previous, 0.0)
    extended = jnp.concatenate([previous, current], axis=0)

    def back(x, by):
        return x + pltpu.roll(x, by, 0)

    two = back(extended, 1)
    four = back(two, 2)
    eight = back(four, 4)
    sixteen = back(eight, 8)
    level = tp[0] % 4
    chosen = jnp.where(
        level == 0, two, jnp.where(level == 1, four, jnp.where(level == 2, eight, sixteen))
    )[HALO:]
    window = jnp.where(
        level == 0, 2.0, jnp.where(level == 1, 4.0, jnp.where(level == 2, 8.0, 16.0))
    )
    position = place * tokens + lax.broadcasted_iota(jnp.int32, (tokens, LANES), 0)
    counts = jnp.minimum(position.astype(f32) + 1.0, window)
    deviation = (chosen / counts - current).astype(bf16)
    mixture = jnp.dot(deviation, pool_weight[...], preferred_element_type=f32)
    done = (mixture * pool_scale[...]).astype(bf16)
    for to in range(mine.shape[0]):
        mine[to, :, :LANES] = done


def output_kernel(core, z, rows, *rest):
    *before, out, held, arrived = rest
    copies = []
    for x in range(z.shape[0]):
        at = pl.ds(pl.multiple_of((2 * x + core[0]) * LANES, LANES), LANES)
        copies.append(pltpu.make_async_copy(rows.at[:, at], held.at[x], arrived.at[x]))
        copies[x].start()
    total = jnp.zeros(out.shape, f32)
    for b in before:
        total = b[...]
    for x in range(z.shape[0]):
        copies[x].wait()
        w = jnp.concatenate(
            [
                jnp.concatenate([held[x, f, :, :LANES], held[x, f, :, LANES:]], axis=0)
                for f in range(rows.shape[0])
            ],
            axis=1,
        )
        total = total + jnp.dot(z[x], w, preferred_element_type=f32)
    out[...] = total.astype(out.dtype)


def output(core, z, rows, before, out):
    vmem = pl.BlockSpec(memory_space=pltpu.VMEM)
    steps = z.shape[0]
    parts, _, width = rows.shape
    return pl.pallas_call(
        output_kernel,
        in_specs=[
            pl.BlockSpec(memory_space=pltpu.SMEM),
            vmem,
            pl.BlockSpec(memory_space=pl.ANY),
        ]
        + [vmem] * len(before),
        out_specs=vmem,
        out_shape=out,
        scratch_shapes=[
            pltpu.VMEM((steps, parts, LANES, width), bf16),
            pltpu.SemaphoreType.DMA((steps,)),
        ],
    )(core, near(z), rows, *before)


def body(
    activations,
    input_norm_gain,
    pooling_channel_weight,
    query_projection_weight,
    key_projection_weight,
    value_projection_weight,
    output_gate_weight,
    decay_first_factor,
    decay_second_factor,
    decay_gate_bias,
    decay_extra_log,
    head_norm_gain,
    starting_state,
    pooling_group_weight,
    pooling_channel_scale,
    pooling_output_rows,
    attention_output_rows,
):
    _, tokens, width = activations.shape
    rows = key_projection_weight.shape[0]
    columns = pooling_output_rows.shape[1]
    own = lax.axis_index("fs").astype(jnp.int32).reshape(1)
    tp = lax.axis_index("tp").astype(jnp.int32)
    early, late = call(
        pack_kernel,
        [struct((rows, 3 * LANES + HEAD), bf16), struct((rows, 4 * LANES), bf16)],
        "pack",
        own,
        key_projection_weight,
        value_projection_weight,
        pooling_channel_weight,
        decay_first_factor,
        query_projection_weight,
        output_gate_weight,
        pooling_output_rows,
        attention_output_rows,
    )
    late, early, activations = lax.optimization_barrier((late, early, activations))
    late = lax.all_gather(late, "sp", axis=0, tiled=True)
    x, inverse = prepare(activations.reshape(tokens, width), input_norm_gain.reshape(1, width))
    x = lax.all_to_all(x, "fs", 0, 0)
    early = lax.all_gather(early, "sp").reshape(-1, early.shape[1])
    inverse = near(inverse)
    parts, x = early_partials(near(x), near(early))
    parts = lax.all_to_all(parts, "fs", 0, 0)
    wide = pltpu.VMEM((tokens, LANES), f32)
    keys, values, pool, sums, prior, opening, run = call(
        local_kernel,
        [
            wide,
            wide,
            pltpu.VMEM((tokens, LANES), bf16),
            wide,
            wide,
            pltpu.VMEM((tokens // BLOCK, LANES), f32),
            struct((RUN_ROWS, LANES), bf16),
        ],
        "local",
        near(parts),
        inverse,
        decay_second_factor,
        decay_gate_bias.reshape(1, LANES),
        decay_extra_log,
        scalars=0,
    )
    start = starting_state[0].transpose(2, 0, 1).reshape(HEAD, LANES)
    late, run = lax.optimization_barrier((late, run))
    late, quarter = late_partials(near(x), late)
    late, quarter, run = lax.optimization_barrier((late, quarter, run))
    out_rows = lax.all_gather(quarter, "fs")
    late = lax.all_to_all(late, "fs", 0, 0)
    runs = lax.all_gather(run, "sp")
    peers = lax.axis_size("tp")
    (mine,) = call(
        finish_kernel,
        [struct((peers // 2, tokens, 2 * LANES), bf16)],
        "finish",
        lax.axis_index("sp").astype(jnp.int32).reshape(1),
        tp.reshape(1),
        near(runs),
        near(start),
        near(late),
        inverse,
        near(pool),
        near(keys),
        near(values),
        near(sums),
        near(prior),
        near(opening),
        head_norm_gain.reshape(1, LANES),
        pooling_group_weight[0],
        pooling_channel_scale.reshape(1, LANES),
        scalars=2,
    )
    groups = [[c + 2 * x for x in range(peers // 2)] for c in range(2)]
    same = lax.all_to_all(mine, "tp", 0, 0, axis_index_groups=groups)
    same, out_rows = lax.optimization_barrier((same, out_rows))
    other = lax.ppermute(same, "tp", [(i, i ^ 1) for i in range(peers)])
    core = (tp & 1).reshape(1)
    half = output(core, same, out_rows, (), pltpu.VMEM((tokens, columns), f32))
    result = output(1 - core, other, out_rows, (near(half),), struct((tokens, columns), bf16))
    return result[None]


def solution(mesh):
    in_specs = (
        P("fs", "sp", None),
        P(),
        P(("sp", "fs"), "tp"),
        P(("sp", "fs"), "tp"),
        P(("sp", "fs"), "tp"),
        P(("sp", "fs"), "tp"),
        P(("sp", "fs"), "tp"),
        P(("sp", "fs"), None),
        P(None, "tp"),
        P("tp"),
        P("tp", "sp"),
        P("tp"),
        P("fs", "tp", None, None),
        P("tp", None, None),
        P("tp"),
        P("sp", "tp"),
        P("sp", "tp"),
    )
    out_specs = P("fs", "sp", "tp")

    return jax.shard_map(body, mesh=mesh, in_specs=in_specs, out_specs=out_specs, check_vma=False)
```

```python
import jax
import jax.numpy as jnp
from jax import lax
from jax.experimental import pallas as pl
from jax.experimental.pallas import tpu as pltpu
from jax.sharding import PartitionSpec as P


BLOCK = 64
HEAD = 64
LANES = 128
HALO = 16
RUN_ROWS = 96
norm_eps = 1e-06
decay_temper = 16.0
highest = lax.Precision.HIGHEST
f32 = jnp.float32
bf16 = jnp.bfloat16
limit = pltpu.CompilerParams(vmem_limit_bytes=24 << 20)


def call(kernel, outs, name, *args, scalars=1, aliases={}):
    smem = pl.BlockSpec(memory_space=pltpu.SMEM)
    vmem = pl.BlockSpec(memory_space=pltpu.VMEM)
    return pl.pallas_call(
        kernel,
        in_specs=[smem] * scalars + [vmem] * (len(args) - scalars),
        out_specs=[vmem] * len(outs),
        out_shape=outs,
        input_output_aliases=aliases,
        compiler_params=limit if name in ("local", "finish") else None,
    )(*args)


def near(x):
    return pltpu.with_memory_space_constraint(x, pltpu.VMEM)


def struct(shape, dtype):
    return jax.ShapeDtypeStruct(shape, dtype)


def pack_kernel(own, key, value, pool, low, query, gate, pool_rows, state_rows, early, late):
    at = 0
    for r in (key, value, pool, low):
        early[:, at : at + r.shape[1]] = r[...]
        at += r.shape[1]
    mine = pl.ds(pl.multiple_of(own[0] * LANES, LANES), LANES)
    blocks = (query[...], gate[...], pool_rows[:, mine], state_rows[:, mine])
    for j, block in enumerate(blocks):
        late[:, j * LANES : (j + 1) * LANES] = block


def prep_kernel(act, gain, x, inverse, held, arrived):
    tokens, width = act.shape
    rows = tokens // 4
    copies = []
    for c in range(4):
        at = pl.ds(c * rows, rows)
        copies.append(pltpu.make_async_copy(act.at[at], held.at[at], arrived.at[c]))
        copies[c].start()
    half = lax.broadcasted_iota(jnp.int32, (rows, LANES), 1) < HEAD
    for c in range(4):
        copies[c].wait()
        block = pl.ds(c * rows, rows)
        squares = jnp.zeros((rows, LANES), f32)
        for p in range(width // 512):
            tiles = []
            for q in range(4):
                at = p * 512 + q * LANES
                t = held[block, at : at + LANES].astype(f32)
                squares = squares + t * t
                tiles.append(t * gain[:, at : at + LANES])
            to = slice(p * LANES, (p + 1) * LANES)
            for j, (a, b) in enumerate(((tiles[0], tiles[2]), (tiles[1], tiles[3]))):
                x[2 * j, block, to] = jnp.where(half, a, pltpu.roll(b, HEAD, 1)).astype(bf16)
                x[2 * j + 1, block, to] = jnp.where(half, pltpu.roll(a, HEAD, 1), b).astype(bf16)
        total = jnp.sum(squares, axis=1, keepdims=True)
        inverse[block] = jnp.broadcast_to(lax.rsqrt(total / width + norm_eps), (rows, LANES))


def prepare(act, gain):
    tokens, width = act.shape
    vmem = pl.BlockSpec(memory_space=pltpu.VMEM)
    return pl.pallas_call(
        prep_kernel,
        in_specs=[pl.BlockSpec(memory_space=pl.ANY), vmem],
        out_specs=[vmem, vmem],
        out_shape=[struct((4, tokens, width // 4), bf16), struct((tokens, LANES), f32)],
        scratch_shapes=[pltpu.VMEM((tokens, width), bf16), pltpu.SemaphoreType.DMA((4,))],
        name="prep",
    )(act, gain)


def thirds(x):
    first = x.astype(bf16)
    left = x - first.astype(f32)
    second = left.astype(bf16)
    return first, second, (left - second.astype(f32)).astype(bf16)


def early_kernel(x, w, out, same_x, made, left):
    tokens = x.shape[1]
    half = lax.broadcasted_iota(jnp.int32, (tokens // 2, LANES), 1) < HEAD
    weight = w[...]
    copies = []
    for f in range(4):
        p = jnp.dot(x[f], weight, preferred_element_type=f32)
        for j in range(3):
            at = slice(j * tokens, (j + 1) * tokens)
            made[f, at] = p[:, j * LANES : (j + 1) * LANES].astype(bf16)
        d = jnp.concatenate([p[:, 3 * LANES :], p[:, 3 * LANES :]], axis=1)
        d = jnp.where(half, d[: tokens // 2], d[tokens // 2 :])
        made[f, 3 * tokens :] = d.astype(bf16)
        copies.append(pltpu.make_async_copy(made.at[f], out.at[f], left.at[f]))
        copies[f].start()
    for c in copies:
        c.wait()


def late_kernel(x, w, out, quarter, held, made, arrived, left):
    tokens = x.shape[1]
    columns = 2 * LANES
    into = pltpu.make_async_copy(w, held, arrived)
    into.start()
    into.wait()
    across = pltpu.make_async_copy(held.at[:, columns:], quarter, left.at[4])
    across.start()
    weight = held[:, :columns]
    copies = [across]
    for f in range(4):
        p = jnp.dot(x[f], weight, preferred_element_type=f32)
        made[f, :tokens] = p[:, :LANES].astype(bf16)
        made[f, tokens:] = p[:, LANES:].astype(bf16)
        copies.append(pltpu.make_async_copy(made.at[f], out.at[f], left.at[f]))
        copies[f + 1].start()
    for c in copies:
        c.wait()


def early_partials(x, w):
    _, tokens, _ = x.shape
    vmem = pl.BlockSpec(memory_space=pltpu.VMEM)
    anywhere = pl.BlockSpec(memory_space=pl.ANY)
    shape = (4, tokens * w.shape[1] // LANES, LANES)
    return pl.pallas_call(
        early_kernel,
        in_specs=[vmem, vmem],
        out_specs=[anywhere, vmem],
        out_shape=[struct(shape, bf16), pltpu.VMEM(x.shape, bf16)],
        scratch_shapes=[pltpu.VMEM(shape, bf16), pltpu.SemaphoreType.DMA((4,))],
        input_output_aliases={0: 1},
        compiler_params=limit,
        name="early_parts",
    )(x, w)


def late_partials(x, w):
    _, tokens, depth = x.shape
    vmem = pl.BlockSpec(memory_space=pltpu.VMEM)
    anywhere = pl.BlockSpec(memory_space=pl.ANY)
    shape = (4, 2 * tokens, LANES)
    return pl.pallas_call(
        late_kernel,
        in_specs=[vmem, pl.BlockSpec(memory_space=pltpu.HBM)],
        out_specs=[anywhere, anywhere],
        out_shape=[struct(shape, bf16), struct((depth, w.shape[1] - 2 * LANES), bf16)],
        scratch_shapes=[
            pltpu.VMEM(w.shape, bf16),
            pltpu.VMEM(shape, bf16),
            pltpu.SemaphoreType.DMA,
            pltpu.SemaphoreType.DMA((5,)),
        ],
        compiler_params=limit,
        name="late_parts",
    )(x, pltpu.with_memory_space_constraint(w, pltpu.HBM))


def total_of(parts, at, rows):
    s = parts[0, at : at + rows].astype(f32)
    for k in (1, 2, 3):
        s = s + parts[k, at : at + rows].astype(f32)
    return s


def projected(parts, inverse, j):
    tokens = inverse.shape[0]
    return (total_of(parts, j * tokens, tokens) * inverse).astype(bf16)


def heads_of(x, half):
    return jnp.where(half, x[:HEAD], x[HEAD:])


def thirds(x):
    first = x.astype(bf16)
    left = x - first.astype(f32)
    second = left.astype(bf16)
    return first, second, (left - second.astype(f32)).astype(bf16)


def local_kernel(
    parts, inverse, second, bias, extra, keys, values, pool, sums, prior, opening, spread
):
    inv = inverse[...]
    tokens = inv.shape[0]
    keys[...] = projected(parts, inv, 0).astype(f32)
    values[...] = projected(parts, inv, 1).astype(f32)
    pooled = projected(parts, inv, 2)
    pool[...] = pooled
    both = total_of(parts, 3 * tokens, tokens // 2)
    low = jnp.concatenate([both[:, :HEAD], both[:, HEAD:]], axis=0)
    low = (low * inv[:, :HEAD]).astype(bf16)
    x = jnp.dot(low, second[...], preferred_element_type=f32) + bias[...]
    rates = (jnp.minimum(x, 0.0) - jnp.log1p(jnp.exp(-jnp.abs(x)))) / decay_temper
    wide = lax.broadcasted_iota(jnp.int32, (2, LANES), 1) // HEAD
    pick = (wide == lax.broadcasted_iota(jnp.int32, (2, LANES), 0)).astype(f32)
    rates = rates + lax.dot_general(
        extra[...], pick, (((0,), (0,)), ((), ())), precision=highest, preferred_element_type=f32
    )
    r = lax.broadcasted_iota(jnp.int32, (BLOCK, BLOCK), 0)
    c = lax.broadcasted_iota(jnp.int32, (BLOCK, BLOCK), 1)
    lower = (r >= c).astype(f32)
    half = lax.broadcasted_iota(jnp.int32, (HEAD, LANES), 1) < HEAD
    state = jnp.zeros((HEAD, LANES), f32)
    before = jnp.zeros((1, LANES), f32)
    for n in range(tokens // BLOCK):
        at = slice(n * BLOCK, (n + 1) * BLOCK)
        total = jnp.dot(lower, rates[at], precision=highest, preferred_element_type=f32)
        sums[at] = total
        final = total[BLOCK - 1 :]
        pairs = lax.dot_general(
            values[at],
            keys[at] * jnp.exp(final - total),
            (((0,), (0,)), ((), ())),
            precision=highest,
            preferred_element_type=f32,
        )
        prior[at] = state
        opening[n : n + 1] = before
        state = jnp.exp(final) * state + heads_of(pairs, half)
        before = before + final
    for to in range(spread.shape[0]):
        write_run(spread, to, state, before, pooled[tokens - HALO :])


def write_run(out, to, state, log, tail):
    row = lax.broadcasted_iota(jnp.int32, (HALO, LANES), 0)
    logs = jnp.zeros((HALO, LANES), f32)
    for j, part in enumerate(thirds(log)):
        logs = jnp.where(row == j, part.astype(f32), logs)
    out[to, :HEAD] = state.astype(bf16)
    out[to, HEAD : HEAD + HALO] = logs.astype(bf16)
    out[to, HEAD + HALO :] = tail


def read_run(came):
    came = came.astype(f32)
    log = came[HEAD : HEAD + 1] + came[HEAD + 1 : HEAD + 2] + came[HEAD + 2 : HEAD + 3]
    return came[:HEAD], log


def quad_kernel(sp, quad, total, within, log_within, previous):
    place = sp[0] % 4
    state = jnp.zeros((HEAD, LANES), f32)
    log = jnp.zeros((1, LANES), f32)
    for j in range(4):

        @pl.when(place == j)
        def _(state=state, log=log):
            within[...] = state
            log_within[...] = jnp.broadcast_to(log, log_within.shape)

        s, decay = read_run(quad[j])
        state = jnp.exp(decay) * state + s
        log = log + decay
    write_run(total, 0, state, log, quad[3, HEAD + HALO :])
    previous[...] = quad[jnp.maximum(place - 1, 0), HEAD + HALO :]


def finish_kernel(
    sp,
    tp,
    runs,
    within_quad,
    log_within,
    previous,
    start,
    parts,
    inverse,
    pool,
    keys,
    values,
    sums,
    prior,
    opening,
    gain,
    pool_weight,
    pool_scale,
    mine,
):
    inv = inverse[...]
    tokens = inv.shape[0]
    place = sp[0]
    state = start[...]
    for j in range(runs.shape[0]):
        came, log = read_run(runs[j])
        state = jnp.where(j < place // 4, jnp.exp(log) * state + came, state)
    state = jnp.exp(log_within[:1]) * state + within_quad[...]
    queries = projected(parts, inv, 0).astype(f32) * HEAD ** (-0.5)
    outgate = projected(parts, inv, 1).astype(f32)
    half = lax.broadcasted_iota(jnp.int32, (HEAD, LANES), 1) < HEAD
    r = lax.broadcasted_iota(jnp.int32, (2 * BLOCK, BLOCK), 0) % BLOCK
    c = lax.broadcasted_iota(jnp.int32, (2 * BLOCK, BLOCK), 1)
    causal = r >= c

    def split(x):
        return jnp.concatenate([jnp.where(half, x, 0.0), jnp.where(half, 0.0, x)], axis=0)

    last = (((1,), (1,)), ((), ()))
    for n in range(tokens // BLOCK):
        at = slice(n * BLOCK, (n + 1) * BLOCK)
        total = sums[at]
        middle = total[BLOCK // 2 - 1 : BLOCK // 2]
        q = queries[at]
        scores = lax.dot_general(
            split(q * jnp.exp(total - middle)),
            keys[at] * jnp.exp(middle - total),
            last,
            precision=highest,
            preferred_element_type=f32,
        )
        scores = jnp.where(causal, scores, 0.0)
        within = jnp.dot(scores, values[at], precision=highest, preferred_element_type=f32)
        begin = prior[at] + jnp.exp(opening[n : n + 1]) * state
        carried = lax.dot_general(
            split(q * jnp.exp(total)),
            jnp.concatenate([begin, begin], axis=0),
            last,
            precision=highest,
            preferred_element_type=f32,
        )
        raw = heads_of(within + carried, half)
        square = raw * raw
        first = jnp.sum(jnp.where(half, square, 0.0), axis=1, keepdims=True)
        second = jnp.sum(jnp.where(half, 0.0, square), axis=1, keepdims=True)
        mean = jnp.where(half, first, second) / HEAD
        g = outgate[at]
        scaled = raw * lax.rsqrt(mean + norm_eps) * gain[...]
        done = (scaled * (g / (1.0 + jnp.exp(-g)))).astype(bf16)
        for to in range(mine.shape[0]):
            mine[to, at, LANES:] = done

    current = pool[...].astype(f32)
    outside = runs[jnp.maximum(place // 4 - 1, 0), HEAD + HALO :].astype(f32)
    outside = jnp.where(place >= 4, outside, 0.0)
    before = jnp.where(place % 4 > 0, previous[...].astype(f32), outside)
    extended = jnp.concatenate([before, current], axis=0)

    def back(x, by):
        return x + pltpu.roll(x, by, 0)

    two = back(extended, 1)
    four = back(two, 2)
    eight = back(four, 4)
    sixteen = back(eight, 8)
    level = tp[0] % 4
    chosen = jnp.where(
        level == 0, two, jnp.where(level == 1, four, jnp.where(level == 2, eight, sixteen))
    )[HALO:]
    window = jnp.where(
        level == 0, 2.0, jnp.where(level == 1, 4.0, jnp.where(level == 2, 8.0, 16.0))
    )
    position = place * tokens + lax.broadcasted_iota(jnp.int32, (tokens, LANES), 0)
    counts = jnp.minimum(position.astype(f32) + 1.0, window)
    deviation = (chosen / counts - current).astype(bf16)
    mixture = jnp.dot(deviation, pool_weight[...], preferred_element_type=f32)
    done = (mixture * pool_scale[...]).astype(bf16)
    for to in range(mine.shape[0]):
        mine[to, :, :LANES] = done


def output_kernel(core, z, rows, *rest):
    *before, out, held, arrived = rest
    copies = []
    for x in range(z.shape[0]):
        at = pl.ds(pl.multiple_of((2 * x + core[0]) * LANES, LANES), LANES)
        copies.append(pltpu.make_async_copy(rows.at[:, at], held.at[x], arrived.at[x]))
        copies[x].start()
    total = jnp.zeros(out.shape, f32)
    for b in before:
        total = b[...]
    for x in range(z.shape[0]):
        copies[x].wait()
        w = jnp.concatenate(
            [
                jnp.concatenate([held[x, f, :, :LANES], held[x, f, :, LANES:]], axis=0)
                for f in range(rows.shape[0])
            ],
            axis=1,
        )
        total = total + jnp.dot(z[x], w, preferred_element_type=f32)
    out[...] = total.astype(out.dtype)


def output(core, z, rows, before, out):
    vmem = pl.BlockSpec(memory_space=pltpu.VMEM)
    steps = z.shape[0]
    parts, _, width = rows.shape
    return pl.pallas_call(
        output_kernel,
        in_specs=[
            pl.BlockSpec(memory_space=pltpu.SMEM),
            vmem,
            pl.BlockSpec(memory_space=pl.ANY),
        ]
        + [vmem] * len(before),
        out_specs=vmem,
        out_shape=out,
        scratch_shapes=[
            pltpu.VMEM((steps, parts, LANES, width), bf16),
            pltpu.SemaphoreType.DMA((steps,)),
        ],
    )(core, near(z), rows, *before)


def body(
    activations,
    input_norm_gain,
    pooling_channel_weight,
    query_projection_weight,
    key_projection_weight,
    value_projection_weight,
    output_gate_weight,
    decay_first_factor,
    decay_second_factor,
    decay_gate_bias,
    decay_extra_log,
    head_norm_gain,
    starting_state,
    pooling_group_weight,
    pooling_channel_scale,
    pooling_output_rows,
    attention_output_rows,
):
    _, tokens, width = activations.shape
    rows = key_projection_weight.shape[0]
    columns = pooling_output_rows.shape[1]
    own = lax.axis_index("fs").astype(jnp.int32).reshape(1)
    tp = lax.axis_index("tp").astype(jnp.int32)
    early, late = call(
        pack_kernel,
        [struct((rows, 3 * LANES + HEAD), bf16), struct((rows, 4 * LANES), bf16)],
        "pack",
        own,
        key_projection_weight,
        value_projection_weight,
        pooling_channel_weight,
        decay_first_factor,
        query_projection_weight,
        output_gate_weight,
        pooling_output_rows,
        attention_output_rows,
    )
    late, early, activations = lax.optimization_barrier((late, early, activations))
    late = lax.all_gather(late, "sp", axis=0, tiled=True)
    x, inverse = prepare(activations.reshape(tokens, width), input_norm_gain.reshape(1, width))
    x = lax.all_to_all(x, "fs", 0, 0)
    early = lax.all_gather(early, "sp").reshape(-1, early.shape[1])
    inverse = near(inverse)
    parts, x = early_partials(near(x), near(early))
    parts = lax.all_to_all(parts, "fs", 0, 0)
    wide = pltpu.VMEM((tokens, LANES), f32)
    keys, values, pool, sums, prior, opening, spread = call(
        local_kernel,
        [
            wide,
            wide,
            pltpu.VMEM((tokens, LANES), bf16),
            wide,
            wide,
            pltpu.VMEM((tokens // BLOCK, LANES), f32),
            struct((4, RUN_ROWS, LANES), bf16),
        ],
        "local",
        near(parts),
        inverse,
        decay_second_factor,
        decay_gate_bias.reshape(1, LANES),
        decay_extra_log,
        scalars=0,
    )
    start = starting_state[0].transpose(2, 0, 1).reshape(HEAD, LANES)
    quads = [[4 * a + b for b in range(4)] for a in range(lax.axis_size("sp") // 4)]
    late, _ = lax.optimization_barrier((late, spread))
    quad = lax.all_to_all(spread, "sp", 0, 0, axis_index_groups=quads)
    late, quarter = late_partials(near(x), late)
    _, _, quad = lax.optimization_barrier((late, quarter, quad))
    out_rows = lax.all_gather(quarter, "fs")
    late = lax.all_to_all(late, "fs", 0, 0)
    sp = lax.axis_index("sp").astype(jnp.int32).reshape(1)
    total, within, log_within, previous = call(
        quad_kernel,
        [
            struct((1, RUN_ROWS, LANES), bf16),
            pltpu.VMEM((HEAD, LANES), f32),
            pltpu.VMEM((8, LANES), f32),
            pltpu.VMEM((HALO, LANES), bf16),
        ],
        "quad_total",
        sp,
        near(quad),
    )
    strided = [list(column) for column in zip(*quads)]
    runs = lax.all_gather(total[0], "sp", axis_index_groups=strided)
    peers = lax.axis_size("tp")
    (mine,) = call(
        finish_kernel,
        [struct((peers // 2, tokens, 2 * LANES), bf16)],
        "finish",
        sp,
        tp.reshape(1),
        near(runs),
        near(within),
        near(log_within),
        near(previous),
        near(start),
        near(late),
        inverse,
        near(pool),
        near(keys),
        near(values),
        near(sums),
        near(prior),
        near(opening),
        head_norm_gain.reshape(1, LANES),
        pooling_group_weight[0],
        pooling_channel_scale.reshape(1, LANES),
        scalars=2,
    )
    groups = [[c + 2 * x for x in range(peers // 2)] for c in range(2)]
    same = lax.all_to_all(mine, "tp", 0, 0, axis_index_groups=groups)
    same, out_rows = lax.optimization_barrier((same, out_rows))
    other = lax.ppermute(same, "tp", [(i, i ^ 1) for i in range(peers)])
    core = (tp & 1).reshape(1)
    half = output(core, same, out_rows, (), pltpu.VMEM((tokens, columns), f32))
    result = output(1 - core, other, out_rows, (near(half),), struct((tokens, columns), bf16))
    return result[None]


def solution(mesh):
    in_specs = (
        P("fs", "sp", None),
        P(),
        P(("sp", "fs"), "tp"),
        P(("sp", "fs"), "tp"),
        P(("sp", "fs"), "tp"),
        P(("sp", "fs"), "tp"),
        P(("sp", "fs"), "tp"),
        P(("sp", "fs"), None),
        P(None, "tp"),
        P("tp"),
        P("tp", "sp"),
        P("tp"),
        P("fs", "tp", None, None),
        P("tp", None, None),
        P("tp"),
        P("sp", "tp"),
        P("sp", "tp"),
    )
    out_specs = P("fs", "sp", "tp")

    return jax.shard_map(body, mesh=mesh, in_specs=in_specs, out_specs=out_specs, check_vma=False)
```

```python
import jax
import jax.numpy as jnp
from jax import lax
from jax.experimental import pallas as pl
from jax.experimental.pallas import tpu as pltpu
from jax.sharding import PartitionSpec as P


BLOCK = 64
HEAD = 64
LANES = 128
HALO = 16
RUN_ROWS = 96
norm_eps = 1e-06
decay_temper = 16.0
highest = lax.Precision.HIGHEST
f32 = jnp.float32
bf16 = jnp.bfloat16
limit = pltpu.CompilerParams(vmem_limit_bytes=24 << 20)


def call(kernel, outs, name, *args, scalars=1, aliases={}):
    smem = pl.BlockSpec(memory_space=pltpu.SMEM)
    vmem = pl.BlockSpec(memory_space=pltpu.VMEM)
    return pl.pallas_call(
        kernel,
        in_specs=[smem] * scalars + [vmem] * (len(args) - scalars),
        out_specs=[vmem] * len(outs),
        out_shape=outs,
        input_output_aliases=aliases,
        compiler_params=limit if name in ("local", "finish") else None,
    )(*args)


def near(x):
    return pltpu.with_memory_space_constraint(x, pltpu.VMEM)


def struct(shape, dtype):
    return jax.ShapeDtypeStruct(shape, dtype)


def pack_late_kernel(own, query, gate, pool_rows, state_rows, late):
    mine = pl.ds(pl.multiple_of(own[0] * LANES, LANES), LANES)
    blocks = (query[...], gate[...], pool_rows[:, mine], state_rows[:, mine])
    for j, block in enumerate(blocks):
        late[:, j * LANES : (j + 1) * LANES] = block


def prep_kernel(
    act, gain, key, value, pool, low, x, inverse, early, held, made, arrived, left
):
    tokens, width = act.shape
    rows = tokens // 4
    copies = []
    for c in range(4):
        at = pl.ds(c * rows, rows)
        copies.append(pltpu.make_async_copy(act.at[at], held.at[at], arrived.at[c]))
        copies[c].start()
    at = 0
    for r in (key, value, pool, low):
        early[:, at : at + r.shape[1]] = r[...]
        at += r.shape[1]
    half = lax.broadcasted_iota(jnp.int32, (rows, LANES), 1) < HEAD
    out = []
    for c in range(4):
        copies[c].wait()
        block = pl.ds(c * rows, rows)
        squares = jnp.zeros((rows, LANES), f32)
        for p in range(width // 512):
            tiles = []
            for q in range(4):
                at = p * 512 + q * LANES
                t = held[block, at : at + LANES].astype(f32)
                squares = squares + t * t
                tiles.append(t * gain[:, at : at + LANES])
            to = slice(p * LANES, (p + 1) * LANES)
            for j, (a, b) in enumerate(((tiles[0], tiles[2]), (tiles[1], tiles[3]))):
                made[2 * j, block, to] = jnp.where(half, a, pltpu.roll(b, HEAD, 1)).astype(bf16)
                made[2 * j + 1, block, to] = jnp.where(half, pltpu.roll(a, HEAD, 1), b).astype(bf16)
        for f in range(4):
            out.append(
                pltpu.make_async_copy(made.at[f, block], x.at[f, block], left.at[4 * c + f])
            )
            out[-1].start()
        total = jnp.sum(squares, axis=1, keepdims=True)
        inverse[block] = jnp.broadcast_to(lax.rsqrt(total / width + norm_eps), (rows, LANES))
    for o in out:
        o.wait()


def prepare(act, gain, *weights):
    tokens, width = act.shape
    vmem = pl.BlockSpec(memory_space=pltpu.VMEM)
    anywhere = pl.BlockSpec(memory_space=pl.ANY)
    shape = (4, tokens, width // 4)
    columns = sum(w.shape[1] for w in weights)
    return pl.pallas_call(
        prep_kernel,
        in_specs=[anywhere] + [vmem] * (1 + len(weights)),
        out_specs=[anywhere, vmem, vmem],
        out_shape=[
            struct(shape, bf16),
            struct((tokens, LANES), f32),
            struct((weights[0].shape[0], columns), bf16),
        ],
        scratch_shapes=[
            pltpu.VMEM((tokens, width), bf16),
            pltpu.VMEM(shape, bf16),
            pltpu.SemaphoreType.DMA((4,)),
            pltpu.SemaphoreType.DMA((16,)),
        ],
        name="prep",
    )(act, gain, *weights)


def early_kernel(x, w, out, same_x, made, left):
    tokens = x.shape[1]
    half = lax.broadcasted_iota(jnp.int32, (tokens // 2, LANES), 1) < HEAD
    weight = w[...]
    copies = []
    for f in range(4):
        p = jnp.dot(x[f], weight, preferred_element_type=f32)
        for j in range(3):
            at = slice(j * tokens, (j + 1) * tokens)
            made[f, at] = p[:, j * LANES : (j + 1) * LANES].astype(bf16)
        d = jnp.concatenate([p[:, 3 * LANES :], p[:, 3 * LANES :]], axis=1)
        d = jnp.where(half, d[: tokens // 2], d[tokens // 2 :])
        made[f, 3 * tokens :] = d.astype(bf16)
        copies.append(pltpu.make_async_copy(made.at[f], out.at[f], left.at[f]))
        copies[f].start()
    for c in copies:
        c.wait()


def late_kernel(x, w, out, quarter, held, made, arrived, left):
    tokens = x.shape[1]
    columns = 2 * LANES
    depth = w.shape[0] // 4
    into = []
    for c in range(4):
        at = pl.ds(c * depth, depth)
        into.append(pltpu.make_async_copy(w.at[at], held.at[at], arrived.at[c]))
        into[c].start()
    first = jnp.zeros((tokens, columns), f32)
    for c in range(4):
        into[c].wait()
        at = slice(c * depth, (c + 1) * depth)
        first = first + jnp.dot(x[0, :, at], held[at, :columns], preferred_element_type=f32)
    across = pltpu.make_async_copy(held.at[:, columns:], quarter, left.at[4])
    across.start()
    weight = held[:, :columns]
    copies = [across]
    for f in range(4):
        p = first if f == 0 else jnp.dot(x[f], weight, preferred_element_type=f32)
        made[f, :tokens] = p[:, :LANES].astype(bf16)
        made[f, tokens:] = p[:, LANES:].astype(bf16)
        copies.append(pltpu.make_async_copy(made.at[f], out.at[f], left.at[f]))
        copies[f + 1].start()
    for c in copies:
        c.wait()


def early_partials(x, w):
    _, tokens, _ = x.shape
    vmem = pl.BlockSpec(memory_space=pltpu.VMEM)
    anywhere = pl.BlockSpec(memory_space=pl.ANY)
    shape = (4, tokens * w.shape[1] // LANES, LANES)
    return pl.pallas_call(
        early_kernel,
        in_specs=[vmem, vmem],
        out_specs=[anywhere, vmem],
        out_shape=[struct(shape, bf16), pltpu.VMEM(x.shape, bf16)],
        scratch_shapes=[pltpu.VMEM(shape, bf16), pltpu.SemaphoreType.DMA((4,))],
        input_output_aliases={0: 1},
        compiler_params=limit,
        name="early_parts",
    )(x, w)


def late_partials(x, w):
    _, tokens, depth = x.shape
    vmem = pl.BlockSpec(memory_space=pltpu.VMEM)
    anywhere = pl.BlockSpec(memory_space=pl.ANY)
    shape = (4, 2 * tokens, LANES)
    return pl.pallas_call(
        late_kernel,
        in_specs=[vmem, pl.BlockSpec(memory_space=pltpu.HBM)],
        out_specs=[anywhere, anywhere],
        out_shape=[struct(shape, bf16), struct((depth, w.shape[1] - 2 * LANES), bf16)],
        scratch_shapes=[
            pltpu.VMEM(w.shape, bf16),
            pltpu.VMEM(shape, bf16),
            pltpu.SemaphoreType.DMA((4,)),
            pltpu.SemaphoreType.DMA((5,)),
        ],
        compiler_params=limit,
        name="late_parts",
    )(x, pltpu.with_memory_space_constraint(w, pltpu.HBM))


def total_of(parts, at, rows):
    s = parts[0, at : at + rows].astype(f32)
    for k in (1, 2, 3):
        s = s + parts[k, at : at + rows].astype(f32)
    return s


def projected(parts, inverse, j):
    tokens = inverse.shape[0]
    return (total_of(parts, j * tokens, tokens) * inverse).astype(bf16)


def heads_of(x, half):
    return jnp.where(half, x[:HEAD], x[HEAD:])


def thirds(x):
    first = x.astype(bf16)
    left = x - first.astype(f32)
    second = left.astype(bf16)
    return first, second, (left - second.astype(f32)).astype(bf16)


def local_kernel(
    parts, inverse, second, bias, extra, keys, values, pool, sums, prior, opening, spread
):
    inv = inverse[...]
    tokens = inv.shape[0]
    keys[...] = projected(parts, inv, 0).astype(f32)
    values[...] = projected(parts, inv, 1).astype(f32)
    pooled = projected(parts, inv, 2)
    pool[...] = pooled
    both = total_of(parts, 3 * tokens, tokens // 2)
    low = jnp.concatenate([both[:, :HEAD], both[:, HEAD:]], axis=0)
    low = (low * inv[:, :HEAD]).astype(bf16)
    x = jnp.dot(low, second[...], preferred_element_type=f32) + bias[...]
    rates = (jnp.minimum(x, 0.0) - jnp.log1p(jnp.exp(-jnp.abs(x)))) / decay_temper
    wide = lax.broadcasted_iota(jnp.int32, (2, LANES), 1) // HEAD
    pick = (wide == lax.broadcasted_iota(jnp.int32, (2, LANES), 0)).astype(f32)
    rates = rates + lax.dot_general(
        extra[...], pick, (((0,), (0,)), ((), ())), precision=highest, preferred_element_type=f32
    )
    r = lax.broadcasted_iota(jnp.int32, (BLOCK, BLOCK), 0)
    c = lax.broadcasted_iota(jnp.int32, (BLOCK, BLOCK), 1)
    lower = (r >= c).astype(f32)
    half = lax.broadcasted_iota(jnp.int32, (HEAD, LANES), 1) < HEAD
    state = jnp.zeros((HEAD, LANES), f32)
    before = jnp.zeros((1, LANES), f32)
    for n in range(tokens // BLOCK):
        at = slice(n * BLOCK, (n + 1) * BLOCK)
        total = jnp.dot(lower, rates[at], precision=highest, preferred_element_type=f32)
        sums[at] = total
        final = total[BLOCK - 1 :]
        pairs = lax.dot_general(
            values[at],
            keys[at] * jnp.exp(final - total),
            (((0,), (0,)), ((), ())),
            precision=highest,
            preferred_element_type=f32,
        )
        prior[at] = state
        opening[n : n + 1] = before
        state = jnp.exp(final) * state + heads_of(pairs, half)
        before = before + final
    for to in range(spread.shape[0]):
        write_run(spread, to, state, before, pooled[tokens - HALO :])


def write_run(out, to, state, log, tail):
    row = lax.broadcasted_iota(jnp.int32, (HALO, LANES), 0)
    logs = jnp.zeros((HALO, LANES), f32)
    for j, part in enumerate(thirds(log)):
        logs = jnp.where(row == j, part.astype(f32), logs)
    out[to, :HEAD] = state.astype(bf16)
    out[to, HEAD : HEAD + HALO] = logs.astype(bf16)
    out[to, HEAD + HALO :] = tail


def read_run(came):
    came = came.astype(f32)
    log = came[HEAD : HEAD + 1] + came[HEAD + 1 : HEAD + 2] + came[HEAD + 2 : HEAD + 3]
    return came[:HEAD], log


def quad_kernel(sp, quad, total, within, log_within, previous):
    place = sp[0] % 4
    state = jnp.zeros((HEAD, LANES), f32)
    log = jnp.zeros((1, LANES), f32)
    for j in range(4):

        @pl.when(place == j)
        def _(state=state, log=log):
            within[...] = state
            log_within[...] = jnp.broadcast_to(log, log_within.shape)

        s, decay = read_run(quad[j])
        state = jnp.exp(decay) * state + s
        log = log + decay
    write_run(total, 0, state, log, quad[3, HEAD + HALO :])
    previous[...] = quad[jnp.maximum(place - 1, 0), HEAD + HALO :]


def finish_kernel(
    sp,
    tp,
    runs,
    within_quad,
    log_within,
    previous,
    start,
    parts,
    inverse,
    pool,
    keys,
    values,
    sums,
    prior,
    opening,
    gain,
    pool_weight,
    pool_scale,
    mine,
):
    inv = inverse[...]
    tokens = inv.shape[0]
    place = sp[0]
    state = start[...]
    for j in range(runs.shape[0]):
        came, log = read_run(runs[j])
        state = jnp.where(j < place // 4, jnp.exp(log) * state + came, state)
    state = jnp.exp(log_within[:1]) * state + within_quad[...]
    queries = projected(parts, inv, 0).astype(f32) * HEAD ** (-0.5)
    outgate = projected(parts, inv, 1).astype(f32)
    half = lax.broadcasted_iota(jnp.int32, (HEAD, LANES), 1) < HEAD
    r = lax.broadcasted_iota(jnp.int32, (2 * BLOCK, BLOCK), 0) % BLOCK
    c = lax.broadcasted_iota(jnp.int32, (2 * BLOCK, BLOCK), 1)
    causal = r >= c

    def split(x):
        return jnp.concatenate([jnp.where(half, x, 0.0), jnp.where(half, 0.0, x)], axis=0)

    last = (((1,), (1,)), ((), ()))
    for n in range(tokens // BLOCK):
        at = slice(n * BLOCK, (n + 1) * BLOCK)
        total = sums[at]
        middle = total[BLOCK // 2 - 1 : BLOCK // 2]
        q = queries[at]
        scores = lax.dot_general(
            split(q * jnp.exp(total - middle)),
            keys[at] * jnp.exp(middle - total),
            last,
            precision=highest,
            preferred_element_type=f32,
        )
        scores = jnp.where(causal, scores, 0.0)
        within = jnp.dot(scores, values[at], precision=highest, preferred_element_type=f32)
        begin = prior[at] + jnp.exp(opening[n : n + 1]) * state
        carried = lax.dot_general(
            split(q * jnp.exp(total)),
            jnp.concatenate([begin, begin], axis=0),
            last,
            precision=highest,
            preferred_element_type=f32,
        )
        raw = heads_of(within + carried, half)
        square = raw * raw
        first = jnp.sum(jnp.where(half, square, 0.0), axis=1, keepdims=True)
        second = jnp.sum(jnp.where(half, 0.0, square), axis=1, keepdims=True)
        mean = jnp.where(half, first, second) / HEAD
        g = outgate[at]
        scaled = raw * lax.rsqrt(mean + norm_eps) * gain[...]
        done = (scaled * (g / (1.0 + jnp.exp(-g)))).astype(bf16)
        for to in range(mine.shape[0]):
            mine[to, at, LANES:] = done

    current = pool[...].astype(f32)
    outside = runs[jnp.maximum(place // 4 - 1, 0), HEAD + HALO :].astype(f32)
    outside = jnp.where(place >= 4, outside, 0.0)
    before = jnp.where(place % 4 > 0, previous[...].astype(f32), outside)
    extended = jnp.concatenate([before, current], axis=0)

    def back(x, by):
        return x + pltpu.roll(x, by, 0)

    two = back(extended, 1)
    four = back(two, 2)
    eight = back(four, 4)
    sixteen = back(eight, 8)
    level = tp[0] % 4
    chosen = jnp.where(
        level == 0, two, jnp.where(level == 1, four, jnp.where(level == 2, eight, sixteen))
    )[HALO:]
    window = jnp.where(
        level == 0, 2.0, jnp.where(level == 1, 4.0, jnp.where(level == 2, 8.0, 16.0))
    )
    position = place * tokens + lax.broadcasted_iota(jnp.int32, (tokens, LANES), 0)
    counts = jnp.minimum(position.astype(f32) + 1.0, window)
    deviation = (chosen / counts - current).astype(bf16)
    mixture = jnp.dot(deviation, pool_weight[...], preferred_element_type=f32)
    done = (mixture * pool_scale[...]).astype(bf16)
    for to in range(mine.shape[0]):
        mine[to, :, :LANES] = done


def output_kernel(core, z, rows, *rest):
    *before, out, held, arrived = rest
    copies = []
    for x in range(z.shape[0]):
        at = pl.ds(pl.multiple_of((2 * x + core[0]) * LANES, LANES), LANES)
        copies.append(pltpu.make_async_copy(rows.at[:, at], held.at[x], arrived.at[x]))
        copies[x].start()
    total = jnp.zeros(out.shape, f32)
    for b in before:
        total = b[...]
    for x in range(z.shape[0]):
        copies[x].wait()
        w = jnp.concatenate(
            [
                jnp.concatenate([held[x, f, :, :LANES], held[x, f, :, LANES:]], axis=0)
                for f in range(rows.shape[0])
            ],
            axis=1,
        )
        total = total + jnp.dot(z[x], w, preferred_element_type=f32)
    out[...] = total.astype(out.dtype)


def output(core, z, rows, before, out):
    vmem = pl.BlockSpec(memory_space=pltpu.VMEM)
    steps = z.shape[0]
    parts, _, width = rows.shape
    return pl.pallas_call(
        output_kernel,
        in_specs=[
            pl.BlockSpec(memory_space=pltpu.SMEM),
            vmem,
            pl.BlockSpec(memory_space=pl.ANY),
        ]
        + [vmem] * len(before),
        out_specs=vmem,
        out_shape=out,
        scratch_shapes=[
            pltpu.VMEM((steps, parts, LANES, width), bf16),
            pltpu.SemaphoreType.DMA((steps,)),
        ],
    )(core, near(z), rows, *before)


def body(
    activations,
    input_norm_gain,
    pooling_channel_weight,
    query_projection_weight,
    key_projection_weight,
    value_projection_weight,
    output_gate_weight,
    decay_first_factor,
    decay_second_factor,
    decay_gate_bias,
    decay_extra_log,
    head_norm_gain,
    starting_state,
    pooling_group_weight,
    pooling_channel_scale,
    pooling_output_rows,
    attention_output_rows,
):
    _, tokens, width = activations.shape
    rows = key_projection_weight.shape[0]
    columns = pooling_output_rows.shape[1]
    own = lax.axis_index("fs").astype(jnp.int32).reshape(1)
    tp = lax.axis_index("tp").astype(jnp.int32)
    (late,) = call(
        pack_late_kernel,
        [struct((rows, 4 * LANES), bf16)],
        "pack_late",
        own,
        query_projection_weight,
        output_gate_weight,
        pooling_output_rows,
        attention_output_rows,
    )
    late, activations = lax.optimization_barrier((late, activations))
    late = lax.all_gather(late, "sp", axis=0, tiled=True)
    x, inverse, early = prepare(
        activations.reshape(tokens, width),
        input_norm_gain.reshape(1, width),
        key_projection_weight,
        value_projection_weight,
        pooling_channel_weight,
        decay_first_factor,
    )
    x = lax.all_to_all(x, "fs", 0, 0)
    early = lax.all_gather(early, "sp").reshape(-1, early.shape[1])
    inverse = near(inverse)
    parts, x = early_partials(near(x), near(early))
    parts = lax.all_to_all(parts, "fs", 0, 0)
    wide = pltpu.VMEM((tokens, LANES), f32)
    keys, values, pool, sums, prior, opening, spread = call(
        local_kernel,
        [
            wide,
            wide,
            pltpu.VMEM((tokens, LANES), bf16),
            wide,
            wide,
            pltpu.VMEM((tokens // BLOCK, LANES), f32),
            struct((4, RUN_ROWS, LANES), bf16),
        ],
        "local",
        near(parts),
        inverse,
        decay_second_factor,
        decay_gate_bias.reshape(1, LANES),
        decay_extra_log,
        scalars=0,
    )
    start = starting_state[0].transpose(2, 0, 1).reshape(HEAD, LANES)
    quads = [[4 * a + b for b in range(4)] for a in range(lax.axis_size("sp") // 4)]
    late, _ = lax.optimization_barrier((late, spread))
    quad = lax.all_to_all(spread, "sp", 0, 0, axis_index_groups=quads)
    late, quarter = late_partials(near(x), late)
    _, _, quad = lax.optimization_barrier((late, quarter, quad))
    out_rows = lax.all_gather(quarter, "fs")
    late = lax.all_to_all(late, "fs", 0, 0)
    sp = lax.axis_index("sp").astype(jnp.int32).reshape(1)
    total, within, log_within, previous = call(
        quad_kernel,
        [
            struct((1, RUN_ROWS, LANES), bf16),
            pltpu.VMEM((HEAD, LANES), f32),
            pltpu.VMEM((8, LANES), f32),
            pltpu.VMEM((HALO, LANES), bf16),
        ],
        "quad_total",
        sp,
        near(quad),
    )
    strided = [list(column) for column in zip(*quads)]
    runs = lax.all_gather(total[0], "sp", axis_index_groups=strided)
    peers = lax.axis_size("tp")
    (mine,) = call(
        finish_kernel,
        [struct((peers // 2, tokens, 2 * LANES), bf16)],
        "finish",
        sp,
        tp.reshape(1),
        near(runs),
        near(within),
        near(log_within),
        near(previous),
        near(start),
        near(late),
        inverse,
        near(pool),
        near(keys),
        near(values),
        near(sums),
        near(prior),
        near(opening),
        head_norm_gain.reshape(1, LANES),
        pooling_group_weight[0],
        pooling_channel_scale.reshape(1, LANES),
        scalars=2,
    )
    groups = [[c + 2 * x for x in range(peers // 2)] for c in range(2)]
    same = lax.all_to_all(mine, "tp", 0, 0, axis_index_groups=groups)
    same, out_rows = lax.optimization_barrier((same, out_rows))
    other = lax.ppermute(same, "tp", [(i, i ^ 1) for i in range(peers)])
    core = (tp & 1).reshape(1)
    half = output(core, same, out_rows, (), pltpu.VMEM((tokens, columns), f32))
    result = output(1 - core, other, out_rows, (near(half),), struct((tokens, columns), bf16))
    return result[None]


def solution(mesh):
    in_specs = (
        P("fs", "sp", None),
        P(),
        P(("sp", "fs"), "tp"),
        P(("sp", "fs"), "tp"),
        P(("sp", "fs"), "tp"),
        P(("sp", "fs"), "tp"),
        P(("sp", "fs"), "tp"),
        P(("sp", "fs"), None),
        P(None, "tp"),
        P("tp"),
        P("tp", "sp"),
        P("tp"),
        P("fs", "tp", None, None),
        P("tp", None, None),
        P("tp"),
        P("sp", "tp"),
        P("sp", "tp"),
    )
    out_specs = P("fs", "sp", "tp")

    return jax.shard_map(body, mesh=mesh, in_specs=in_specs, out_specs=out_specs, check_vma=False)
```

```python
import jax
import jax.numpy as jnp
from jax import lax
from jax.experimental import pallas as pl
from jax.experimental.pallas import tpu as pltpu
from jax.sharding import PartitionSpec as P


BLOCK = 64
HEAD = 64
LANES = 128
HALO = 16
RUN_ROWS = 80
norm_eps = 1e-06
decay_temper = 16.0
highest = lax.Precision.HIGHEST
f32 = jnp.float32
bf16 = jnp.bfloat16
limit = pltpu.CompilerParams(vmem_limit_bytes=24 << 20)


def call(kernel, outs, name, *args, scalars=1, aliases={}):
    smem = pl.BlockSpec(memory_space=pltpu.SMEM)
    vmem = pl.BlockSpec(memory_space=pltpu.VMEM)
    return pl.pallas_call(
        kernel,
        in_specs=[smem] * scalars + [vmem] * (len(args) - scalars),
        out_specs=[vmem] * len(outs),
        out_shape=outs,
        input_output_aliases=aliases,
        compiler_params=limit if name in ("local", "finish") else None,
    )(*args)


def near(x):
    return pltpu.with_memory_space_constraint(x, pltpu.VMEM)


def struct(shape, dtype):
    return jax.ShapeDtypeStruct(shape, dtype)


def pack_late_kernel(own, query, gate, pool, pool_rows, state_rows, late):
    mine = pl.ds(pl.multiple_of(own[0] * LANES, LANES), LANES)
    blocks = (query[...], gate[...], pool[...], pool_rows[:, mine], state_rows[:, mine])
    for j, block in enumerate(blocks):
        late[:, j * LANES : (j + 1) * LANES] = block


def prep_kernel(
    act, gain, key, value, low, x, inverse, early, held, made, arrived, left
):
    tokens, width = act.shape
    rows = tokens // 4
    copies = []
    for c in range(4):
        at = pl.ds(c * rows, rows)
        copies.append(pltpu.make_async_copy(act.at[at], held.at[at], arrived.at[c]))
        copies[c].start()
    at = 0
    for r in (key, value, low):
        early[:, at : at + r.shape[1]] = r[...]
        at += r.shape[1]
    half = lax.broadcasted_iota(jnp.int32, (rows, LANES), 1) < HEAD
    out = []
    for c in range(4):
        copies[c].wait()
        block = pl.ds(c * rows, rows)
        squares = jnp.zeros((rows, LANES), f32)
        for p in range(width // 512):
            tiles = []
            for q in range(4):
                at = p * 512 + q * LANES
                t = held[block, at : at + LANES].astype(f32)
                squares = squares + t * t
                tiles.append(t * gain[:, at : at + LANES])
            to = slice(p * LANES, (p + 1) * LANES)
            for j, (a, b) in enumerate(((tiles[0], tiles[2]), (tiles[1], tiles[3]))):
                made[2 * j, block, to] = jnp.where(half, a, pltpu.roll(b, HEAD, 1)).astype(bf16)
                made[2 * j + 1, block, to] = jnp.where(half, pltpu.roll(a, HEAD, 1), b).astype(bf16)
        for f in range(4):
            out.append(
                pltpu.make_async_copy(made.at[f, block], x.at[f, block], left.at[4 * c + f])
            )
            out[-1].start()
        total = jnp.sum(squares, axis=1, keepdims=True)
        inverse[block] = jnp.broadcast_to(lax.rsqrt(total / width + norm_eps), (rows, LANES))
    for o in out:
        o.wait()


def prepare(act, gain, *weights):
    tokens, width = act.shape
    vmem = pl.BlockSpec(memory_space=pltpu.VMEM)
    anywhere = pl.BlockSpec(memory_space=pl.ANY)
    shape = (4, tokens, width // 4)
    columns = sum(w.shape[1] for w in weights)
    return pl.pallas_call(
        prep_kernel,
        in_specs=[anywhere] + [vmem] * (1 + len(weights)),
        out_specs=[anywhere, vmem, vmem],
        out_shape=[
            struct(shape, bf16),
            struct((tokens, LANES), f32),
            struct((weights[0].shape[0], columns), bf16),
        ],
        scratch_shapes=[
            pltpu.VMEM((tokens, width), bf16),
            pltpu.VMEM(shape, bf16),
            pltpu.SemaphoreType.DMA((4,)),
            pltpu.SemaphoreType.DMA((16,)),
        ],
        name="prep",
    )(act, gain, *weights)


def early_kernel(x, w, out, same_x, ends, made, left):
    tokens = x.shape[1]
    half = lax.broadcasted_iota(jnp.int32, (tokens // 2, LANES), 1) < HEAD
    weight = w[...]
    copies = []
    for f in range(4):
        p = jnp.dot(x[f], weight, preferred_element_type=f32)
        for j in range(2):
            at = slice(j * tokens, (j + 1) * tokens)
            made[f, at] = p[:, j * LANES : (j + 1) * LANES].astype(bf16)
        d = jnp.concatenate([p[:, 2 * LANES :], p[:, 2 * LANES :]], axis=1)
        d = jnp.where(half, d[: tokens // 2], d[tokens // 2 :])
        made[f, 2 * tokens :] = d.astype(bf16)
        ends[f] = x[f, tokens - HALO :]
        copies.append(pltpu.make_async_copy(made.at[f], out.at[f], left.at[f]))
        copies[f].start()
    for c in copies:
        c.wait()


def late_kernel(x, w, ends, out, quarter, held, made, arrived, left):
    tokens = x.shape[1]
    columns = 3 * LANES
    depth = w.shape[0] // 4
    into = []
    for c in range(4):
        at = pl.ds(c * depth, depth)
        into.append(pltpu.make_async_copy(w.at[at], held.at[at], arrived.at[c]))
        into[c].start()
    first = jnp.zeros((tokens, columns), f32)
    for c in range(4):
        into[c].wait()
        at = slice(c * depth, (c + 1) * depth)
        first = first + jnp.dot(x[0, :, at], held[at, :columns], preferred_element_type=f32)
    across = pltpu.make_async_copy(held.at[:, columns:], quarter, left.at[4])
    across.start()
    weight = held[:, :columns]
    copies = [across]
    for f in range(4):
        p = first if f == 0 else jnp.dot(x[f], weight, preferred_element_type=f32)
        for j in range(3):
            at = slice(j * tokens, (j + 1) * tokens)
            made[f, at] = p[:, j * LANES : (j + 1) * LANES].astype(bf16)
        edge = jnp.dot(ends[f], weight[:, 2 * LANES :], preferred_element_type=f32)
        made[f, 3 * tokens :] = edge.astype(bf16)
        copies.append(pltpu.make_async_copy(made.at[f], out.at[f], left.at[f]))
        copies[f + 1].start()
    for c in copies:
        c.wait()


def early_partials(x, w):
    _, tokens, depth = x.shape
    vmem = pl.BlockSpec(memory_space=pltpu.VMEM)
    anywhere = pl.BlockSpec(memory_space=pl.ANY)
    shape = (4, tokens * w.shape[1] // LANES, LANES)
    return pl.pallas_call(
        early_kernel,
        in_specs=[vmem, vmem],
        out_specs=[anywhere, vmem, vmem],
        out_shape=[
            struct(shape, bf16),
            pltpu.VMEM(x.shape, bf16),
            struct((4, HALO, depth), bf16),
        ],
        scratch_shapes=[pltpu.VMEM(shape, bf16), pltpu.SemaphoreType.DMA((4,))],
        input_output_aliases={0: 1},
        compiler_params=limit,
        name="early_parts",
    )(x, w)


def late_partials(x, w, ends):
    _, tokens, depth = x.shape
    vmem = pl.BlockSpec(memory_space=pltpu.VMEM)
    anywhere = pl.BlockSpec(memory_space=pl.ANY)
    shape = (4, 3 * tokens + HALO, LANES)
    return pl.pallas_call(
        late_kernel,
        in_specs=[vmem, pl.BlockSpec(memory_space=pltpu.HBM), vmem],
        out_specs=[anywhere, anywhere],
        out_shape=[struct(shape, bf16), struct((depth, w.shape[1] - 3 * LANES), bf16)],
        scratch_shapes=[
            pltpu.VMEM(w.shape, bf16),
            pltpu.VMEM(shape, bf16),
            pltpu.SemaphoreType.DMA((4,)),
            pltpu.SemaphoreType.DMA((5,)),
        ],
        compiler_params=limit,
        name="late_parts",
    )(x, pltpu.with_memory_space_constraint(w, pltpu.HBM), ends)


def total_of(parts, at, rows):
    s = parts[0, at : at + rows].astype(f32)
    for k in (1, 2, 3):
        s = s + parts[k, at : at + rows].astype(f32)
    return s


def projected(parts, inverse, j):
    tokens = inverse.shape[0]
    return (total_of(parts, j * tokens, tokens) * inverse).astype(bf16)


def heads_of(x, half):
    return jnp.where(half, x[:HEAD], x[HEAD:])


def thirds(x):
    first = x.astype(bf16)
    left = x - first.astype(f32)
    second = left.astype(bf16)
    return first, second, (left - second.astype(f32)).astype(bf16)


def local_kernel(
    parts, inverse, second, bias, extra, keys, values, sums, prior, opening, spread
):
    inv = inverse[...]
    tokens = inv.shape[0]
    keys[...] = projected(parts, inv, 0).astype(f32)
    values[...] = projected(parts, inv, 1).astype(f32)
    both = total_of(parts, 2 * tokens, tokens // 2)
    low = jnp.concatenate([both[:, :HEAD], both[:, HEAD:]], axis=0)
    low = (low * inv[:, :HEAD]).astype(bf16)
    x = jnp.dot(low, second[...], preferred_element_type=f32) + bias[...]
    rates = (jnp.minimum(x, 0.0) - jnp.log1p(jnp.exp(-jnp.abs(x)))) / decay_temper
    wide = lax.broadcasted_iota(jnp.int32, (2, LANES), 1) // HEAD
    pick = (wide == lax.broadcasted_iota(jnp.int32, (2, LANES), 0)).astype(f32)
    rates = rates + lax.dot_general(
        extra[...], pick, (((0,), (0,)), ((), ())), precision=highest, preferred_element_type=f32
    )
    r = lax.broadcasted_iota(jnp.int32, (BLOCK, BLOCK), 0)
    c = lax.broadcasted_iota(jnp.int32, (BLOCK, BLOCK), 1)
    lower = (r >= c).astype(f32)
    half = lax.broadcasted_iota(jnp.int32, (HEAD, LANES), 1) < HEAD
    state = jnp.zeros((HEAD, LANES), f32)
    before = jnp.zeros((1, LANES), f32)
    for n in range(tokens // BLOCK):
        at = slice(n * BLOCK, (n + 1) * BLOCK)
        total = jnp.dot(lower, rates[at], precision=highest, preferred_element_type=f32)
        sums[at] = total
        final = total[BLOCK - 1 :]
        pairs = lax.dot_general(
            values[at],
            keys[at] * jnp.exp(final - total),
            (((0,), (0,)), ((), ())),
            precision=highest,
            preferred_element_type=f32,
        )
        prior[at] = state
        opening[n : n + 1] = before
        state = jnp.exp(final) * state + heads_of(pairs, half)
        before = before + final
    row = lax.broadcasted_iota(jnp.int32, (HALO, LANES), 0)
    lane = lax.broadcasted_iota(jnp.int32, (HALO, LANES), 1)
    last = jnp.sum(jnp.where(row == lane, inv[tokens - HALO :], 0.0), axis=0, keepdims=True)
    mine = run_of(state, before, last)
    for to in range(spread.shape[0]):
        spread[to] = mine


def run_of(state, log, inverse):
    row = lax.broadcasted_iota(jnp.int32, (HALO, LANES), 0)
    extra = jnp.zeros((HALO, LANES), f32)
    for j, part in enumerate(thirds(log) + thirds(inverse)):
        extra = jnp.where(row == j, part.astype(f32), extra)
    return jnp.concatenate([state, extra], axis=0).astype(bf16)


def read_run(came):
    came = came.astype(f32)
    log = came[HEAD : HEAD + 1] + came[HEAD + 1 : HEAD + 2] + came[HEAD + 2 : HEAD + 3]
    inverse = came[HEAD + 3 : HEAD + 4] + came[HEAD + 4 : HEAD + 5] + came[HEAD + 5 : HEAD + 6]
    return came[:HEAD], log, inverse


def quad_kernel(sp, quad, total, within, log_within, inverse_within):
    place = sp[0] % 4
    state = jnp.zeros((HEAD, LANES), f32)
    log = jnp.zeros((1, LANES), f32)
    inverse = jnp.zeros((1, LANES), f32)
    for j in range(4):

        @pl.when(place == j)
        def _(state=state, log=log, inverse=inverse):
            within[...] = state
            log_within[...] = jnp.broadcast_to(log, log_within.shape)
            inverse_within[...] = jnp.broadcast_to(inverse, inverse_within.shape)

        s, decay, inverse = read_run(quad[j])
        state = jnp.exp(decay) * state + s
        log = log + decay
    total[0] = run_of(state, log, inverse)


def finish_kernel(
    sp,
    tp,
    runs,
    within_quad,
    log_within,
    inverse_within,
    start,
    parts,
    inverse,
    keys,
    values,
    sums,
    prior,
    opening,
    gain,
    pool_weight,
    pool_scale,
    mine,
):
    inv = inverse[...]
    tokens = inv.shape[0]
    place = sp[0]
    state = start[...]
    edge = jnp.zeros((1, LANES), f32)
    for j in range(runs.shape[0]):
        came, log, outside = read_run(runs[j])
        state = jnp.where(j < place // 4, jnp.exp(log) * state + came, state)
        edge = jnp.where(j < place // 4, outside, edge)
    state = jnp.exp(log_within[:1]) * state + within_quad[...]
    queries = projected(parts, inv, 0).astype(f32) * HEAD ** (-0.5)
    outgate = projected(parts, inv, 1).astype(f32)
    half = lax.broadcasted_iota(jnp.int32, (HEAD, LANES), 1) < HEAD
    r = lax.broadcasted_iota(jnp.int32, (2 * BLOCK, BLOCK), 0) % BLOCK
    c = lax.broadcasted_iota(jnp.int32, (2 * BLOCK, BLOCK), 1)
    causal = r >= c

    def split(x):
        return jnp.concatenate([jnp.where(half, x, 0.0), jnp.where(half, 0.0, x)], axis=0)

    last = (((1,), (1,)), ((), ()))
    for n in range(tokens // BLOCK):
        at = slice(n * BLOCK, (n + 1) * BLOCK)
        total = sums[at]
        middle = total[BLOCK // 2 - 1 : BLOCK // 2]
        q = queries[at]
        scores = lax.dot_general(
            split(q * jnp.exp(total - middle)),
            keys[at] * jnp.exp(middle - total),
            last,
            precision=highest,
            preferred_element_type=f32,
        )
        scores = jnp.where(causal, scores, 0.0)
        within = jnp.dot(scores, values[at], precision=highest, preferred_element_type=f32)
        begin = prior[at] + jnp.exp(opening[n : n + 1]) * state
        carried = lax.dot_general(
            split(q * jnp.exp(total)),
            jnp.concatenate([begin, begin], axis=0),
            last,
            precision=highest,
            preferred_element_type=f32,
        )
        raw = heads_of(within + carried, half)
        square = raw * raw
        first = jnp.sum(jnp.where(half, square, 0.0), axis=1, keepdims=True)
        second = jnp.sum(jnp.where(half, 0.0, square), axis=1, keepdims=True)
        mean = jnp.where(half, first, second) / HEAD
        g = outgate[at]
        scaled = raw * lax.rsqrt(mean + norm_eps) * gain[...]
        done = (scaled * (g / (1.0 + jnp.exp(-g)))).astype(bf16)
        for to in range(mine.shape[0]):
            mine[to, at, LANES:] = done

    current = projected(parts, inv, 2).astype(f32)
    edge = jnp.where(place % 4 > 0, inverse_within[:1], edge)
    row = lax.broadcasted_iota(jnp.int32, (HALO, LANES), 0)
    lane = lax.broadcasted_iota(jnp.int32, (HALO, LANES), 1)
    scale = jnp.sum(jnp.where(row == lane, edge, 0.0), axis=1, keepdims=True)
    before = (total_of(parts, 3 * tokens, HALO) * scale).astype(bf16).astype(f32)
    extended = jnp.concatenate([before, current], axis=0)

    def back(x, by):
        return x + pltpu.roll(x, by, 0)

    two = back(extended, 1)
    four = back(two, 2)
    eight = back(four, 4)
    sixteen = back(eight, 8)
    level = tp[0] % 4
    chosen = jnp.where(
        level == 0, two, jnp.where(level == 1, four, jnp.where(level == 2, eight, sixteen))
    )[HALO:]
    window = jnp.where(
        level == 0, 2.0, jnp.where(level == 1, 4.0, jnp.where(level == 2, 8.0, 16.0))
    )
    position = place * tokens + lax.broadcasted_iota(jnp.int32, (tokens, LANES), 0)
    counts = jnp.minimum(position.astype(f32) + 1.0, window)
    deviation = (chosen / counts - current).astype(bf16)
    mixture = jnp.dot(deviation, pool_weight[...], preferred_element_type=f32)
    done = (mixture * pool_scale[...]).astype(bf16)
    for to in range(mine.shape[0]):
        mine[to, :, :LANES] = done


def output_kernel(core, z, rows, *rest):
    *before, out, held, arrived = rest
    copies = []
    for x in range(z.shape[0]):
        at = pl.ds(pl.multiple_of((2 * x + core[0]) * LANES, LANES), LANES)
        copies.append(pltpu.make_async_copy(rows.at[:, at], held.at[x], arrived.at[x]))
        copies[x].start()
    total = jnp.zeros(out.shape, f32)
    for b in before:
        total = b[...]
    for x in range(z.shape[0]):
        copies[x].wait()
        w = jnp.concatenate(
            [
                jnp.concatenate([held[x, f, :, :LANES], held[x, f, :, LANES:]], axis=0)
                for f in range(rows.shape[0])
            ],
            axis=1,
        )
        total = total + jnp.dot(z[x], w, preferred_element_type=f32)
    out[...] = total.astype(out.dtype)


def output(core, z, rows, before, out):
    vmem = pl.BlockSpec(memory_space=pltpu.VMEM)
    steps = z.shape[0]
    parts, _, width = rows.shape
    return pl.pallas_call(
        output_kernel,
        in_specs=[
            pl.BlockSpec(memory_space=pltpu.SMEM),
            vmem,
            pl.BlockSpec(memory_space=pl.ANY),
        ]
        + [vmem] * len(before),
        out_specs=vmem,
        out_shape=out,
        scratch_shapes=[
            pltpu.VMEM((steps, parts, LANES, width), bf16),
            pltpu.SemaphoreType.DMA((steps,)),
        ],
    )(core, near(z), rows, *before)


def body(
    activations,
    input_norm_gain,
    pooling_channel_weight,
    query_projection_weight,
    key_projection_weight,
    value_projection_weight,
    output_gate_weight,
    decay_first_factor,
    decay_second_factor,
    decay_gate_bias,
    decay_extra_log,
    head_norm_gain,
    starting_state,
    pooling_group_weight,
    pooling_channel_scale,
    pooling_output_rows,
    attention_output_rows,
):
    _, tokens, width = activations.shape
    rows = key_projection_weight.shape[0]
    columns = pooling_output_rows.shape[1]
    own = lax.axis_index("fs").astype(jnp.int32).reshape(1)
    tp = lax.axis_index("tp").astype(jnp.int32)
    (late,) = call(
        pack_late_kernel,
        [struct((rows, 5 * LANES), bf16)],
        "pack_late",
        own,
        query_projection_weight,
        output_gate_weight,
        pooling_channel_weight,
        pooling_output_rows,
        attention_output_rows,
    )
    late, activations = lax.optimization_barrier((late, activations))
    late = lax.all_gather(late, "sp", axis=0, tiled=True)
    x, inverse, early = prepare(
        activations.reshape(tokens, width),
        input_norm_gain.reshape(1, width),
        key_projection_weight,
        value_projection_weight,
        decay_first_factor,
    )
    x = lax.all_to_all(x, "fs", 0, 0)
    early = lax.all_gather(early, "sp").reshape(-1, early.shape[1])
    inverse = near(inverse)
    parts, x, ends = early_partials(near(x), near(early))
    count = lax.axis_size("sp")
    ends = lax.ppermute(ends, "sp", [(i, i + 1) for i in range(count - 1)])
    parts = lax.all_to_all(parts, "fs", 0, 0)
    wide = pltpu.VMEM((tokens, LANES), f32)
    keys, values, sums, prior, opening, spread = call(
        local_kernel,
        [
            wide,
            wide,
            wide,
            wide,
            pltpu.VMEM((tokens // BLOCK, LANES), f32),
            struct((4, RUN_ROWS, LANES), bf16),
        ],
        "local",
        near(parts),
        inverse,
        decay_second_factor,
        decay_gate_bias.reshape(1, LANES),
        decay_extra_log,
        scalars=0,
    )
    start = starting_state[0].transpose(2, 0, 1).reshape(HEAD, LANES)
    quads = [[4 * a + b for b in range(4)] for a in range(lax.axis_size("sp") // 4)]
    late, _ = lax.optimization_barrier((late, spread))
    quad = lax.all_to_all(spread, "sp", 0, 0, axis_index_groups=quads)
    late, quarter = late_partials(near(x), late, near(ends))
    _, _, quad = lax.optimization_barrier((late, quarter, quad))
    out_rows = lax.all_gather(quarter, "fs")
    late = lax.all_to_all(late, "fs", 0, 0)
    sp = lax.axis_index("sp").astype(jnp.int32).reshape(1)
    total, within, log_within, inverse_within = call(
        quad_kernel,
        [
            struct((1, RUN_ROWS, LANES), bf16),
            pltpu.VMEM((HEAD, LANES), f32),
            pltpu.VMEM((8, LANES), f32),
            pltpu.VMEM((8, LANES), f32),
        ],
        "quad_total",
        sp,
        near(quad),
    )
    strided = [list(column) for column in zip(*quads)]
    runs = lax.all_gather(total[0], "sp", axis_index_groups=strided)
    peers = lax.axis_size("tp")
    (mine,) = call(
        finish_kernel,
        [struct((peers // 2, tokens, 2 * LANES), bf16)],
        "finish",
        sp,
        tp.reshape(1),
        near(runs),
        near(within),
        near(log_within),
        near(inverse_within),
        near(start),
        near(late),
        inverse,
        near(keys),
        near(values),
        near(sums),
        near(prior),
        near(opening),
        head_norm_gain.reshape(1, LANES),
        pooling_group_weight[0],
        pooling_channel_scale.reshape(1, LANES),
        scalars=2,
    )
    groups = [[c + 2 * x for x in range(peers // 2)] for c in range(2)]
    same = lax.all_to_all(mine, "tp", 0, 0, axis_index_groups=groups)
    same, out_rows = lax.optimization_barrier((same, out_rows))
    other = lax.ppermute(same, "tp", [(i, i ^ 1) for i in range(peers)])
    core = (tp & 1).reshape(1)
    half = output(core, same, out_rows, (), pltpu.VMEM((tokens, columns), f32))
    result = output(1 - core, other, out_rows, (near(half),), struct((tokens, columns), bf16))
    return result[None]


def solution(mesh):
    in_specs = (
        P("fs", "sp", None),
        P(),
        P(("sp", "fs"), "tp"),
        P(("sp", "fs"), "tp"),
        P(("sp", "fs"), "tp"),
        P(("sp", "fs"), "tp"),
        P(("sp", "fs"), "tp"),
        P(("sp", "fs"), None),
        P(None, "tp"),
        P("tp"),
        P("tp", "sp"),
        P("tp"),
        P("fs", "tp", None, None),
        P("tp", None, None),
        P("tp"),
        P("sp", "tp"),
        P("sp", "tp"),
    )
    out_specs = P("fs", "sp", "tp")

    return jax.shard_map(body, mesh=mesh, in_specs=in_specs, out_specs=out_specs, check_vma=False)
```

```python
import jax
import jax.numpy as jnp
from jax import lax
from jax.experimental import pallas as pl
from jax.experimental.pallas import tpu as pltpu
from jax.sharding import PartitionSpec as P


BLOCK = 64
HEAD = 64
LANES = 128
HALO = 16
RUN_ROWS = 80
norm_eps = 1e-06
decay_temper = 16.0
highest = lax.Precision.HIGHEST
f32 = jnp.float32
bf16 = jnp.bfloat16
limit = pltpu.CompilerParams(vmem_limit_bytes=24 << 20)


def call(kernel, outs, name, *args, scalars=1, aliases={}):
    smem = pl.BlockSpec(memory_space=pltpu.SMEM)
    vmem = pl.BlockSpec(memory_space=pltpu.VMEM)
    return pl.pallas_call(
        kernel,
        in_specs=[smem] * scalars + [vmem] * (len(args) - scalars),
        out_specs=[vmem] * len(outs),
        out_shape=outs,
        input_output_aliases=aliases,
        compiler_params=limit if name in ("local", "finish", "output") else None,
    )(*args)


def near(x):
    return pltpu.with_memory_space_constraint(x, pltpu.VMEM)


def struct(shape, dtype):
    return jax.ShapeDtypeStruct(shape, dtype)


def pack_late_kernel(own, query, gate, pool, pool_rows, state_rows, late):
    mine = pl.ds(pl.multiple_of(own[0] * LANES, LANES), LANES)
    blocks = (query[...], gate[...], pool[...], pool_rows[:, mine], state_rows[:, mine])
    for j, block in enumerate(blocks):
        late[:, j * LANES : (j + 1) * LANES] = block


def prep_kernel(
    act, gain, key, value, low, x, inverse, early, held, made, arrived, left
):
    tokens, width = act.shape
    rows = tokens // 4
    copies = []
    for c in range(4):
        at = pl.ds(c * rows, rows)
        copies.append(pltpu.make_async_copy(act.at[at], held.at[at], arrived.at[c]))
        copies[c].start()
    at = 0
    for r in (key, value, low):
        early[:, at : at + r.shape[1]] = r[...]
        at += r.shape[1]
    half = lax.broadcasted_iota(jnp.int32, (rows, LANES), 1) < HEAD
    out = []
    for c in range(4):
        copies[c].wait()
        block = pl.ds(c * rows, rows)
        squares = jnp.zeros((rows, LANES), f32)
        for p in range(width // 512):
            tiles = []
            for q in range(4):
                at = p * 512 + q * LANES
                t = held[block, at : at + LANES].astype(f32)
                squares = squares + t * t
                tiles.append(t * gain[:, at : at + LANES])
            to = slice(p * LANES, (p + 1) * LANES)
            for j, (a, b) in enumerate(((tiles[0], tiles[2]), (tiles[1], tiles[3]))):
                made[2 * j, block, to] = jnp.where(half, a, pltpu.roll(b, HEAD, 1)).astype(bf16)
                made[2 * j + 1, block, to] = jnp.where(half, pltpu.roll(a, HEAD, 1), b).astype(bf16)
        for f in range(4):
            out.append(
                pltpu.make_async_copy(made.at[f, block], x.at[f, block], left.at[4 * c + f])
            )
            out[-1].start()
        total = jnp.sum(squares, axis=1, keepdims=True)
        inverse[block] = jnp.broadcast_to(lax.rsqrt(total / width + norm_eps), (rows, LANES))
    for o in out:
        o.wait()


def prepare(act, gain, *weights):
    tokens, width = act.shape
    vmem = pl.BlockSpec(memory_space=pltpu.VMEM)
    anywhere = pl.BlockSpec(memory_space=pl.ANY)
    shape = (4, tokens, width // 4)
    columns = sum(w.shape[1] for w in weights)
    return pl.pallas_call(
        prep_kernel,
        in_specs=[anywhere] + [vmem] * (1 + len(weights)),
        out_specs=[anywhere, vmem, vmem],
        out_shape=[
            struct(shape, bf16),
            struct((tokens, LANES), f32),
            struct((weights[0].shape[0], columns), bf16),
        ],
        scratch_shapes=[
            pltpu.VMEM((tokens, width), bf16),
            pltpu.VMEM(shape, bf16),
            pltpu.SemaphoreType.DMA((4,)),
            pltpu.SemaphoreType.DMA((16,)),
        ],
        name="prep",
    )(act, gain, *weights)


def early_kernel(x, w, out, same_x, ends, made, left):
    tokens = x.shape[1]
    half = lax.broadcasted_iota(jnp.int32, (tokens // 2, LANES), 1) < HEAD
    weight = w[...]
    copies = []
    for f in range(4):
        p = jnp.dot(x[f], weight, preferred_element_type=f32)
        for j in range(2):
            at = slice(j * tokens, (j + 1) * tokens)
            made[f, at] = p[:, j * LANES : (j + 1) * LANES].astype(bf16)
        d = jnp.concatenate([p[:, 2 * LANES :], p[:, 2 * LANES :]], axis=1)
        d = jnp.where(half, d[: tokens // 2], d[tokens // 2 :])
        made[f, 2 * tokens :] = d.astype(bf16)
        ends[f] = x[f, tokens - HALO :]
        copies.append(pltpu.make_async_copy(made.at[f], out.at[f], left.at[f]))
        copies[f].start()
    for c in copies:
        c.wait()


def late_kernel(x, w, ends, out, quarter, held, made, arrived, left):
    tokens = x.shape[1]
    columns = 3 * LANES
    depth = w.shape[0] // 4
    into = []
    for c in range(4):
        at = pl.ds(c * depth, depth)
        into.append(pltpu.make_async_copy(w.at[at], held.at[at], arrived.at[c]))
        into[c].start()
    first = jnp.zeros((tokens, columns), f32)
    for c in range(4):
        into[c].wait()
        at = slice(c * depth, (c + 1) * depth)
        first = first + jnp.dot(x[0, :, at], held[at, :columns], preferred_element_type=f32)
    across = pltpu.make_async_copy(held.at[:, columns:], quarter, left.at[4])
    across.start()
    weight = held[:, :columns]
    edges = jnp.dot(
        ends[...].reshape(4 * HALO, x.shape[2]),
        weight[:, 2 * LANES :],
        preferred_element_type=f32,
    ).astype(bf16)
    copies = [across]
    for f in range(4):
        p = first if f == 0 else jnp.dot(x[f], weight, preferred_element_type=f32)
        for j in range(3):
            at = slice(j * tokens, (j + 1) * tokens)
            made[f, at] = p[:, j * LANES : (j + 1) * LANES].astype(bf16)
        made[f, 3 * tokens :] = edges[f * HALO : (f + 1) * HALO]
        copies.append(pltpu.make_async_copy(made.at[f], out.at[f], left.at[f]))
        copies[f + 1].start()
    for c in copies:
        c.wait()


def early_partials(x, w):
    _, tokens, depth = x.shape
    vmem = pl.BlockSpec(memory_space=pltpu.VMEM)
    anywhere = pl.BlockSpec(memory_space=pl.ANY)
    shape = (4, tokens * w.shape[1] // LANES, LANES)
    return pl.pallas_call(
        early_kernel,
        in_specs=[vmem, vmem],
        out_specs=[anywhere, vmem, vmem],
        out_shape=[
            struct(shape, bf16),
            pltpu.VMEM(x.shape, bf16),
            struct((4, HALO, depth), bf16),
        ],
        scratch_shapes=[pltpu.VMEM(shape, bf16), pltpu.SemaphoreType.DMA((4,))],
        input_output_aliases={0: 1},
        compiler_params=limit,
        name="early_parts",
    )(x, w)


def late_partials(x, w, ends):
    _, tokens, depth = x.shape
    vmem = pl.BlockSpec(memory_space=pltpu.VMEM)
    anywhere = pl.BlockSpec(memory_space=pl.ANY)
    shape = (4, 3 * tokens + HALO, LANES)
    return pl.pallas_call(
        late_kernel,
        in_specs=[vmem, pl.BlockSpec(memory_space=pltpu.HBM), vmem],
        out_specs=[anywhere, anywhere],
        out_shape=[struct(shape, bf16), struct((depth, w.shape[1] - 3 * LANES), bf16)],
        scratch_shapes=[
            pltpu.VMEM(w.shape, bf16),
            pltpu.VMEM(shape, bf16),
            pltpu.SemaphoreType.DMA((4,)),
            pltpu.SemaphoreType.DMA((5,)),
        ],
        compiler_params=limit,
        name="late_parts",
    )(x, pltpu.with_memory_space_constraint(w, pltpu.HBM), ends)


def total_of(parts, at, rows):
    s = parts[0, at : at + rows].astype(f32)
    for k in (1, 2, 3):
        s = s + parts[k, at : at + rows].astype(f32)
    return s


def projected(parts, inverse, j):
    tokens = inverse.shape[0]
    return (total_of(parts, j * tokens, tokens) * inverse).astype(bf16)


def heads_of(x, half):
    return jnp.where(half, x[:HEAD], x[HEAD:])


def thirds(x):
    first = x.astype(bf16)
    left = x - first.astype(f32)
    second = left.astype(bf16)
    return first, second, (left - second.astype(f32)).astype(bf16)


def local_kernel(
    parts, inverse, second, bias, extra, keys, values, sums, prior, opening, spread
):
    inv = inverse[...]
    tokens = inv.shape[0]
    keys[...] = projected(parts, inv, 0).astype(f32)
    values[...] = projected(parts, inv, 1).astype(f32)
    both = total_of(parts, 2 * tokens, tokens // 2)
    low = jnp.concatenate([both[:, :HEAD], both[:, HEAD:]], axis=0)
    low = (low * inv[:, :HEAD]).astype(bf16)
    x = jnp.dot(low, second[...], preferred_element_type=f32) + bias[...]
    rates = (jnp.minimum(x, 0.0) - jnp.log1p(jnp.exp(-jnp.abs(x)))) / decay_temper
    wide = lax.broadcasted_iota(jnp.int32, (2, LANES), 1) // HEAD
    pick = (wide == lax.broadcasted_iota(jnp.int32, (2, LANES), 0)).astype(f32)
    rates = rates + lax.dot_general(
        extra[...], pick, (((0,), (0,)), ((), ())), precision=highest, preferred_element_type=f32
    )
    r = lax.broadcasted_iota(jnp.int32, (BLOCK, BLOCK), 0)
    c = lax.broadcasted_iota(jnp.int32, (BLOCK, BLOCK), 1)
    lower = (r >= c).astype(f32)
    half = lax.broadcasted_iota(jnp.int32, (HEAD, LANES), 1) < HEAD
    state = jnp.zeros((HEAD, LANES), f32)
    before = jnp.zeros((1, LANES), f32)
    for n in range(tokens // BLOCK):
        at = slice(n * BLOCK, (n + 1) * BLOCK)
        total = jnp.dot(lower, rates[at], precision=highest, preferred_element_type=f32)
        sums[at] = total
        final = total[BLOCK - 1 :]
        pairs = lax.dot_general(
            values[at],
            keys[at] * jnp.exp(final - total),
            (((0,), (0,)), ((), ())),
            precision=highest,
            preferred_element_type=f32,
        )
        prior[at] = state
        opening[n : n + 1] = before
        state = jnp.exp(final) * state + heads_of(pairs, half)
        before = before + final
    row = lax.broadcasted_iota(jnp.int32, (HALO, LANES), 0)
    lane = lax.broadcasted_iota(jnp.int32, (HALO, LANES), 1)
    last = jnp.sum(jnp.where(row == lane, inv[tokens - HALO :], 0.0), axis=0, keepdims=True)
    mine = run_of(state, before, last)
    for to in range(spread.shape[0]):
        spread[to] = mine


def run_of(state, log, inverse):
    row = lax.broadcasted_iota(jnp.int32, (HALO, LANES), 0)
    extra = jnp.zeros((HALO, LANES), f32)
    for j, part in enumerate(thirds(log) + thirds(inverse)):
        extra = jnp.where(row == j, part.astype(f32), extra)
    return jnp.concatenate([state, extra], axis=0).astype(bf16)


def read_run(came):
    came = came.astype(f32)
    log = came[HEAD : HEAD + 1] + came[HEAD + 1 : HEAD + 2] + came[HEAD + 2 : HEAD + 3]
    inverse = came[HEAD + 3 : HEAD + 4] + came[HEAD + 4 : HEAD + 5] + came[HEAD + 5 : HEAD + 6]
    return came[:HEAD], log, inverse


def quad_kernel(sp, quad, total, within, log_within, inverse_within):
    place = sp[0] % 4
    state = jnp.zeros((HEAD, LANES), f32)
    log = jnp.zeros((1, LANES), f32)
    inverse = jnp.zeros((1, LANES), f32)
    for j in range(4):

        @pl.when(place == j)
        def _(state=state, log=log, inverse=inverse):
            within[...] = state
            log_within[...] = jnp.broadcast_to(log, log_within.shape)
            inverse_within[...] = jnp.broadcast_to(inverse, inverse_within.shape)

        s, decay, inverse = read_run(quad[j])
        state = jnp.exp(decay) * state + s
        log = log + decay
    total[0] = run_of(state, log, inverse)


def finish_kernel(
    sp,
    tp,
    runs,
    within_quad,
    log_within,
    inverse_within,
    start,
    parts,
    inverse,
    keys,
    values,
    sums,
    prior,
    opening,
    gain,
    pool_weight,
    pool_scale,
    mine,
):
    inv = inverse[...]
    tokens = inv.shape[0]
    place = sp[0]
    state = start[...]
    edge = jnp.zeros((1, LANES), f32)
    for j in range(runs.shape[0]):
        came, log, outside = read_run(runs[j])
        state = jnp.where(j < place // 4, jnp.exp(log) * state + came, state)
        edge = jnp.where(j < place // 4, outside, edge)
    state = jnp.exp(log_within[:1]) * state + within_quad[...]
    queries = projected(parts, inv, 0).astype(f32) * HEAD ** (-0.5)
    outgate = projected(parts, inv, 1).astype(f32)
    half = lax.broadcasted_iota(jnp.int32, (HEAD, LANES), 1) < HEAD
    r = lax.broadcasted_iota(jnp.int32, (2 * BLOCK, BLOCK), 0) % BLOCK
    c = lax.broadcasted_iota(jnp.int32, (2 * BLOCK, BLOCK), 1)
    causal = r >= c

    def split(x):
        return jnp.concatenate([jnp.where(half, x, 0.0), jnp.where(half, 0.0, x)], axis=0)

    last = (((1,), (1,)), ((), ()))
    for n in range(tokens // BLOCK):
        at = slice(n * BLOCK, (n + 1) * BLOCK)
        total = sums[at]
        middle = total[BLOCK // 2 - 1 : BLOCK // 2]
        q = queries[at]
        scores = lax.dot_general(
            split(q * jnp.exp(total - middle)),
            keys[at] * jnp.exp(middle - total),
            last,
            precision=highest,
            preferred_element_type=f32,
        )
        scores = jnp.where(causal, scores, 0.0)
        within = jnp.dot(scores, values[at], precision=highest, preferred_element_type=f32)
        begin = prior[at] + jnp.exp(opening[n : n + 1]) * state
        carried = lax.dot_general(
            split(q * jnp.exp(total)),
            jnp.concatenate([begin, begin], axis=0),
            last,
            precision=highest,
            preferred_element_type=f32,
        )
        raw = heads_of(within + carried, half)
        square = raw * raw
        first = jnp.sum(jnp.where(half, square, 0.0), axis=1, keepdims=True)
        second = jnp.sum(jnp.where(half, 0.0, square), axis=1, keepdims=True)
        mean = jnp.where(half, first, second) / HEAD
        g = outgate[at]
        scaled = raw * lax.rsqrt(mean + norm_eps) * gain[...]
        done = (scaled * (g / (1.0 + jnp.exp(-g)))).astype(bf16)
        for to in range(mine.shape[0]):
            mine[to, at, LANES:] = done

    current = projected(parts, inv, 2).astype(f32)
    edge = jnp.where(place % 4 > 0, inverse_within[:1], edge)
    row = lax.broadcasted_iota(jnp.int32, (HALO, LANES), 0)
    lane = lax.broadcasted_iota(jnp.int32, (HALO, LANES), 1)
    scale = jnp.sum(jnp.where(row == lane, edge, 0.0), axis=1, keepdims=True)
    before = (total_of(parts, 3 * tokens, HALO) * scale).astype(bf16).astype(f32)
    extended = jnp.concatenate([before, current], axis=0)

    def back(x, by):
        return x + pltpu.roll(x, by, 0)

    two = back(extended, 1)
    four = back(two, 2)
    eight = back(four, 4)
    sixteen = back(eight, 8)
    level = tp[0] % 4
    chosen = jnp.where(
        level == 0, two, jnp.where(level == 1, four, jnp.where(level == 2, eight, sixteen))
    )[HALO:]
    window = jnp.where(
        level == 0, 2.0, jnp.where(level == 1, 4.0, jnp.where(level == 2, 8.0, 16.0))
    )
    position = place * tokens + lax.broadcasted_iota(jnp.int32, (tokens, LANES), 0)
    counts = jnp.minimum(position.astype(f32) + 1.0, window)
    deviation = (chosen / counts - current).astype(bf16)
    mixture = jnp.dot(deviation, pool_weight[...], preferred_element_type=f32)
    done = (mixture * pool_scale[...]).astype(bf16)
    for to in range(mine.shape[0]):
        mine[to, :, :LANES] = done


def block_of(held, x):
    return jnp.concatenate(
        [
            jnp.concatenate([held[x, f, :, :LANES], held[x, f, :, LANES:]], axis=0)
            for f in range(held.shape[1])
        ],
        axis=1,
    )


def half_kernel(core, z, rows, out, staged, held, arrived):
    steps = z.shape[0]
    copies = []
    for j, (to, c) in enumerate(((held, core[0]), (staged, 1 - core[0]))):
        for x in range(steps):
            at = pl.ds(pl.multiple_of((2 * x + c) * LANES, LANES), LANES)
            k = j * steps + x
            copies.append(pltpu.make_async_copy(rows.at[:, at], to.at[x], arrived.at[k]))
            copies[k].start()
    total = jnp.zeros(out.shape, f32)
    for x in range(steps):
        copies[x].wait()
        total = total + jnp.dot(z[x], block_of(held, x), preferred_element_type=f32)
    out[...] = total
    for x in range(steps):
        copies[steps + x].wait()


def output_kernel(z, staged, half, out):
    total = half[...]
    for x in range(z.shape[0]):
        total = total + jnp.dot(z[x], block_of(staged, x), preferred_element_type=f32)
    out[...] = total.astype(out.dtype)


def first_half(core, z, rows):
    vmem = pl.BlockSpec(memory_space=pltpu.VMEM)
    steps, tokens, width = z.shape
    parts = rows.shape[0]
    shape = (steps, parts, LANES, width)
    return pl.pallas_call(
        half_kernel,
        in_specs=[
            pl.BlockSpec(memory_space=pltpu.SMEM),
            vmem,
            pl.BlockSpec(memory_space=pltpu.HBM),
        ],
        out_specs=[vmem, vmem],
        compiler_params=limit,
        out_shape=[pltpu.VMEM((tokens, parts * LANES), f32), pltpu.VMEM(shape, bf16)],
        scratch_shapes=[pltpu.VMEM(shape, bf16), pltpu.SemaphoreType.DMA((2 * steps,))],
        name="half",
    )(core, near(z), pltpu.with_memory_space_constraint(rows, pltpu.HBM))


def body(
    activations,
    input_norm_gain,
    pooling_channel_weight,
    query_projection_weight,
    key_projection_weight,
    value_projection_weight,
    output_gate_weight,
    decay_first_factor,
    decay_second_factor,
    decay_gate_bias,
    decay_extra_log,
    head_norm_gain,
    starting_state,
    pooling_group_weight,
    pooling_channel_scale,
    pooling_output_rows,
    attention_output_rows,
):
    _, tokens, width = activations.shape
    rows = key_projection_weight.shape[0]
    columns = pooling_output_rows.shape[1]
    own = lax.axis_index("fs").astype(jnp.int32).reshape(1)
    tp = lax.axis_index("tp").astype(jnp.int32)
    (late,) = call(
        pack_late_kernel,
        [struct((rows, 5 * LANES), bf16)],
        "pack_late",
        own,
        query_projection_weight,
        output_gate_weight,
        pooling_channel_weight,
        pooling_output_rows,
        attention_output_rows,
    )
    late, activations = lax.optimization_barrier((late, activations))
    late = lax.all_gather(late, "sp", axis=0, tiled=True)
    x, inverse, early = prepare(
        activations.reshape(tokens, width),
        input_norm_gain.reshape(1, width),
        key_projection_weight,
        value_projection_weight,
        decay_first_factor,
    )
    x = lax.all_to_all(x, "fs", 0, 0)
    early = lax.all_gather(early, "sp").reshape(-1, early.shape[1])
    inverse = near(inverse)
    parts, x, ends = early_partials(near(x), near(early))
    count = lax.axis_size("sp")
    ends = lax.ppermute(ends, "sp", [(i, i + 1) for i in range(count - 1)])
    parts = lax.all_to_all(parts, "fs", 0, 0)
    wide = pltpu.VMEM((tokens, LANES), f32)
    keys, values, sums, prior, opening, spread = call(
        local_kernel,
        [
            wide,
            wide,
            wide,
            wide,
            pltpu.VMEM((tokens // BLOCK, LANES), f32),
            struct((4, RUN_ROWS, LANES), bf16),
        ],
        "local",
        near(parts),
        inverse,
        decay_second_factor,
        decay_gate_bias.reshape(1, LANES),
        decay_extra_log,
        scalars=0,
    )
    start = starting_state[0].transpose(2, 0, 1).reshape(HEAD, LANES)
    quads = [[4 * a + b for b in range(4)] for a in range(lax.axis_size("sp") // 4)]
    late, _ = lax.optimization_barrier((late, spread))
    quad = lax.all_to_all(spread, "sp", 0, 0, axis_index_groups=quads)
    late_parts, quarter = late_partials(near(x), late, near(ends))
    _, _, quad = lax.optimization_barrier((late_parts, quarter, quad))
    out_rows = lax.all_gather(quarter, "fs")
    late = lax.all_to_all(late_parts, "fs", 0, 0)
    sp = lax.axis_index("sp").astype(jnp.int32).reshape(1)
    total, within, log_within, inverse_within = call(
        quad_kernel,
        [
            struct((1, RUN_ROWS, LANES), bf16),
            pltpu.VMEM((HEAD, LANES), f32),
            pltpu.VMEM((8, LANES), f32),
            pltpu.VMEM((8, LANES), f32),
        ],
        "quad_total",
        sp,
        near(quad),
    )
    strided = [list(column) for column in zip(*quads)]
    runs = lax.all_gather(total[0], "sp", axis_index_groups=strided)
    peers = lax.axis_size("tp")
    (mine,) = call(
        finish_kernel,
        [struct((peers // 2, tokens, 2 * LANES), bf16)],
        "finish",
        sp,
        tp.reshape(1),
        near(runs),
        near(within),
        near(log_within),
        near(inverse_within),
        near(start),
        near(late),
        inverse,
        near(keys),
        near(values),
        near(sums),
        near(prior),
        near(opening),
        head_norm_gain.reshape(1, LANES),
        pooling_group_weight[0],
        pooling_channel_scale.reshape(1, LANES),
        scalars=2,
    )
    groups = [[c + 2 * x for x in range(peers // 2)] for c in range(2)]
    same = lax.all_to_all(mine, "tp", 0, 0, axis_index_groups=groups)
    same, out_rows = lax.optimization_barrier((same, out_rows))
    other = lax.ppermute(same, "tp", [(i, i ^ 1) for i in range(peers)])
    core = (tp & 1).reshape(1)
    half, staged = first_half(core, same, out_rows)
    (result,) = call(
        output_kernel,
        [struct((tokens, columns), bf16)],
        "output",
        near(other),
        near(staged),
        near(half),
        scalars=0,
    )
    return result[None]


def solution(mesh):
    in_specs = (
        P("fs", "sp", None),
        P(),
        P(("sp", "fs"), "tp"),
        P(("sp", "fs"), "tp"),
        P(("sp", "fs"), "tp"),
        P(("sp", "fs"), "tp"),
        P(("sp", "fs"), "tp"),
        P(("sp", "fs"), None),
        P(None, "tp"),
        P("tp"),
        P("tp", "sp"),
        P("tp"),
        P("fs", "tp", None, None),
        P("tp", None, None),
        P("tp"),
        P("sp", "tp"),
        P("sp", "tp"),
    )
    out_specs = P("fs", "sp", "tp")

    return jax.shard_map(
        body, mesh=mesh, in_specs=in_specs, out_specs=out_specs, check_vma=False
    )
```

```python
import jax
import jax.numpy as jnp
from jax import lax
from jax.experimental import pallas as pl
from jax.experimental.pallas import tpu as pltpu
from jax.sharding import PartitionSpec as P


BLOCK = 64
HEAD = 64
LANES = 128
HALO = 16
RUN_ROWS = 80
norm_eps = 1e-06
decay_temper = 16.0
highest = lax.Precision.HIGHEST
f32 = jnp.float32
bf16 = jnp.bfloat16
limit = pltpu.CompilerParams(vmem_limit_bytes=24 << 20)


def call(kernel, outs, name, *args, scalars=1, aliases={}):
    smem = pl.BlockSpec(memory_space=pltpu.SMEM)
    vmem = pl.BlockSpec(memory_space=pltpu.VMEM)
    return pl.pallas_call(
        kernel,
        in_specs=[smem] * scalars + [vmem] * (len(args) - scalars),
        out_specs=[vmem] * len(outs),
        out_shape=outs,
        input_output_aliases=aliases,
        compiler_params=limit if name in ("local", "finish", "output") else None,
    )(*args)


def near(x):
    return pltpu.with_memory_space_constraint(x, pltpu.VMEM)


def struct(shape, dtype):
    return jax.ShapeDtypeStruct(shape, dtype)


def pack_late_kernel(own, query, gate, pool, pool_rows, state_rows, late):
    for j, block in enumerate((query, gate, pool, pool_rows, state_rows)):
        late[:, j * LANES : (j + 1) * LANES] = block[...]


def pack_late(own, query, gate, pool, pool_rows, state_rows):
    rows = query.shape[0]
    whole = pl.BlockSpec((rows, LANES), lambda i, own: (0, 0))
    mine = pl.BlockSpec((rows, LANES), lambda i, own: (0, own[0]))
    return pl.pallas_call(
        pack_late_kernel,
        grid_spec=pltpu.PrefetchScalarGridSpec(
            num_scalar_prefetch=1,
            grid=(1,),
            in_specs=[whole, whole, whole, mine, mine],
            out_specs=pl.BlockSpec((rows, 5 * LANES), lambda i, own: (0, 0)),
        ),
        out_shape=struct((rows, 5 * LANES), bf16),
        name="pack_late",
    )(own, query, gate, pool, pool_rows, state_rows)


def prep_kernel(
    act, gain, key, value, low, x, inverse, early, held, made, arrived, left
):
    tokens, width = act.shape
    rows = tokens // 4
    copies = []
    for c in range(4):
        at = pl.ds(c * rows, rows)
        copies.append(pltpu.make_async_copy(act.at[at], held.at[at], arrived.at[c]))
        copies[c].start()
    at = 0
    for r in (key, value, low):
        early[:, at : at + r.shape[1]] = r[...]
        at += r.shape[1]
    half = lax.broadcasted_iota(jnp.int32, (rows, LANES), 1) < HEAD
    out = []
    for c in range(4):
        copies[c].wait()
        block = pl.ds(c * rows, rows)
        squares = jnp.zeros((rows, LANES), f32)
        for p in range(width // 512):
            tiles = []
            for q in range(4):
                at = p * 512 + q * LANES
                t = held[block, at : at + LANES].astype(f32)
                squares = squares + t * t
                tiles.append(t * gain[:, at : at + LANES])
            to = slice(p * LANES, (p + 1) * LANES)
            for j, (a, b) in enumerate(((tiles[0], tiles[2]), (tiles[1], tiles[3]))):
                made[2 * j, block, to] = jnp.where(half, a, pltpu.roll(b, HEAD, 1)).astype(bf16)
                made[2 * j + 1, block, to] = jnp.where(half, pltpu.roll(a, HEAD, 1), b).astype(bf16)
        for f in range(4):
            out.append(
                pltpu.make_async_copy(made.at[f, block], x.at[f, block], left.at[4 * c + f])
            )
            out[-1].start()
        total = jnp.sum(squares, axis=1, keepdims=True)
        inverse[block] = jnp.broadcast_to(lax.rsqrt(total / width + norm_eps), (rows, LANES))
    for o in out:
        o.wait()


def prepare(act, gain, *weights):
    tokens, width = act.shape
    vmem = pl.BlockSpec(memory_space=pltpu.VMEM)
    anywhere = pl.BlockSpec(memory_space=pl.ANY)
    shape = (4, tokens, width // 4)
    columns = sum(w.shape[1] for w in weights)
    return pl.pallas_call(
        prep_kernel,
        in_specs=[anywhere] + [vmem] * (1 + len(weights)),
        out_specs=[anywhere, vmem, vmem],
        out_shape=[
            struct(shape, bf16),
            struct((tokens, LANES), f32),
            struct((weights[0].shape[0], columns), bf16),
        ],
        scratch_shapes=[
            pltpu.VMEM((tokens, width), bf16),
            pltpu.VMEM(shape, bf16),
            pltpu.SemaphoreType.DMA((4,)),
            pltpu.SemaphoreType.DMA((16,)),
        ],
        name="prep",
    )(act, gain, *weights)


def early_kernel(x, w, out, same_x, ends, made, left):
    tokens = x.shape[1]
    half = lax.broadcasted_iota(jnp.int32, (tokens // 2, LANES), 1) < HEAD
    weight = w[...]
    copies = []
    for f in range(4):
        p = jnp.dot(x[f], weight, preferred_element_type=f32)
        for j in range(2):
            at = slice(j * tokens, (j + 1) * tokens)
            made[f, at] = p[:, j * LANES : (j + 1) * LANES].astype(bf16)
        d = jnp.concatenate([p[:, 2 * LANES :], p[:, 2 * LANES :]], axis=1)
        d = jnp.where(half, d[: tokens // 2], d[tokens // 2 :])
        made[f, 2 * tokens :] = d.astype(bf16)
        ends[f] = x[f, tokens - HALO :]
        copies.append(pltpu.make_async_copy(made.at[f], out.at[f], left.at[f]))
        copies[f].start()
    for c in copies:
        c.wait()


def late_kernel(x, w, ends, out, quarter, held, made, arrived, left):
    tokens = x.shape[1]
    columns = 3 * LANES
    depth = w.shape[0] // 4
    into = []
    for c in range(4):
        at = pl.ds(c * depth, depth)
        into.append(pltpu.make_async_copy(w.at[at], held.at[at], arrived.at[c]))
        into[c].start()
    first = jnp.zeros((tokens, columns), f32)
    for c in range(4):
        into[c].wait()
        at = slice(c * depth, (c + 1) * depth)
        first = first + jnp.dot(x[0, :, at], held[at, :columns], preferred_element_type=f32)
    across = pltpu.make_async_copy(held.at[:, columns:], quarter, left.at[4])
    across.start()
    weight = held[:, :columns]
    edges = jnp.dot(
        ends[...].reshape(4 * HALO, x.shape[2]),
        weight[:, 2 * LANES :],
        preferred_element_type=f32,
    ).astype(bf16)
    copies = [across]
    for f in range(4):
        p = first if f == 0 else jnp.dot(x[f], weight, preferred_element_type=f32)
        for j in range(3):
            at = slice(j * tokens, (j + 1) * tokens)
            made[f, at] = p[:, j * LANES : (j + 1) * LANES].astype(bf16)
        made[f, 3 * tokens :] = edges[f * HALO : (f + 1) * HALO]
        copies.append(pltpu.make_async_copy(made.at[f], out.at[f], left.at[f]))
        copies[f + 1].start()
    for c in copies:
        c.wait()


def early_partials(x, w):
    _, tokens, depth = x.shape
    vmem = pl.BlockSpec(memory_space=pltpu.VMEM)
    anywhere = pl.BlockSpec(memory_space=pl.ANY)
    shape = (4, tokens * w.shape[1] // LANES, LANES)
    return pl.pallas_call(
        early_kernel,
        in_specs=[vmem, vmem],
        out_specs=[anywhere, vmem, vmem],
        out_shape=[
            struct(shape, bf16),
            pltpu.VMEM(x.shape, bf16),
            struct((4, HALO, depth), bf16),
        ],
        scratch_shapes=[pltpu.VMEM(shape, bf16), pltpu.SemaphoreType.DMA((4,))],
        input_output_aliases={0: 1},
        compiler_params=limit,
        name="early_parts",
    )(x, w)


def late_partials(x, w, ends):
    _, tokens, depth = x.shape
    vmem = pl.BlockSpec(memory_space=pltpu.VMEM)
    anywhere = pl.BlockSpec(memory_space=pl.ANY)
    shape = (4, 3 * tokens + HALO, LANES)
    return pl.pallas_call(
        late_kernel,
        in_specs=[vmem, pl.BlockSpec(memory_space=pltpu.HBM), vmem],
        out_specs=[anywhere, anywhere],
        out_shape=[struct(shape, bf16), struct((depth, w.shape[1] - 3 * LANES), bf16)],
        scratch_shapes=[
            pltpu.VMEM(w.shape, bf16),
            pltpu.VMEM(shape, bf16),
            pltpu.SemaphoreType.DMA((4,)),
            pltpu.SemaphoreType.DMA((5,)),
        ],
        compiler_params=limit,
        name="late_parts",
    )(x, pltpu.with_memory_space_constraint(w, pltpu.HBM), ends)


def total_of(parts, at, rows):
    s = parts[0, at : at + rows].astype(f32)
    for k in (1, 2, 3):
        s = s + parts[k, at : at + rows].astype(f32)
    return s


def projected(parts, inverse, j):
    tokens = inverse.shape[0]
    return (total_of(parts, j * tokens, tokens) * inverse).astype(bf16)


def heads_of(x, half):
    return jnp.where(half, x[:HEAD], x[HEAD:])


def thirds(x):
    first = x.astype(bf16)
    left = x - first.astype(f32)
    second = left.astype(bf16)
    return first, second, (left - second.astype(f32)).astype(bf16)


def local_kernel(
    parts, inverse, second, bias, extra, keys, values, sums, prior, opening, spread
):
    inv = inverse[...]
    tokens = inv.shape[0]
    keys[...] = projected(parts, inv, 0).astype(f32)
    values[...] = projected(parts, inv, 1).astype(f32)
    both = total_of(parts, 2 * tokens, tokens // 2)
    low = jnp.concatenate([both[:, :HEAD], both[:, HEAD:]], axis=0)
    low = (low * inv[:, :HEAD]).astype(bf16)
    x = jnp.dot(low, second[...], preferred_element_type=f32) + bias[...]
    rates = (jnp.minimum(x, 0.0) - jnp.log1p(jnp.exp(-jnp.abs(x)))) / decay_temper
    wide = lax.broadcasted_iota(jnp.int32, (2, LANES), 1) // HEAD
    pick = (wide == lax.broadcasted_iota(jnp.int32, (2, LANES), 0)).astype(f32)
    rates = rates + lax.dot_general(
        extra[...], pick, (((0,), (0,)), ((), ())), precision=highest, preferred_element_type=f32
    )
    r = lax.broadcasted_iota(jnp.int32, (BLOCK, BLOCK), 0)
    c = lax.broadcasted_iota(jnp.int32, (BLOCK, BLOCK), 1)
    lower = (r >= c).astype(f32)
    half = lax.broadcasted_iota(jnp.int32, (HEAD, LANES), 1) < HEAD
    state = jnp.zeros((HEAD, LANES), f32)
    before = jnp.zeros((1, LANES), f32)
    for n in range(tokens // BLOCK):
        at = slice(n * BLOCK, (n + 1) * BLOCK)
        total = jnp.dot(lower, rates[at], precision=highest, preferred_element_type=f32)
        sums[at] = total
        final = total[BLOCK - 1 :]
        pairs = lax.dot_general(
            values[at],
            keys[at] * jnp.exp(final - total),
            (((0,), (0,)), ((), ())),
            precision=highest,
            preferred_element_type=f32,
        )
        prior[at] = state
        opening[n : n + 1] = before
        state = jnp.exp(final) * state + heads_of(pairs, half)
        before = before + final
    row = lax.broadcasted_iota(jnp.int32, (HALO, LANES), 0)
    lane = lax.broadcasted_iota(jnp.int32, (HALO, LANES), 1)
    last = jnp.sum(jnp.where(row == lane, inv[tokens - HALO :], 0.0), axis=0, keepdims=True)
    mine = run_of(state, before, last)
    for to in range(spread.shape[0]):
        spread[to] = mine


def run_of(state, log, inverse):
    row = lax.broadcasted_iota(jnp.int32, (HALO, LANES), 0)
    extra = jnp.zeros((HALO, LANES), f32)
    for j, part in enumerate(thirds(log) + thirds(inverse)):
        extra = jnp.where(row == j, part.astype(f32), extra)
    return jnp.concatenate([state, extra], axis=0).astype(bf16)


def read_run(came):
    came = came.astype(f32)
    log = came[HEAD : HEAD + 1] + came[HEAD + 1 : HEAD + 2] + came[HEAD + 2 : HEAD + 3]
    inverse = came[HEAD + 3 : HEAD + 4] + came[HEAD + 4 : HEAD + 5] + came[HEAD + 5 : HEAD + 6]
    return came[:HEAD], log, inverse


def quad_kernel(sp, quad, total, within, log_within, inverse_within):
    place = sp[0] % 4
    state = jnp.zeros((HEAD, LANES), f32)
    log = jnp.zeros((1, LANES), f32)
    inverse = jnp.zeros((1, LANES), f32)
    for j in range(4):

        @pl.when(place == j)
        def _(state=state, log=log, inverse=inverse):
            within[...] = state
            log_within[...] = jnp.broadcast_to(log, log_within.shape)
            inverse_within[...] = jnp.broadcast_to(inverse, inverse_within.shape)

        s, decay, inverse = read_run(quad[j])
        state = jnp.exp(decay) * state + s
        log = log + decay
    total[0] = run_of(state, log, inverse)


def finish_kernel(
    sp,
    tp,
    runs,
    within_quad,
    log_within,
    inverse_within,
    start,
    parts,
    inverse,
    keys,
    values,
    sums,
    prior,
    opening,
    gain,
    pool_weight,
    pool_scale,
    mine,
):
    inv = inverse[...]
    tokens = inv.shape[0]
    place = sp[0]
    state = start[...]
    edge = jnp.zeros((1, LANES), f32)
    for j in range(runs.shape[0]):
        came, log, outside = read_run(runs[j])
        state = jnp.where(j < place // 4, jnp.exp(log) * state + came, state)
        edge = jnp.where(j < place // 4, outside, edge)
    state = jnp.exp(log_within[:1]) * state + within_quad[...]
    queries = projected(parts, inv, 0).astype(f32) * HEAD ** (-0.5)
    outgate = projected(parts, inv, 1).astype(f32)
    half = lax.broadcasted_iota(jnp.int32, (HEAD, LANES), 1) < HEAD
    r = lax.broadcasted_iota(jnp.int32, (2 * BLOCK, BLOCK), 0) % BLOCK
    c = lax.broadcasted_iota(jnp.int32, (2 * BLOCK, BLOCK), 1)
    causal = r >= c

    def split(x):
        return jnp.concatenate([jnp.where(half, x, 0.0), jnp.where(half, 0.0, x)], axis=0)

    last = (((1,), (1,)), ((), ()))
    for n in range(tokens // BLOCK):
        at = slice(n * BLOCK, (n + 1) * BLOCK)
        total = sums[at]
        middle = total[BLOCK // 2 - 1 : BLOCK // 2]
        q = queries[at]
        scores = lax.dot_general(
            split(q * jnp.exp(total - middle)),
            keys[at] * jnp.exp(middle - total),
            last,
            precision=highest,
            preferred_element_type=f32,
        )
        scores = jnp.where(causal, scores, 0.0)
        within = jnp.dot(scores, values[at], precision=highest, preferred_element_type=f32)
        begin = prior[at] + jnp.exp(opening[n : n + 1]) * state
        carried = lax.dot_general(
            split(q * jnp.exp(total)),
            jnp.concatenate([begin, begin], axis=0),
            last,
            precision=highest,
            preferred_element_type=f32,
        )
        raw = heads_of(within + carried, half)
        square = raw * raw
        first = jnp.sum(jnp.where(half, square, 0.0), axis=1, keepdims=True)
        second = jnp.sum(jnp.where(half, 0.0, square), axis=1, keepdims=True)
        mean = jnp.where(half, first, second) / HEAD
        g = outgate[at]
        scaled = raw * lax.rsqrt(mean + norm_eps) * gain[...]
        done = (scaled * (g / (1.0 + jnp.exp(-g)))).astype(bf16)
        for to in range(mine.shape[0]):
            mine[to, at, LANES:] = done

    current = projected(parts, inv, 2).astype(f32)
    edge = jnp.where(place % 4 > 0, inverse_within[:1], edge)
    row = lax.broadcasted_iota(jnp.int32, (HALO, LANES), 0)
    lane = lax.broadcasted_iota(jnp.int32, (HALO, LANES), 1)
    scale = jnp.sum(jnp.where(row == lane, edge, 0.0), axis=1, keepdims=True)
    before = (total_of(parts, 3 * tokens, HALO) * scale).astype(bf16).astype(f32)
    extended = jnp.concatenate([before, current], axis=0)

    def back(x, by):
        return x + pltpu.roll(x, by, 0)

    two = back(extended, 1)
    four = back(two, 2)
    eight = back(four, 4)
    sixteen = back(eight, 8)
    level = tp[0] % 4
    chosen = jnp.where(
        level == 0, two, jnp.where(level == 1, four, jnp.where(level == 2, eight, sixteen))
    )[HALO:]
    window = jnp.where(
        level == 0, 2.0, jnp.where(level == 1, 4.0, jnp.where(level == 2, 8.0, 16.0))
    )
    position = place * tokens + lax.broadcasted_iota(jnp.int32, (tokens, LANES), 0)
    counts = jnp.minimum(position.astype(f32) + 1.0, window)
    deviation = (chosen / counts - current).astype(bf16)
    mixture = jnp.dot(deviation, pool_weight[...], preferred_element_type=f32)
    done = (mixture * pool_scale[...]).astype(bf16)
    for to in range(mine.shape[0]):
        mine[to, :, :LANES] = done


def block_of(held, x):
    return jnp.concatenate(
        [
            jnp.concatenate([held[x, f, :, :LANES], held[x, f, :, LANES:]], axis=0)
            for f in range(held.shape[1])
        ],
        axis=1,
    )


def half_kernel(core, z, rows, out, staged, held, arrived):
    steps = z.shape[0]
    copies = []
    for j, (to, c) in enumerate(((held, core[0]), (staged, 1 - core[0]))):
        for x in range(steps):
            at = pl.ds(pl.multiple_of((2 * x + c) * LANES, LANES), LANES)
            k = j * steps + x
            copies.append(pltpu.make_async_copy(rows.at[:, at], to.at[x], arrived.at[k]))
            copies[k].start()
    total = jnp.zeros(out.shape, f32)
    for x in range(steps):
        copies[x].wait()
        total = total + jnp.dot(z[x], block_of(held, x), preferred_element_type=f32)
    out[...] = total
    for x in range(steps):
        copies[steps + x].wait()


def output_kernel(z, staged, half, out):
    total = half[...]
    for x in range(z.shape[0]):
        total = total + jnp.dot(z[x], block_of(staged, x), preferred_element_type=f32)
    out[...] = total.astype(out.dtype)


def first_half(core, z, rows):
    vmem = pl.BlockSpec(memory_space=pltpu.VMEM)
    steps, tokens, width = z.shape
    parts = rows.shape[0]
    shape = (steps, parts, LANES, width)
    return pl.pallas_call(
        half_kernel,
        in_specs=[
            pl.BlockSpec(memory_space=pltpu.SMEM),
            vmem,
            pl.BlockSpec(memory_space=pltpu.HBM),
        ],
        out_specs=[vmem, vmem],
        compiler_params=limit,
        out_shape=[pltpu.VMEM((tokens, parts * LANES), f32), pltpu.VMEM(shape, bf16)],
        scratch_shapes=[pltpu.VMEM(shape, bf16), pltpu.SemaphoreType.DMA((2 * steps,))],
        name="half",
    )(core, near(z), pltpu.with_memory_space_constraint(rows, pltpu.HBM))


def body(
    activations,
    input_norm_gain,
    pooling_channel_weight,
    query_projection_weight,
    key_projection_weight,
    value_projection_weight,
    output_gate_weight,
    decay_first_factor,
    decay_second_factor,
    decay_gate_bias,
    decay_extra_log,
    head_norm_gain,
    starting_state,
    pooling_group_weight,
    pooling_channel_scale,
    pooling_output_rows,
    attention_output_rows,
):
    _, tokens, width = activations.shape
    columns = pooling_output_rows.shape[1]
    own = lax.axis_index("fs").astype(jnp.int32).reshape(1)
    tp = lax.axis_index("tp").astype(jnp.int32)
    late = pack_late(
        own,
        query_projection_weight,
        output_gate_weight,
        pooling_channel_weight,
        pooling_output_rows,
        attention_output_rows,
    )
    late, activations = lax.optimization_barrier((late, activations))
    late = lax.all_gather(late, "sp", axis=0, tiled=True)
    x, inverse, early = prepare(
        activations.reshape(tokens, width),
        input_norm_gain.reshape(1, width),
        key_projection_weight,
        value_projection_weight,
        decay_first_factor,
    )
    x = lax.all_to_all(x, "fs", 0, 0)
    early = lax.all_gather(early, "sp").reshape(-1, early.shape[1])
    inverse = near(inverse)
    parts, x, ends = early_partials(near(x), near(early))
    count = lax.axis_size("sp")
    ends = lax.ppermute(ends, "sp", [(i, i + 1) for i in range(count - 1)])
    parts = lax.all_to_all(parts, "fs", 0, 0)
    wide = pltpu.VMEM((tokens, LANES), f32)
    keys, values, sums, prior, opening, spread = call(
        local_kernel,
        [
            wide,
            wide,
            wide,
            wide,
            pltpu.VMEM((tokens // BLOCK, LANES), f32),
            struct((4, RUN_ROWS, LANES), bf16),
        ],
        "local",
        near(parts),
        inverse,
        decay_second_factor,
        decay_gate_bias.reshape(1, LANES),
        decay_extra_log,
        scalars=0,
    )
    start = starting_state[0].transpose(2, 0, 1).reshape(HEAD, LANES)
    quads = [[4 * a + b for b in range(4)] for a in range(lax.axis_size("sp") // 4)]
    late, _ = lax.optimization_barrier((late, spread))
    quad = lax.all_to_all(spread, "sp", 0, 0, axis_index_groups=quads)
    late_parts, quarter = late_partials(near(x), late, near(ends))
    _, _, quad = lax.optimization_barrier((late_parts, quarter, quad))
    out_rows = lax.all_gather(quarter, "fs")
    late = lax.all_to_all(late_parts, "fs", 0, 0)
    sp = lax.axis_index("sp").astype(jnp.int32).reshape(1)
    total, within, log_within, inverse_within = call(
        quad_kernel,
        [
            struct((1, RUN_ROWS, LANES), bf16),
            pltpu.VMEM((HEAD, LANES), f32),
            pltpu.VMEM((8, LANES), f32),
            pltpu.VMEM((8, LANES), f32),
        ],
        "quad_total",
        sp,
        near(quad),
    )
    strided = [list(column) for column in zip(*quads)]
    runs = lax.all_gather(total[0], "sp", axis_index_groups=strided)
    peers = lax.axis_size("tp")
    (mine,) = call(
        finish_kernel,
        [struct((peers // 2, tokens, 2 * LANES), bf16)],
        "finish",
        sp,
        tp.reshape(1),
        near(runs),
        near(within),
        near(log_within),
        near(inverse_within),
        near(start),
        near(late),
        inverse,
        near(keys),
        near(values),
        near(sums),
        near(prior),
        near(opening),
        head_norm_gain.reshape(1, LANES),
        pooling_group_weight[0],
        pooling_channel_scale.reshape(1, LANES),
        scalars=2,
    )
    groups = [[c + 2 * x for x in range(peers // 2)] for c in range(2)]
    same = lax.all_to_all(mine, "tp", 0, 0, axis_index_groups=groups)
    same, out_rows = lax.optimization_barrier((same, out_rows))
    other = lax.ppermute(same, "tp", [(i, i ^ 1) for i in range(peers)])
    core = (tp & 1).reshape(1)
    half, staged = first_half(core, same, out_rows)
    (result,) = call(
        output_kernel,
        [struct((tokens, columns), bf16)],
        "output",
        near(other),
        near(staged),
        near(half),
        scalars=0,
    )
    return result[None]


def solution(mesh):
    in_specs = (
        P("fs", "sp", None),
        P(),
        P(("sp", "fs"), "tp"),
        P(("sp", "fs"), "tp"),
        P(("sp", "fs"), "tp"),
        P(("sp", "fs"), "tp"),
        P(("sp", "fs"), "tp"),
        P(("sp", "fs"), None),
        P(None, "tp"),
        P("tp"),
        P("tp", "sp"),
        P("tp"),
        P("fs", "tp", None, None),
        P("tp", None, None),
        P("tp"),
        P("sp", "tp"),
        P("sp", "tp"),
    )
    out_specs = P("fs", "sp", "tp")

    return jax.shard_map(
        body, mesh=mesh, in_specs=in_specs, out_specs=out_specs, check_vma=False
    )
```
